32 devices in a mesh: ep: 8 (over z, core), tp: 4 (over y, x).
Axes of the slice: x: 2, y: 2, z: 4, core: 2. Of those that a mesh axis runs over, the one named last changes fastest.
Arguments:
- tokens: bfloat16 [1024, 4096], P('ep', 'tp'), may hold values from -6 to 6
- routes: int32 [1024, 2], P('ep'), may hold values from 0 to 15, all different within a row; in each aligned block of 128 rows (0 to 127, 128 to 255, ...) at most 20 rows name the same one
- route_weights: float32 [1024, 2], P('ep'), may hold values from 0.2 to 2
- cotangent: bfloat16 [1024, 4096], P('ep', 'tp'), may hold values from -6 to 6
- expert_gate: bfloat16 [16, 4096, 512], P('ep', 'tp'), may hold values from -0.09375 to 0.09375
- expert_up: bfloat16 [16, 4096, 512], P('ep', 'tp'), may hold values from -0.09375 to 0.09375
- expert_down: bfloat16 [16, 512, 4096], P('ep', None, 'tp'), may hold values from -0.25 to 0.25
- shared_gate: bfloat16 [4096, 512], P('tp'), may hold values from -0.09375 to 0.09375
- shared_up: bfloat16 [4096, 512], P('tp'), may hold values from -0.09375 to 0.09375
- shared_down: bfloat16 [512, 4096], P(None, 'tp'), may hold values from -0.25 to 0.25
Outputs:
- grad_tokens: bfloat16 [1024, 4096], P('ep', 'tp')
- grad_weights: float32 [1024, 2], P('ep')
- grad_expert_gate: float32 [16, 4096, 512], P('ep', 'tp')
- grad_expert_up: float32 [16, 4096, 512], P('ep', 'tp')
- grad_expert_down: float32 [16, 512, 4096], P('ep', None, 'tp')
- grad_shared_gate: float32 [4096, 512], P('tp', 'ep')
- grad_shared_up: float32 [4096, 512], P('tp', 'ep')
- grad_shared_down: float32 [512, 4096], P('ep', 'tp')
The draws below stay inside these ranges and needn't reach their ends.
Inputs may be any that keep to these rules, and one draw needn't show every extreme that they name: `routes`: each row names 2 different experts. In each aligned block of 128 rows (the rows of one index of ep) no expert is named by more than 20 rows, a bound that some block reaches.
All inputs are finite; a program needn't handle non-finite values.
Results may differ from the reference program's by a relative error of at most 0.0054.
Values may be sent and summed in bfloat16 or wider, within the bound.
A program may use at most 64 MiB of HBM per device.

```python
import math
import jax
import jax.numpy as jnp
import numpy as np
from jax import lax

D = 4096
FF = 512
SFF = 512
TOPK = 2
TOK_DEV = 128
EXPERTS = 16
CAP = 20
TOKENS = 1024
N_EP = 8


def levels(own_key, shape, cuts, least, largest):
    def one(position, parts):
        heights = jax.random.uniform(jax.random.fold_in(jax.random.fold_in(own_key, 6), position), (parts,), jnp.float32, least / len(cuts), largest / len(cuts))
        return jnp.repeat(jnp.exp(heights), shape[position] // parts).reshape((-1,) + (1,) * (len(shape) - position - 1))

    level = one(*cuts[0])
    for cut in cuts[1:]:
        level = level * one(*cut)
    return level


def routed_block(own_key, own, number, rows, count, top, reach, lean):
    ranking = jax.random.permutation(own_key, count)
    heavy_load, common = portions_of(count, rows * top, reach, lean, True), portions_of(count, rows * top, reach, lean, False)
    places = jnp.arange(count)

    def named(lengths, rotation):
        used = int((lengths > 0).sum())
        fixed = max(1, used // 4)
        shifted = fixed + (places - fixed + rotation * (used - fixed)) % max(1, count - fixed)
        return jnp.zeros((count,), jnp.int32).at[ranking[jnp.where(places < fixed, places, shifted)]].set(jnp.asarray(lengths, jnp.int32))

    lengths = jnp.where(number % 4 == 0, named(heavy_load, number // 4), named(common, number - number // 4 - 1))
    mixed = jax.random.permutation(jax.random.fold_in(own, 3), count)
    giver, sink = mixed[0:count // 2 * 2:2], mixed[1:count // 2 * 2:2]
    margin = jnp.minimum(lengths[giver] - 1, reach - lengths[sink]) // 2
    margin = jnp.where((giver == ranking[0]) | (sink == ranking[0]) | (lengths[sink] == 0), 0, jnp.maximum(margin, 0))
    shifted = jax.random.randint(jax.random.fold_in(own, 4), (count // 2,), 0, 1 << 20) % (margin + 1)
    lengths = lengths.at[giver].add(-shifted).at[sink].add(shifted)
    members = jnp.searchsorted(jnp.cumsum(lengths), jnp.arange(rows * top), side="right").astype(jnp.int32)
    table = members.reshape(top, rows).T
    table = table[jax.random.permutation(jax.random.fold_in(own, 1), rows)]
    rotation = jax.random.randint(jax.random.fold_in(own, 2), (rows, 1), 0, top)
    return jnp.take_along_axis(table, (jnp.arange(top)[None, :] + rotation) % top, axis=1)


def portions_of(number_of, total, most, lean, full):
    loads = [(1 << 20) // math.isqrt(grade ** lean) + 1 for grade in range(1, number_of + 1)]
    largest = most if full else min(most, max(-(-total // number_of), total * loads[0] // sum(loads)))
    least = 1 if total - largest >= number_of - 1 else 0
    given, rest = [largest] + [least] * (number_of - 1), total - largest - least * (number_of - 1)
    while rest > 0:
        free = [i for i in range(1, number_of) if given[i] < largest] or [i for i in range(1, number_of) if given[i] < most]
        pool, remaining = sum([loads[i] for i in free]), rest
        for i in free:
            extra = min(most - given[i], max(1, remaining * loads[i] // pool), rest)
            given[i] = given[i] + extra
            rest = rest - extra
    return np.array(given)


def centred(own_key, dims, width, bound, shards=(), kind=jnp.bfloat16):
    entries = width * jax.random.normal(own_key, dims, jnp.float32)
    if shards:
        entries = entries * levels(own_key, dims, shards, -0.22, 0.18)
    return jnp.clip(entries, -bound, bound).astype(kind)


def setup_inputs(seed: int = 0) -> dict:
    streams_of = jax.random.split(jax.random.key(seed), 11)
    tokens = centred(streams_of[0], (TOKENS, D), 1.0, 6.0, ((0, 8), (1, 4)))
    routes_keys = jax.random.split(jax.random.fold_in(streams_of[1], 1), TOKENS // TOK_DEV)
    routes_turns = jax.random.permutation(jax.random.fold_in(streams_of[1], 3), TOKENS // TOK_DEV)
    routes = jax.vmap(lambda own, number: routed_block(jax.random.fold_in(streams_of[1], 2), own, number, TOK_DEV, EXPERTS, TOPK, CAP, 2))(routes_keys, routes_turns).reshape((TOKENS, TOPK))
    route_weights = jnp.clip(0.2 + 1.8 * jax.random.uniform(streams_of[2], (TOKENS, TOPK), jnp.float32) ** levels(streams_of[2], (TOKENS, TOPK), ((0, 8),), -0.2, 0.2), 0.2, 2.0)
    cotangent = centred(streams_of[3], (TOKENS, D), 1.0, 6.0, ((0, 8), (1, 4)))
    expert_gate = centred(streams_of[4], (EXPERTS, D, FF), D ** -0.5, 0.09375, ((0, 8), (1, 4)))
    expert_up = centred(streams_of[5], (EXPERTS, D, FF), D ** -0.5, 0.09375, ((0, 8), (1, 4)))
    expert_down = centred(streams_of[6], (EXPERTS, FF, D), FF ** -0.5, 0.25, ((0, 8), (2, 4)))
    shared_gate = centred(streams_of[7], (D, SFF), D ** -0.5, 0.09375, ((0, 4),))
    shared_up = centred(streams_of[8], (D, SFF), D ** -0.5, 0.09375, ((0, 4),))
    shared_down = centred(streams_of[9], (SFF, D), SFF ** -0.5, 0.25, ((1, 4),))
    return dict(tokens=tokens, routes=routes, route_weights=route_weights, cotangent=cotangent, expert_gate=expert_gate, expert_up=expert_up, expert_down=expert_down, shared_gate=shared_gate, shared_up=shared_up, shared_down=shared_down)


def rounded(values):
    return lax.optimization_barrier(values.astype(jnp.bfloat16)).astype(jnp.float32)


def hidden_terms(gate_pre, up_pre, back_grad, scaling):
    logistic = jax.nn.sigmoid(gate_pre)
    product = gate_pre * logistic * up_pre
    grad_act = scaling * back_grad
    gate_grad = (grad_act * up_pre * logistic * (1.0 + gate_pre * (1.0 - logistic))).astype(jnp.bfloat16)
    up_grad = (grad_act * gate_pre * logistic).astype(jnp.bfloat16)
    hidden = (scaling * product).astype(jnp.bfloat16)
    return gate_grad, up_grad, hidden, jnp.sum(back_grad * product, axis=-1)


def reference(tokens, routes, route_weights, cotangent, expert_gate, expert_up, expert_down,
              shared_gate, shared_up, shared_down):
    picked = routes.reshape(N_EP, TOK_DEV * TOPK)
    onehot = (picked[:, :, None] == jnp.arange(EXPERTS, dtype=jnp.int32)[None, None, :]).astype(jnp.int32)
    ranked = jnp.sum(jnp.cumsum(onehot, axis=1) * onehot, axis=2) - 1
    block_ids = jnp.arange(N_EP, dtype=jnp.int32)[:, None]
    slot_ids = (picked * (N_EP * CAP) + block_ids * CAP + ranked).reshape(-1).astype(jnp.int32)
    source_ids = jnp.full((EXPERTS * N_EP * CAP,), TOKENS * TOPK, jnp.int32)
    source_ids = source_ids.at[slot_ids].set(jnp.arange(TOKENS * TOPK, dtype=jnp.int32))
    token_ids = (source_ids // TOPK).astype(jnp.int32)
    tokens_pad = jnp.concatenate([tokens, jnp.zeros((1, D), jnp.bfloat16)], axis=0)
    cot_pad = jnp.concatenate([cotangent, jnp.zeros((1, D), jnp.bfloat16)], axis=0)
    gates_pad = jnp.concatenate([rounded(route_weights).reshape(-1), jnp.zeros((1,), jnp.float32)], axis=0)

    def expert_pass(inputs):
        token_index, source_index, weight_gate, weight_up, weight_down = inputs
        slot_tokens = tokens_pad[token_index]
        slot_cotan = cot_pad[token_index]
        slot_gates = gates_pad[source_index]
        gate_pre = jnp.dot(slot_tokens, weight_gate, preferred_element_type=jnp.float32)
        up_pre = jnp.dot(slot_tokens, weight_up, preferred_element_type=jnp.float32)
        back_grad = jnp.dot(slot_cotan, weight_down.T, preferred_element_type=jnp.float32)
        gate_grad, up_grad, hidden, slot_dg = hidden_terms(gate_pre, up_pre, back_grad, slot_gates[:, None])
        slot_grad = (jnp.dot(gate_grad, weight_gate.T, preferred_element_type=jnp.float32)
                     + jnp.dot(up_grad, weight_up.T, preferred_element_type=jnp.float32))
        grad_gate = jnp.dot(slot_tokens.T, gate_grad, preferred_element_type=jnp.float32)
        grad_up = jnp.dot(slot_tokens.T, up_grad, preferred_element_type=jnp.float32)
        grad_down = jnp.dot(hidden.T, slot_cotan, preferred_element_type=jnp.float32)
        return slot_grad, slot_dg, grad_gate, grad_up, grad_down

    slot_grad, slot_dg, grad_expert_gate, grad_expert_up, grad_expert_down = lax.map(
        expert_pass,
        (token_ids.reshape(EXPERTS, N_EP * CAP), source_ids.reshape(EXPERTS, N_EP * CAP),
         expert_gate, expert_up, expert_down))
    routed_grad = slot_grad.reshape(-1, D)[slot_ids].reshape(TOKENS, TOPK, D)
    routed_grad = jnp.sum(routed_grad, axis=1)
    grad_weights = slot_dg.reshape(-1)[slot_ids].reshape(TOKENS, TOPK)

    shared_gate_pre = jnp.dot(tokens, shared_gate, preferred_element_type=jnp.float32)
    shared_up_pre = jnp.dot(tokens, shared_up, preferred_element_type=jnp.float32)
    shared_back = jnp.dot(cotangent, shared_down.T, preferred_element_type=jnp.float32)
    shared_gate_grad, shared_up_grad, shared_hidden, unused_sum = hidden_terms(
        shared_gate_pre, shared_up_pre, shared_back, 1.0)
    shared_grad = (jnp.dot(shared_gate_grad, shared_gate.T, preferred_element_type=jnp.float32)
                   + jnp.dot(shared_up_grad, shared_up.T, preferred_element_type=jnp.float32))
    grad_shared_gate = jnp.dot(tokens.T, shared_gate_grad, preferred_element_type=jnp.float32)
    grad_shared_up = jnp.dot(tokens.T, shared_up_grad, preferred_element_type=jnp.float32)
    grad_shared_down = jnp.dot(shared_hidden.T, cotangent, preferred_element_type=jnp.float32)
    grad_tokens = (routed_grad + shared_grad).astype(jnp.bfloat16)
    return (grad_tokens, grad_weights, grad_expert_gate, grad_expert_up, grad_expert_down,
            grad_shared_gate, grad_shared_up, grad_shared_down)
```

```python
import functools

import jax
import jax.numpy as jnp
from jax import lax
from jax.experimental import pallas as pl
from jax.experimental.pallas import tpu as pltpu
from jax.sharding import PartitionSpec as P

CORES = 2
BF = jnp.bfloat16
F32 = jnp.float32


def up_to(value, unit):
    return -(-value // unit) * unit


def dot(a, b):
    return jnp.dot(a, b, preferred_element_type=F32)


def dot_t(a, b):
    return lax.dot_general(a, b, (((1,), (1,)), ((), ())), preferred_element_type=F32)


def hidden_terms(gate_pre, up_pre, back_grad, scaling):
    logistic = jax.nn.sigmoid(gate_pre)
    silu = gate_pre * logistic
    product = silu * up_pre
    grad_act = back_grad if scaling is None else scaling * back_grad
    gate_grad = grad_act * up_pre * logistic * (1.0 + gate_pre * (1.0 - logistic))
    hidden = product if scaling is None else scaling * product
    return (
        gate_grad.astype(BF),
        (grad_act * silu).astype(BF),
        hidden.astype(BF),
        jnp.sum(back_grad * product, axis=-1, keepdims=True),
    )


def ring_plan(length):
    plan = []
    for step in range(1, length // 2 + 1):
        last_even = length % 2 == 0 and step == length // 2
        plan.append((step, 0, (0,) if last_even else (0, 1)))
        plan.append((step, 1, (1,) if last_even else (1, 0)))
    return plan


def rows_kernel(
    dims,
    meta_in,
    tok_in,
    cot_in,
    eg_in,
    eu_in,
    ed_in,
    sg_in,
    su_in,
    sd_in,
    gtok_out,
    gw_out,
    osg,
    osu,
    osd,
    stok,
    scot,
    hg,
    hu,
    hh,
    all_tok,
    all_cot,
    all_meta,
    eg,
    eu,
    ed,
    sg,
    su,
    sd,
    sel,
    gates,
    sh_part,
    sh_recv,
    sh_all,
    share_t,
    part,
    exact,
    recv,
    dgs,
    back_send,
    back,
    shsum,
    load_sem,
    own_sem,
    ring_s,
    ring_r,
    mate_s,
    mate_r,
    shr_s,
    shr_r,
    sha_s,
    sha_r,
    pr_s,
    pr_r,
    pa_s,
    pa_r,
    xt_s,
    xt_r,
    bk_s,
    bk_r,
):
    ep, tp, tok, dl, ne, ff, sff, cap, re, rows, rpp, rpt, cp, swid = dims
    me = lax.axis_index("ep")
    mt = lax.axis_index("tp")
    length = ep // CORES
    chip = me // CORES
    core = me % CORES
    mate = chip * CORES + (1 - core)
    nxt = ((chip + 1) % length) * CORES + core
    prv = ((chip + length - 1) % length) * CORES + core

    owns = []
    for n, (src, dst) in enumerate(((tok_in, all_tok), (cot_in, all_cot), (meta_in, all_meta))):
        c = pltpu.make_async_copy(src, dst.at[me], own_sem.at[n])
        c.start()
        owns.append(c)
    loads = []
    for n, (src, dst) in enumerate(
        ((sg_in, sg), (su_in, su), (sd_in, sd), (eg_in, eg), (eu_in, eu), (ed_in, ed))
    ):
        c = pltpu.make_async_copy(src, dst, load_sem.at[n])
        c.start()
        loads.append(c)

    barrier = pltpu.get_barrier_semaphore()
    for o in range(1, ep):
        pl.semaphore_signal(barrier, inc=1, device_id={"ep": (me + o) % ep})
    for o in range(1, tp):
        pl.semaphore_signal(barrier, inc=1, device_id={"tp": (mt + o) % tp})
    pl.semaphore_wait(barrier, ep + tp - 2)

    sends = []

    def remote(src, dst, ssem, rsem, dev):
        c = pltpu.make_async_remote_copy(
            src_ref=src, dst_ref=dst, send_sem=ssem, recv_sem=rsem, device_id=dev
        )
        c.start()
        sends.append(c)
        return c

    bufs = (all_tok, all_cot, all_meta)
    ring_copies = {}
    mate_copies = []
    plan = {(step, d): items for step, d, items in ring_plan(length)}

    def ring_send(step, d, item, src):
        dest = nxt if d == 0 else prv
        subs = (0, 2) if item == 0 else (1,)
        for b in subs:
            n = ((step - 1) * 2 + d) * 3 + b
            ring_copies[step, d, b] = remote(
                bufs[b].at[src], bufs[b].at[src], ring_s.at[n], ring_r.at[n], {"ep": dest}
            )

    def mate_send(item, src):
        for b in (0, 2) if item == 0 else (1,):
            n = len(mate_copies)
            mate_copies.append(
                remote(
                    bufs[b].at[src], bufs[b].at[src], mate_s.at[n], mate_r.at[n], {"ep": mate}
                )
            )

    for c in owns:
        c.wait()
    for pos in range(2):
        for d in range(2):
            items = plan.get((1, d), ())
            if pos < len(items):
                ring_send(1, d, items[pos], me)
    mate_send(0, me)
    mate_send(1, me)

    tp_order = [(mt + o) % tp for o in range(1, tp)]
    if rpt * tp > tok:
        sh_part[:, tok:, :] = jnp.zeros((3, rpt * tp - tok, sff), BF)
    for n in range(3):
        loads[n].wait()
        if n < 2:
            val = dot(all_tok[me], (sg, su)[n][...])
        else:
            val = dot_t(all_cot[me], sd[...])
        sh_part[n, :tok, :] = val.astype(BF)
    sh_copies = []
    for o in range(1, tp):
        peer = tp_order[o - 1]
        sh_copies.append(
            remote(
                sh_part.at[:, pl.ds(pl.multiple_of(peer * rpt, 16), rpt), :],
                sh_recv.at[o],
                shr_s.at[o],
                shr_r.at[o],
                {"tp": peer},
            )
        )

    def ring_arrivals(step):
        for pos in range(2):
            for d in range(2):
                items = plan.get((step, d), ())
                if pos >= len(items):
                    continue
                item = items[pos]
                away = length - step if d == 0 else step
                src = ((chip + away) % length) * CORES + core
                for b in (0, 2) if item == 0 else (1,):
                    ring_copies[step, d, b].wait_recv()
                if item in plan.get((step + 1, d), ()):
                    ring_send(step + 1, d, item, src)
                mate_send(item, src)

    if length > 1:
        ring_arrivals(1)

    for c in sh_copies:
        c.wait_recv()
    mine_t = pl.ds(pl.multiple_of(mt * rpt, 16), rpt)
    tot = [sh_part[n, mine_t, :].astype(F32) for n in range(3)]
    for o in range(1, tp):
        for n in range(3):
            tot[n] = tot[n] + sh_recv[o, n].astype(F32)
    a, b, c3, _ = hidden_terms(tot[0], tot[1], tot[2], None)
    sh_all[0, mine_t, :] = a
    sh_all[1, mine_t, :] = b
    sh_all[2, mine_t, :] = c3
    sha = []
    for o in range(1, tp):
        sha.append(
            remote(
                sh_all.at[:, mine_t, :],
                sh_all.at[:, mine_t, :],
                sha_s.at[o],
                sha_r.at[o],
                {"tp": tp_order[o - 1]},
            )
        )

    for step in range(2, length // 2 + 1):
        ring_arrivals(step)
    for c in mate_copies:
        c.wait_recv()

    row_id = lax.broadcasted_iota(jnp.int32, (rows, tok), 0)
    gate = jnp.zeros((rows, 1), F32)
    for j in range(ep):
        m = all_meta[j]
        code = m[0:2, :].astype(jnp.int32) + (j * cap - me * (ne * re))
        p0 = (row_id == code[0:1, :]).astype(F32)
        p1 = (row_id == code[1:2, :]).astype(F32)
        sel[:, j * tok : (j + 1) * tok] = (p0 + p1).astype(BF)
        gate = gate + jnp.sum(p0 * m[2:3, :] + p1 * m[3:4, :], axis=1, keepdims=True)
    te = rpp * tp
    for e in range(ne):
        gates[e, :re, :] = jnp.broadcast_to(gate[e * re : (e + 1) * re, :], (re, 128))
        if te > re:
            gates[e, re:, :] = jnp.zeros((te - re, 128), F32)
            part[e, :, re:, :] = jnp.zeros((3, te - re, ff), BF)
            exact[e, :, re:, :] = jnp.zeros((3, te - re, ff), F32)

    stok[...] = dot(sel[...], all_tok[...].reshape(ep * tok, dl)).astype(BF)
    scot[...] = dot(sel[...], all_cot[...].reshape(ep * tok, dl)).astype(BF)
    for n in range(3):
        loads[3 + n].wait()
    p_copies = [[] for _ in range(ne)]
    for e in range(ne):
        for n in range(3):
            r = slice(e * re, (e + 1) * re)
            val = dot_t(scot[r, :], ed[e]) if n == 2 else dot(stok[r, :], (eg, eu)[n][e])
            exact[e, n, :re, :] = val
            part[e, n, :re, :] = val.astype(BF)
            for o in range(1, tp):
                peer = tp_order[o - 1]
                k = (e * 3 + n) * tp + o
                p_copies[e].append(
                    remote(
                        part.at[e, n, pl.ds(pl.multiple_of(peer * rpp, 8), rpp), :],
                        recv.at[o, e, n],
                        pr_s.at[k],
                        pr_r.at[k],
                        {"tp": peer},
                    )
                )

    for c in sha:
        c.wait_recv()
    for n in range(3):
        back_t = sh_all[n, :tok, :].astype(F32).T.astype(BF)
        for j in range(ep):
            share_t[0, n, j] = back_t[j * swid : (j + 1) * swid, :]
    xts = []
    for o in range(1, ep):
        peer = (me + o) % ep
        xts.append(
            remote(
                share_t.at[0, :, peer],
                share_t.at[1, :, me],
                xt_s.at[o],
                xt_r.at[o],
                {"ep": peer},
            )
        )
    for n in range(3):
        share_t[1, n, me] = share_t[0, n, me]
    mine = pl.ds(pl.multiple_of(mt * rpp, 8), rpp)
    lane = lax.broadcasted_iota(jnp.int32, (rpp, 128), 1)
    pas = []
    for e in range(ne):
        for c in p_copies[e]:
            c.wait_recv()
        tot = [exact[e, n, mine, :] for n in range(3)]
        for o in range(1, tp):
            for n in range(3):
                tot[n] = tot[n] + recv[o, e, n].astype(F32)
        a, b, c3, dg = hidden_terms(tot[0], tot[1], tot[2], gates[e, mine, :][:, 0:1])
        hg[e, mine, :] = a
        hu[e, mine, :] = b
        hh[e, mine, :] = c3
        high = dg.astype(BF).astype(F32)
        dgs[e, mine, :] = jnp.where(
            lane == 0, high, jnp.where(lane == 1, dg - high, 0.0)
        ).astype(BF)
        group = []
        for k, buf in enumerate((hg, hu, dgs, hh)):
            for o in range(1, tp):
                n = (e * 4 + k) * tp + o
                group.append(
                    remote(
                        buf.at[e, mine, :],
                        buf.at[e, mine, :],
                        pa_s.at[n],
                        pa_r.at[n],
                        {"tp": tp_order[o - 1]},
                    )
                )
        pas.append(group)

    col = lax.broadcasted_iota(jnp.int32, (8, re), 1)
    block = jnp.zeros((8, re), jnp.int32)
    for j in range(1, ep):
        block = block + (col >= j * cap).astype(jnp.int32)
    target = block * cp + (col - block * cap)
    target = jnp.where(col < ep * cap, target, -1)
    pick = (
        (lax.broadcasted_iota(jnp.int32, (ep * cp, re), 0) == target[0:1, :])
        .astype(F32)
        .astype(BF)
    )
    bks = []
    for e in range(ne):
        for c in pas[e][: 3 * (tp - 1)]:
            c.wait_recv()
        slot = (dot_t(hg[e, :re, :], eg[e]) + dot_t(hu[e, :re, :], eu[e])).astype(BF)
        back_send[e, :, :, :dl] = dot(pick, slot).astype(BF).reshape(ep, cp, dl)
        back_send[e, :, :, dl:] = dot(pick, dgs[e, :re, :]).astype(BF).reshape(ep, cp, 128)
        for o in range(1, ep):
            peer = (me + o) % ep
            bks.append(
                remote(
                    back_send.at[e, peer],
                    back.at[e, me],
                    bk_s.at[e * ep + o],
                    bk_r.at[e * ep + o],
                    {"ep": peer},
                )
            )
        back[e, me] = back_send[e, me]

    shsum[...] = dot_t(sh_all[0, :tok, :], sg[...]) + dot_t(sh_all[1, :tok, :], su[...])
    for c in xts:
        c.wait_recv()
    flat = [
        jnp.concatenate([share_t[1, n, j] for j in range(ep)], axis=1) for n in range(3)
    ]
    tok_flat = all_tok[...].reshape(ep * tok, dl)
    osg[...] = dot(flat[0], tok_flat)
    osu[...] = dot(flat[1], tok_flat)
    osd[...] = dot(flat[2], all_cot[...].reshape(ep * tok, dl))

    width = ne * ep * cp
    home = all_meta[me].T.astype(jnp.int32)
    hcol = lax.broadcasted_iota(jnp.int32, (tok, width), 1)
    g0 = (hcol == home[:, 4:5]).astype(F32)
    g1 = (hcol == home[:, 5:6]).astype(F32)
    both = (g0 + g1).astype(BF)
    for c in bks:
        c.wait_recv()
    flat_back = back[...].reshape(width, dl + 128)
    gtok_out[...] = (dot(both, flat_back[:, :dl]) + shsum[...]).astype(BF)
    w0 = jnp.sum(dot(g0.astype(BF), flat_back[:, dl:]), axis=1, keepdims=True)
    w1 = jnp.sum(dot(g1.astype(BF), flat_back[:, dl:]), axis=1, keepdims=True)
    wl = lax.broadcasted_iota(jnp.int32, (tok, 128), 1)
    gw_out[...] = jnp.where(wl == 0, w0, w1).T[0:2, :]
    for group in pas:
        for c in group[3 * (tp - 1) :]:
            c.wait_recv()
    for c in sends:
        c.wait_send()


def rows_body(
    tokens,
    routes,
    route_weights,
    cotangent,
    expert_gate,
    expert_up,
    expert_down,
    shared_gate,
    shared_up,
    shared_down,
):
    tok, top = routes.shape
    dl = tokens.shape[1]
    ne, _, ff = expert_gate.shape
    sff = shared_gate.shape[1]
    ep, tp = lax.axis_size("ep"), lax.axis_size("tp")
    cap = max(2, 5 * tok * top // (4 * ep * ne))
    re = up_to(ep * cap, 16)
    rows = ne * re
    rpp = up_to(-(-re // tp), 8)
    rpt = up_to(-(-tok // tp), 16)
    cp = up_to(cap, 8)
    swid = sff // ep
    length = ep // CORES
    total = rpp * tp
    dims = (ep, tp, tok, dl, ne, ff, sff, cap, re, rows, rpp, rpt, cp, swid)

    picked = routes.T.reshape(-1)
    earlier = jnp.arange(top * tok)[None, :] < jnp.arange(top * tok)[:, None]
    same = picked[:, None] == picked[None, :]
    ranked = jnp.sum((same & earlier).astype(jnp.int32), axis=1)
    code = (picked * re + ranked).reshape(top, tok)
    home = (((picked % ne) * ep + picked // ne) * cp + ranked).reshape(top, tok)
    gate = route_weights.astype(BF).astype(F32).T
    meta = jnp.concatenate(
        [code.astype(F32), gate, home.astype(F32), jnp.zeros((8 - 3 * top, tok), F32)], axis=0
    )

    vm = pl.BlockSpec(memory_space=pltpu.VMEM)
    hbm = pl.BlockSpec(memory_space=pl.ANY)
    dma = pltpu.SemaphoreType.DMA
    n_ring = max(1, (length // 2) * 6)
    scratch = [
        pltpu.VMEM((ep, tok, dl), BF),
        pltpu.VMEM((ep, tok, dl), BF),
        pltpu.VMEM((ep, 8, tok), F32),
        pltpu.VMEM(expert_gate.shape, BF),
        pltpu.VMEM(expert_up.shape, BF),
        pltpu.VMEM(expert_down.shape, BF),
        pltpu.VMEM(shared_gate.shape, BF),
        pltpu.VMEM(shared_up.shape, BF),
        pltpu.VMEM(shared_down.shape, BF),
        pltpu.VMEM((rows, ep * tok), BF),
        pltpu.VMEM((ne, total, 128), F32),
        pltpu.VMEM((3, rpt * tp, sff), BF),
        pltpu.VMEM((tp, 3, rpt, sff), BF),
        pltpu.VMEM((3, rpt * tp, sff), BF),
        pltpu.VMEM((2, 3, ep, swid, tok), BF),
        pltpu.VMEM((ne, 3, total, ff), BF),
        pltpu.VMEM((ne, 3, total, ff), F32),
        pltpu.VMEM((tp, ne, 3, rpp, ff), BF),
        pltpu.VMEM((ne, total, 128), BF),
        pltpu.VMEM((ne, ep, cp, dl + 128), BF),
        pltpu.VMEM((ne, ep, cp, dl + 128), BF),
        pltpu.VMEM((tok, dl), F32),
        dma((6,)),
        dma((3,)),
        dma((n_ring,)),
        dma((n_ring,)),
        dma((3 * length,)),
        dma((3 * length,)),
        dma((tp,)),
        dma((tp,)),
        dma((tp,)),
        dma((tp,)),
        dma((3 * ne * tp,)),
        dma((3 * ne * tp,)),
        dma((4 * ne * tp,)),
        dma((4 * ne * tp,)),
        dma((ep,)),
        dma((ep,)),
        dma((ne * ep,)),
        dma((ne * ep,)),
    ]
    sds = jax.ShapeDtypeStruct
    outs = pl.pallas_call(
        functools.partial(rows_kernel, dims),
        out_shape=(
            sds((tok, dl), BF),
            sds((top, tok), F32),
            sds((swid, dl), F32),
            sds((swid, dl), F32),
            sds((swid, dl), F32),
            sds((rows, dl), BF),
            sds((rows, dl), BF),
            sds((ne, total, ff), BF),
            sds((ne, total, ff), BF),
            sds((ne, total, ff), BF),
        ),
        in_specs=[hbm] * 9,
        out_specs=tuple([vm] * 10),
        scratch_shapes=scratch,
        compiler_params=pltpu.CompilerParams(
            collective_id=0, has_side_effects=True, vmem_limit_bytes=60 * 1024 * 1024
        ),
    )(
        meta,
        tokens,
        cotangent,
        expert_gate,
        expert_up,
        expert_down,
        shared_gate,
        shared_up,
        shared_down,
    )
    gtok, gw, osg, osu, osd, stok, scot, hg, hu, hh = outs
    stok = stok.reshape(ne, re, dl)
    scot = scot.reshape(ne, re, dl)
    hg, hu, hh = (h[:, :re] for h in (hg, hu, hh))
    grad_gate = jnp.einsum("esd,esf->edf", stok, hg, preferred_element_type=F32)
    grad_up = jnp.einsum("esd,esf->edf", stok, hu, preferred_element_type=F32)
    grad_down = jnp.einsum("esf,esd->efd", hh, scot, preferred_element_type=F32)
    return gtok, gw.T, grad_gate, grad_up, grad_down, osg.T, osu.T, osd


def line_order(chip, length):
    high = (2 * chip) // length
    far = 1 - 2 * high
    edge = chip * (1 - high) + (length - 1 - chip) * high
    order = [(chip, None, None)]
    for p in range(1, length):
        two_sided = (2 * edge - p + 2 * length) // (2 * length)
        dist = two_sided * ((p + 1) // 2) + (1 - two_sided) * (p - edge)
        toward = far * (1 - 2 * two_sided * (p % 2))
        order.append((chip + toward * dist, chip - toward, two_sided))
    return order


def line_kernel(
    dims,
    meta_in,
    tok_in,
    cot_in,
    eg_in,
    eu_in,
    ed_in,
    sg_in,
    su_in,
    sd_in,
    gtok_out,
    gw_out,
    osg,
    osu,
    osd,
    stok,
    scot,
    hg,
    hu,
    hh,
    all_tok,
    all_cot,
    all_meta,
    eg,
    eu,
    ed,
    sg,
    su,
    sd,
    gates,
    sh_part,
    sh_exact,
    sh_recv,
    sh_all,
    share_t,
    part,
    exact,
    recv,
    hs,
    dgp,
    dgs,
    dgb,
    back_send,
    back,
    shsum,
    load_sem,
    own_sem,
    own_s,
    line_s,
    line_r,
    mate_s,
    mate_r,
    shr_s,
    shr_r,
    sha_s,
    sha_r,
    pr_s,
    pr_r,
    pa_s,
    pa_r,
    xt_s,
    xt_r,
    bk_s,
    bk_r,
):
    ep, tp, tok, dl, ne, ff, sff, cap, rows, width, swidth, swid = dims
    me = lax.axis_index("ep")
    mt = lax.axis_index("tp")
    length = ep // CORES
    chip = me // CORES
    core = me % CORES
    mate = chip * CORES + (1 - core)
    pair = CORES * cap
    group = ne * pair
    home = ne * cap
    order = line_order(chip, length)
    bufs = (all_tok, all_meta, all_cot)

    owns = []
    for n, (src, dst) in enumerate(((tok_in, all_tok), (meta_in, all_meta), (cot_in, all_cot))):
        c = pltpu.make_async_copy(src, dst.at[chip, core], own_sem.at[n])
        c.start()
        owns.append(c)
    loads = []
    for n, (src, dst) in enumerate(
        ((sg_in, sg), (su_in, su), (sd_in, sd), (eg_in, eg), (eu_in, eu), (ed_in, ed))
    ):
        c = pltpu.make_async_copy(src, dst, load_sem.at[n])
        c.start()
        loads.append(c)

    barrier = pltpu.get_barrier_semaphore()
    for o in range(1, ep):
        pl.semaphore_signal(barrier, inc=1, device_id={"ep": (me + o) % ep})
    for o in range(1, tp):
        pl.semaphore_signal(barrier, inc=1, device_id={"tp": (mt + o) % tp})
    pl.semaphore_wait(barrier, ep + tp - 2)

    sends = []

    def copy_of(src, dst, ssem, rsem, dev):
        return pltpu.make_async_remote_copy(
            src_ref=src, dst_ref=dst, send_sem=ssem, recv_sem=rsem, device_id=dev
        )

    def remote(src, dst, ssem, rsem, dev):
        c = copy_of(src, dst, ssem, rsem, dev)
        c.start()
        sends.append((None, c))
        return c

    def along_line(b, src, ssem, there):
        block = bufs[b].at[src, core]
        dest = ((there + length) % length) * CORES + core
        return copy_of(block, block, ssem, line_r.at[b * length + src], {"ep": dest})

    def to_mate(b, p):
        block = bufs[b].at[order[p][0], core]
        n = b * length + p
        return copy_of(block, block, mate_s.at[n], mate_r.at[n], {"ep": mate})

    for b in range(3):
        owns[b].wait()
        for d, there in enumerate((chip + 1, chip - 1)):
            c = along_line(b, chip, own_s.at[2 * b + d], there)
            inside = chip < length - 1 if d == 0 else chip > 0
            pl.when(inside)(c.start)
            sends.append((inside, c))
        c = to_mate(b, 0)
        c.start()
        sends.append((None, c))

    relays = {}
    mates = {}
    for p in range(1, length):
        src, there, _ = order[p]
        for b in range(3):
            relays[b, p] = along_line(b, src, line_s.at[b * length + p], there)
            mates[b, p] = to_mate(b, p)
            sends.append(((there >= 0) & (there < length), relays[b, p]))
            sends.append((None, mates[b, p]))

    def arrivals(p, which, cond=None):
        def run():
            _, there, _ = order[p]
            for b in which:
                relays[b, p].wait_recv()
                pl.when((there >= 0) & (there < length))(relays[b, p].start)
                mates[b, p].start()

        if cond is None:
            run()
        else:
            pl.when(cond)(run)

    def mate_wait(p, which):
        for b in which:
            to_mate(b, p).wait_recv()

    peers = [(mt + o) % tp for o in range(1, tp)]

    own_tok = all_tok[chip, core]
    own_cot = all_cot[chip, core]
    for n in range(3):
        loads[n].wait()
        val = dot(own_tok, (sg, su)[n][...]) if n < 2 else dot_t(own_cot, sd[...])
        for q in range(tp):
            piece = val[:, q * swidth : (q + 1) * swidth]
            sh_exact[q, n] = piece
            sh_part[q, n] = piece.astype(BF)
    sh_copies = []
    for o in range(1, tp):
        sh_copies.append(
            remote(
                sh_part.at[peers[o - 1]],
                sh_recv.at[o],
                shr_s.at[o],
                shr_r.at[o],
                {"tp": peers[o - 1]},
            )
        )

    row_id = lax.broadcasted_iota(jnp.int32, (ne * rows, tok), 0)
    sels = {}
    pr_copies = {}

    def selection(p):
        src = order[p][0]
        halves = []
        gate = jnp.zeros((ne * rows, 1), F32)
        for jj in range(CORES):
            m = all_meta[src, jj]
            code = m[0:2, :].astype(jnp.int32) + (jj * cap - me * (ne * rows))
            p0 = (row_id == code[0:1, :]).astype(F32)
            p1 = (row_id == code[1:2, :]).astype(F32)
            halves.append((p0 + p1).astype(BF))
            gate = gate + jnp.sum(p0 * m[2:3, :] + p1 * m[3:4, :], axis=1, keepdims=True)
        sels[p] = jnp.concatenate(halves, axis=1)
        gate = jnp.concatenate([gate[e * rows : e * rows + pair] for e in range(ne)], axis=0)
        gates[p] = jnp.broadcast_to(gate, (group, 128))

    def products(p, which):
        src = order[p][0]
        buf, out = (all_cot, scot) if which == (2,) else (all_tok, stok)
        picked = dot(sels[p], buf[src].reshape(CORES * tok, dl)).astype(BF)
        for e in range(ne):
            out[e, p * rows : (p + 1) * rows, :] = picked[e * rows : (e + 1) * rows]
        for n in which:
            vals = []
            for e in range(ne):
                x = picked[e * rows : (e + 1) * rows]
                val = dot_t(x, ed[e]) if n == 2 else dot(x, (eg, eu)[n][e])
                vals.append(val[:pair])
            val = jnp.concatenate(vals, axis=0)
            for q in range(tp):
                piece = val[:, q * width : (q + 1) * width]
                exact[p, q, n] = piece
                part[p, q, n] = piece.astype(BF)
        half = 1 if which == (2,) else 0
        span = pl.ds(which[0], len(which))
        for o in range(1, tp):
            k = (p * 2 + half) * tp + o
            pr_copies[p, half, o] = remote(
                part.at[p, peers[o - 1], span],
                recv.at[p, o, span],
                pr_s.at[k],
                pr_r.at[k],
                {"tp": peers[o - 1]},
            )

    def products_all(p):
        selection(p)
        products(p, (0, 1))
        products(p, (2,))

    pa_copies = {}

    def hidden(p):
        for half in range(2):
            for o in range(1, tp):
                pr_copies[p, half, o].wait_recv()
        tot = [exact[p, mt, n] for n in range(3)]
        for o in range(1, tp):
            for n in range(3):
                tot[n] = tot[n] + recv[p, o, n].astype(F32)
        gate = gates[p][:, 0:1]
        logistic = jax.nn.sigmoid(tot[0])
        silu = tot[0] * logistic
        product = silu * tot[1]
        grad_act = gate * tot[2]
        hs[p, mt, 0] = (
            grad_act * tot[1] * logistic * (1.0 + tot[0] * (1.0 - logistic))
        ).astype(BF)
        hs[p, mt, 1] = (grad_act * silu).astype(BF)
        hs[p, mt, 2] = (gate * product).astype(BF)
        terms = tot[2] * product
        fill = jnp.zeros((128 - group, width), F32)
        cols = jnp.concatenate([terms, fill], axis=0).T
        dgp[p, mt] = jnp.broadcast_to(jnp.sum(cols, axis=0, keepdims=True), (8, 128))
        for piece in range(3):
            for o in range(1, tp):
                k = (p * 3 + piece) * tp + o
                if piece < 2:
                    block = hs.at[p, mt, pl.ds(2 * piece, 2 - piece)]
                else:
                    block = dgp.at[p, mt]
                pa_copies[p, piece, o] = remote(
                    block, block, pa_s.at[k], pa_r.at[k], {"tp": peers[o - 1]}
                )

    def pick_rows():
        at = lax.broadcasted_iota(jnp.int32, (group, group), 0)
        col = lax.broadcasted_iota(jnp.int32, (group, group), 1)
        wanted = at * 0
        for jj in range(CORES):
            for e in range(ne):
                low = jj * home + e * cap
                inside = (at >= low) & (at < low + cap)
                wanted = jnp.where(inside, at - low + e * pair + jj * cap, wanted)
        return (col == wanted).astype(F32).astype(BF)

    pick = pick_rows()
    bk_copies = []

    def spread(p, n, out):
        full = jnp.concatenate([hs[p, q, n] for q in range(tp)], axis=1).astype(F32)
        fill = jnp.zeros((rows - pair, ff), F32)
        blocks = []
        for e in range(ne):
            block = full[e * pair : (e + 1) * pair]
            if rows > pair:
                block = jnp.concatenate([block, fill], axis=0)
            block = block.astype(BF)
            out[e, p * rows : (p + 1) * rows, :] = block
            blocks.append(block)
        return blocks

    def slots(p):
        src = order[p][0]
        for o in range(1, tp):
            pa_copies[p, 0, o].wait_recv()
        a = spread(p, 0, hg)
        b = spread(p, 1, hu)
        vals = [(dot_t(a[e], eg[e]) + dot_t(b[e], eu[e]))[:pair] for e in range(ne)]
        slot = jnp.concatenate(vals, axis=0).astype(BF)
        moved = dot(pick, slot)
        for jj in range(CORES):
            back_send[p, jj] = moved[jj * home : (jj + 1) * home].astype(BF)
        for o in range(1, tp):
            pa_copies[p, 2, o].wait_recv()
        total = dgp[p, 0]
        for q in range(1, tp):
            total = total + dgp[p, q]
        dgs[p] = total
        if p == 0:
            back[me] = back_send[0, core]
            dgb[me] = total
            targets = [(1 - core, mate)]
        else:
            targets = [(jj, src * CORES + jj) for jj in range(CORES)]
        for n, (jj, dest) in enumerate(targets):
            k = p * CORES + n
            bk_copies.append(
                remote(back_send.at[p, jj], back.at[me], bk_s.at[2 * k], bk_r.at[me], {"ep": dest})
            )
            bk_copies.append(
                remote(dgs.at[p], dgb.at[me], bk_s.at[2 * k + 1], bk_r.at[ep + me], {"ep": dest})
            )

    def shared_hidden():
        for c in sh_copies:
            c.wait_recv()
        tot = [sh_exact[mt, n] for n in range(3)]
        for o in range(1, tp):
            for n in range(3):
                tot[n] = tot[n] + sh_recv[o, n].astype(F32)
        a, b, c3, _ = hidden_terms(tot[0], tot[1], tot[2], None)
        sh_all[mt, 0] = a
        sh_all[mt, 1] = b
        sh_all[mt, 2] = c3
        return [
            remote(sh_all.at[mt], sh_all.at[mt], sha_s.at[o], sha_r.at[o], {"tp": peers[o - 1]})
            for o in range(1, tp)
        ]

    def shared_full(n):
        return jnp.concatenate([sh_all[q, n] for q in range(tp)], axis=1)

    def shared_shares():
        for n in range(3):
            back_t = shared_full(n).astype(F32).T.astype(BF)
            for j in range(ep):
                share_t[0, n, j] = back_t[j * swid : (j + 1) * swid, :]
        copies = []
        for o in range(1, ep):
            peer = (me + o) % ep
            copies.append(
                remote(
                    share_t.at[0, :, peer],
                    share_t.at[1, :, me],
                    xt_s.at[o],
                    xt_r.at[o],
                    {"ep": peer},
                )
            )
        for n in range(3):
            share_t[1, n, me] = share_t[0, n, me]
        return copies

    mate_wait(0, (0, 1))
    for n in range(3):
        loads[3 + n].wait()
    mate_wait(0, (2,))
    products_all(0)
    sha = shared_hidden()
    hidden(0)
    last = length - 1
    for p in range(1, length):
        two_sided = order[p][2]
        split = p == last and p > 1
        first = (0, 1) if split else (0, 1, 2)
        if p % 2 == 1 or p == 1:
            arrivals(p, first)
            if p + 1 < length:
                arrivals(p + 1, (0, 1, 2), order[p + 1][2] > 0)
        else:
            arrivals(p, first, two_sided < 1)
        mate_wait(p, (0, 1))
        selection(p)
        products(p, (0, 1))
        if split:
            slots(p - 1)
            for c in sha:
                c.wait_recv()
            xts = shared_shares()
            arrivals(p, (2,))
        mate_wait(p, (2,))
        products(p, (2,))
        if not split:
            slots(p - 1)
        hidden(p)
    if last <= 1:
        for c in sha:
            c.wait_recv()
        xts = shared_shares()
    shsum[...] = dot_t(shared_full(0), sg[...]) + dot_t(shared_full(1), su[...])
    slots(last)

    for c in xts:
        c.wait_recv()
    flat = [
        jnp.concatenate([share_t[1, n, j] for j in range(ep)], axis=1) for n in range(3)
    ]
    tok_flat = all_tok[...].reshape(ep * tok, dl)
    osg[...] = dot(flat[0], tok_flat)
    osu[...] = dot(flat[1], tok_flat)
    osd[...] = dot(flat[2], all_cot[...].reshape(ep * tok, dl))

    for p in range(length):
        for o in range(1, tp):
            pa_copies[p, 1, o].wait_recv()
        spread(p, 2, hh)

    own_meta = all_meta[chip, core]
    where_home = own_meta.T.astype(jnp.int32)
    hcol = lax.broadcasted_iota(jnp.int32, (tok, home), 1)
    lane_at = lax.broadcasted_iota(jnp.int32, (ep * 128, tok), 0)
    lanes = own_meta[6:8, :].astype(jnp.int32) + core * cap
    spots = [(lane_at == lanes[k : k + 1, :]).astype(F32).astype(BF) for k in range(2)]
    spots = jnp.concatenate(spots, axis=1)
    for o in range(1, ep):
        peer = (me + o) % ep
        copy_of(back.at[peer], back.at[peer], bk_s.at[0], bk_r.at[peer], {"ep": peer}).wait_recv()
        copy_of(dgb.at[peer], dgb.at[peer], bk_s.at[0], bk_r.at[ep + peer], {"ep": peer}).wait_recv()
    grad = shsum[...]
    for j in range(ep):
        g0 = (hcol == where_home[:, 4:5] - j * home).astype(F32)
        g1 = (hcol == where_home[:, 5:6] - j * home).astype(F32)
        grad = grad + dot((g0 + g1).astype(BF), back[j])
    gtok_out[...] = grad.astype(BF)
    dg = jnp.concatenate([dgb[j] for j in range(ep)], axis=1)
    high = dg.astype(BF)
    low = (dg - high.astype(F32)).astype(BF)
    gw = dot(high, spots) + dot(low, spots)
    gw_out[...] = jnp.concatenate([gw[0:1, :tok], gw[0:1, tok:]], axis=0)
    for cond, c in sends:
        if cond is None:
            c.wait_send()
        else:
            pl.when(cond)(c.wait_send)


def line_body(
    tokens,
    routes,
    route_weights,
    cotangent,
    expert_gate,
    expert_up,
    expert_down,
    shared_gate,
    shared_up,
    shared_down,
):
    tok, top = routes.shape
    dl = tokens.shape[1]
    ne, _, ff = expert_gate.shape
    sff = shared_gate.shape[1]
    ep, tp = lax.axis_size("ep"), lax.axis_size("tp")
    cap = max(2, 5 * tok * top // (4 * ep * ne))
    length = ep // CORES
    pair = CORES * cap
    rows = up_to(pair, 16)
    group = ne * pair
    home = ne * cap
    width, swidth, swid = ff // tp, sff // tp, sff // ep
    dims = (ep, tp, tok, dl, ne, ff, sff, cap, rows, width, swidth, swid)

    picked = routes.T.reshape(-1)
    earlier = jnp.arange(top * tok)[None, :] < jnp.arange(top * tok)[:, None]
    same = picked[:, None] == picked[None, :]
    ranked = jnp.sum((same & earlier).astype(jnp.int32), axis=1)
    code = (picked * rows + ranked).reshape(top, tok)
    place = ((picked // ne) * home + (picked % ne) * cap + ranked).reshape(top, tok)
    lane = ((picked // ne) * 128 + (picked % ne) * pair + ranked).reshape(top, tok)
    gate = route_weights.astype(BF).astype(F32).T
    meta = jnp.concatenate(
        [code.astype(F32), gate, place.astype(F32), lane.astype(F32)], axis=0
    )

    vm = pl.BlockSpec(memory_space=pltpu.VMEM)
    hbm = pl.BlockSpec(memory_space=pl.ANY)
    dma = pltpu.SemaphoreType.DMA
    scratch = [
        pltpu.VMEM((length, CORES, tok, dl), BF),
        pltpu.VMEM((length, CORES, tok, dl), BF),
        pltpu.VMEM((length, CORES, 8, tok), F32),
        pltpu.VMEM(expert_gate.shape, BF),
        pltpu.VMEM(expert_up.shape, BF),
        pltpu.VMEM(expert_down.shape, BF),
        pltpu.VMEM(shared_gate.shape, BF),
        pltpu.VMEM(shared_up.shape, BF),
        pltpu.VMEM(shared_down.shape, BF),
        pltpu.VMEM((length, group, 128), F32),
        pltpu.VMEM((tp, 3, tok, swidth), BF),
        pltpu.VMEM((tp, 3, tok, swidth), F32),
        pltpu.VMEM((tp, 3, tok, swidth), BF),
        pltpu.VMEM((tp, 3, tok, swidth), BF),
        pltpu.VMEM((2, 3, ep, swid, tok), BF),
        pltpu.VMEM((length, tp, 3, group, width), BF),
        pltpu.VMEM((length, tp, 3, group, width), F32),
        pltpu.VMEM((length, tp, 3, group, width), BF),
        pltpu.VMEM((length, tp, 3, group, width), BF),
        pltpu.VMEM((length, tp, 8, 128), F32),
        pltpu.VMEM((length, 8, 128), F32),
        pltpu.VMEM((ep, 8, 128), F32),
        pltpu.VMEM((length, CORES, home, dl), BF),
        pltpu.VMEM((ep, home, dl), BF),
        pltpu.VMEM((tok, dl), F32),
        dma((6,)),
        dma((3,)),
        dma((6,)),
        dma((3 * length,)),
        dma((3 * length,)),
        dma((3 * length,)),
        dma((3 * length,)),
        dma((tp,)),
        dma((tp,)),
        dma((tp,)),
        dma((tp,)),
        dma((2 * length * tp,)),
        dma((2 * length * tp,)),
        dma((3 * length * tp,)),
        dma((3 * length * tp,)),
        dma((ep,)),
        dma((ep,)),
        dma((2 * CORES * length,)),
        dma((2 * ep,)),
    ]
    sds = jax.ShapeDtypeStruct
    outs = pl.pallas_call(
        functools.partial(line_kernel, dims),
        out_shape=(
            sds((tok, dl), BF),
            sds((top, tok), F32),
            sds((swid, dl), F32),
            sds((swid, dl), F32),
            sds((swid, dl), F32),
            sds((ne, length * rows, dl), BF),
            sds((ne, length * rows, dl), BF),
            sds((ne, length * rows, ff), BF),
            sds((ne, length * rows, ff), BF),
            sds((ne, length * rows, ff), BF),
        ),
        in_specs=[hbm] * 9,
        out_specs=tuple([vm] * 10),
        scratch_shapes=scratch,
        compiler_params=pltpu.CompilerParams(
            collective_id=0, has_side_effects=True, vmem_limit_bytes=60 * 1024 * 1024
        ),
    )(
        meta,
        tokens,
        cotangent,
        expert_gate,
        expert_up,
        expert_down,
        shared_gate,
        shared_up,
        shared_down,
    )
    gtok, gw, osg, osu, osd, stok, scot, hg, hu, hh = outs
    grad_gate = jnp.einsum("esd,esf->edf", stok, hg, preferred_element_type=F32)
    grad_up = jnp.einsum("esd,esf->edf", stok, hu, preferred_element_type=F32)
    grad_down = jnp.einsum("esf,esd->efd", hh, scot, preferred_element_type=F32)
    return gtok, gw.T, grad_gate, grad_up, grad_down, osg.T, osu.T, osd


def body(tokens, routes, *rest):
    tok, top = routes.shape
    ne, _, ff = rest[2].shape
    sff = rest[5].shape[1]
    ep, tp = lax.axis_size("ep"), lax.axis_size("tp")
    cap = max(2, 5 * tok * top // (4 * ep * ne))
    lines = (
        ff == tp * 128
        and sff == tp * 128
        and ep % CORES == 0
        and (CORES * cap) % 8 == 0
        and (ne * cap) % 8 == 0
        and (ne * CORES * cap) % 16 == 0
        and ne * CORES * cap <= 128
    )
    return (line_body if lines else rows_body)(tokens, routes, *rest)


def solution(mesh):
    return jax.shard_map(
        body,
        mesh=mesh,
        in_specs=(
            P("ep", "tp"),
            P("ep", None),
            P("ep", None),
            P("ep", "tp"),
            P("ep", "tp", None),
            P("ep", "tp", None),
            P("ep", None, "tp"),
            P("tp", None),
            P("tp", None),
            P(None, "tp"),
        ),
        out_specs=(
            P("ep", "tp"),
            P("ep", None),
            P("ep", "tp", None),
            P("ep", "tp", None),
            P("ep", None, "tp"),
            P("tp", "ep"),
            P("tp", "ep"),
            P("ep", "tp"),
        ),
        check_vma=False,
    )
```

```python
import functools

import jax
import jax.numpy as jnp
from jax import lax
from jax.experimental import pallas as pl
from jax.experimental.pallas import tpu as pltpu
from jax.sharding import PartitionSpec as P

CORES = 2
BF = jnp.bfloat16
F32 = jnp.float32


def up_to(value, unit):
    return -(-value // unit) * unit


def dot(a, b):
    return jnp.dot(a, b, preferred_element_type=F32)


def dot_t(a, b):
    return lax.dot_general(a, b, (((1,), (1,)), ((), ())), preferred_element_type=F32)


def hidden_terms(gate_pre, up_pre, back_grad, scaling):
    logistic = jax.nn.sigmoid(gate_pre)
    silu = gate_pre * logistic
    product = silu * up_pre
    grad_act = back_grad if scaling is None else scaling * back_grad
    gate_grad = grad_act * up_pre * logistic * (1.0 + gate_pre * (1.0 - logistic))
    hidden = product if scaling is None else scaling * product
    return (
        gate_grad.astype(BF),
        (grad_act * silu).astype(BF),
        hidden.astype(BF),
        jnp.sum(back_grad * product, axis=-1, keepdims=True),
    )


def ring_plan(length):
    plan = []
    for step in range(1, length // 2 + 1):
        last_even = length % 2 == 0 and step == length // 2
        plan.append((step, 0, (0,) if last_even else (0, 1)))
        plan.append((step, 1, (1,) if last_even else (1, 0)))
    return plan


def rows_kernel(
    dims,
    meta_in,
    tok_in,
    cot_in,
    eg_in,
    eu_in,
    ed_in,
    sg_in,
    su_in,
    sd_in,
    gtok_out,
    gw_out,
    osg,
    osu,
    osd,
    stok,
    scot,
    hg,
    hu,
    hh,
    all_tok,
    all_cot,
    all_meta,
    eg,
    eu,
    ed,
    sg,
    su,
    sd,
    sel,
    gates,
    sh_part,
    sh_recv,
    sh_all,
    share_t,
    part,
    exact,
    recv,
    dgs,
    back_send,
    back,
    shsum,
    load_sem,
    own_sem,
    ring_s,
    ring_r,
    mate_s,
    mate_r,
    shr_s,
    shr_r,
    sha_s,
    sha_r,
    pr_s,
    pr_r,
    pa_s,
    pa_r,
    xt_s,
    xt_r,
    bk_s,
    bk_r,
):
    ep, tp, tok, dl, ne, ff, sff, cap, re, rows, rpp, rpt, cp, swid = dims
    me = lax.axis_index("ep")
    mt = lax.axis_index("tp")
    length = ep // CORES
    chip = me // CORES
    core = me % CORES
    mate = chip * CORES + (1 - core)
    nxt = ((chip + 1) % length) * CORES + core
    prv = ((chip + length - 1) % length) * CORES + core

    owns = []
    for n, (src, dst) in enumerate(((tok_in, all_tok), (cot_in, all_cot), (meta_in, all_meta))):
        c = pltpu.make_async_copy(src, dst.at[me], own_sem.at[n])
        c.start()
        owns.append(c)
    loads = []
    for n, (src, dst) in enumerate(
        ((sg_in, sg), (su_in, su), (sd_in, sd), (eg_in, eg), (eu_in, eu), (ed_in, ed))
    ):
        c = pltpu.make_async_copy(src, dst, load_sem.at[n])
        c.start()
        loads.append(c)

    barrier = pltpu.get_barrier_semaphore()
    for o in range(1, ep):
        pl.semaphore_signal(barrier, inc=1, device_id={"ep": (me + o) % ep})
    for o in range(1, tp):
        pl.semaphore_signal(barrier, inc=1, device_id={"tp": (mt + o) % tp})
    pl.semaphore_wait(barrier, ep + tp - 2)

    sends = []

    def remote(src, dst, ssem, rsem, dev):
        c = pltpu.make_async_remote_copy(
            src_ref=src, dst_ref=dst, send_sem=ssem, recv_sem=rsem, device_id=dev
        )
        c.start()
        sends.append(c)
        return c

    bufs = (all_tok, all_cot, all_meta)
    ring_copies = {}
    mate_copies = []
    plan = {(step, d): items for step, d, items in ring_plan(length)}

    def ring_send(step, d, item, src):
        dest = nxt if d == 0 else prv
        subs = (0, 2) if item == 0 else (1,)
        for b in subs:
            n = ((step - 1) * 2 + d) * 3 + b
            ring_copies[step, d, b] = remote(
                bufs[b].at[src], bufs[b].at[src], ring_s.at[n], ring_r.at[n], {"ep": dest}
            )

    def mate_send(item, src):
        for b in (0, 2) if item == 0 else (1,):
            n = len(mate_copies)
            mate_copies.append(
                remote(
                    bufs[b].at[src], bufs[b].at[src], mate_s.at[n], mate_r.at[n], {"ep": mate}
                )
            )

    for c in owns:
        c.wait()
    for pos in range(2):
        for d in range(2):
            items = plan.get((1, d), ())
            if pos < len(items):
                ring_send(1, d, items[pos], me)
    mate_send(0, me)
    mate_send(1, me)

    tp_order = [(mt + o) % tp for o in range(1, tp)]
    if rpt * tp > tok:
        sh_part[:, tok:, :] = jnp.zeros((3, rpt * tp - tok, sff), BF)
    for n in range(3):
        loads[n].wait()
        if n < 2:
            val = dot(all_tok[me], (sg, su)[n][...])
        else:
            val = dot_t(all_cot[me], sd[...])
        sh_part[n, :tok, :] = val.astype(BF)
    sh_copies = []
    for o in range(1, tp):
        peer = tp_order[o - 1]
        sh_copies.append(
            remote(
                sh_part.at[:, pl.ds(pl.multiple_of(peer * rpt, 16), rpt), :],
                sh_recv.at[o],
                shr_s.at[o],
                shr_r.at[o],
                {"tp": peer},
            )
        )

    def ring_arrivals(step):
        for pos in range(2):
            for d in range(2):
                items = plan.get((step, d), ())
                if pos >= len(items):
                    continue
                item = items[pos]
                away = length - step if d == 0 else step
                src = ((chip + away) % length) * CORES + core
                for b in (0, 2) if item == 0 else (1,):
                    ring_copies[step, d, b].wait_recv()
                if item in plan.get((step + 1, d), ()):
                    ring_send(step + 1, d, item, src)
                mate_send(item, src)

    if length > 1:
        ring_arrivals(1)

    for c in sh_copies:
        c.wait_recv()
    mine_t = pl.ds(pl.multiple_of(mt * rpt, 16), rpt)
    tot = [sh_part[n, mine_t, :].astype(F32) for n in range(3)]
    for o in range(1, tp):
        for n in range(3):
            tot[n] = tot[n] + sh_recv[o, n].astype(F32)
    a, b, c3, _ = hidden_terms(tot[0], tot[1], tot[2], None)
    sh_all[0, mine_t, :] = a
    sh_all[1, mine_t, :] = b
    sh_all[2, mine_t, :] = c3
    sha = []
    for o in range(1, tp):
        sha.append(
            remote(
                sh_all.at[:, mine_t, :],
                sh_all.at[:, mine_t, :],
                sha_s.at[o],
                sha_r.at[o],
                {"tp": tp_order[o - 1]},
            )
        )

    for step in range(2, length // 2 + 1):
        ring_arrivals(step)
    for c in mate_copies:
        c.wait_recv()

    row_id = lax.broadcasted_iota(jnp.int32, (rows, tok), 0)
    gate = jnp.zeros((rows, 1), F32)
    for j in range(ep):
        m = all_meta[j]
        code = m[0:2, :].astype(jnp.int32) + (j * cap - me * (ne * re))
        p0 = (row_id == code[0:1, :]).astype(F32)
        p1 = (row_id == code[1:2, :]).astype(F32)
        sel[:, j * tok : (j + 1) * tok] = (p0 + p1).astype(BF)
        gate = gate + jnp.sum(p0 * m[2:3, :] + p1 * m[3:4, :], axis=1, keepdims=True)
    te = rpp * tp
    for e in range(ne):
        gates[e, :re, :] = jnp.broadcast_to(gate[e * re : (e + 1) * re, :], (re, 128))
        if te > re:
            gates[e, re:, :] = jnp.zeros((te - re, 128), F32)
            part[e, :, re:, :] = jnp.zeros((3, te - re, ff), BF)
            exact[e, :, re:, :] = jnp.zeros((3, te - re, ff), F32)

    stok[...] = dot(sel[...], all_tok[...].reshape(ep * tok, dl)).astype(BF)
    scot[...] = dot(sel[...], all_cot[...].reshape(ep * tok, dl)).astype(BF)
    for n in range(3):
        loads[3 + n].wait()
    p_copies = [[] for _ in range(ne)]
    for e in range(ne):
        for n in range(3):
            r = slice(e * re, (e + 1) * re)
            val = dot_t(scot[r, :], ed[e]) if n == 2 else dot(stok[r, :], (eg, eu)[n][e])
            exact[e, n, :re, :] = val
            part[e, n, :re, :] = val.astype(BF)
            for o in range(1, tp):
                peer = tp_order[o - 1]
                k = (e * 3 + n) * tp + o
                p_copies[e].append(
                    remote(
                        part.at[e, n, pl.ds(pl.multiple_of(peer * rpp, 8), rpp), :],
                        recv.at[o, e, n],
                        pr_s.at[k],
                        pr_r.at[k],
                        {"tp": peer},
                    )
                )

    for c in sha:
        c.wait_recv()
    for n in range(3):
        back_t = sh_all[n, :tok, :].astype(F32).T.astype(BF)
        for j in range(ep):
            share_t[0, n, j] = back_t[j * swid : (j + 1) * swid, :]
    xts = []
    for o in range(1, ep):
        peer = (me + o) % ep
        xts.append(
            remote(
                share_t.at[0, :, peer],
                share_t.at[1, :, me],
                xt_s.at[o],
                xt_r.at[o],
                {"ep": peer},
            )
        )
    for n in range(3):
        share_t[1, n, me] = share_t[0, n, me]
    mine = pl.ds(pl.multiple_of(mt * rpp, 8), rpp)
    lane = lax.broadcasted_iota(jnp.int32, (rpp, 128), 1)
    pas = []
    for e in range(ne):
        for c in p_copies[e]:
            c.wait_recv()
        tot = [exact[e, n, mine, :] for n in range(3)]
        for o in range(1, tp):
            for n in range(3):
                tot[n] = tot[n] + recv[o, e, n].astype(F32)
        a, b, c3, dg = hidden_terms(tot[0], tot[1], tot[2], gates[e, mine, :][:, 0:1])
        hg[e, mine, :] = a
        hu[e, mine, :] = b
        hh[e, mine, :] = c3
        high = dg.astype(BF).astype(F32)
        dgs[e, mine, :] = jnp.where(
            lane == 0, high, jnp.where(lane == 1, dg - high, 0.0)
        ).astype(BF)
        group = []
        for k, buf in enumerate((hg, hu, dgs, hh)):
            for o in range(1, tp):
                n = (e * 4 + k) * tp + o
                group.append(
                    remote(
                        buf.at[e, mine, :],
                        buf.at[e, mine, :],
                        pa_s.at[n],
                        pa_r.at[n],
                        {"tp": tp_order[o - 1]},
                    )
                )
        pas.append(group)

    col = lax.broadcasted_iota(jnp.int32, (8, re), 1)
    block = jnp.zeros((8, re), jnp.int32)
    for j in range(1, ep):
        block = block + (col >= j * cap).astype(jnp.int32)
    target = block * cp + (col - block * cap)
    target = jnp.where(col < ep * cap, target, -1)
    pick = (
        (lax.broadcasted_iota(jnp.int32, (ep * cp, re), 0) == target[0:1, :])
        .astype(F32)
        .astype(BF)
    )
    bks = []
    for e in range(ne):
        for c in pas[e][: 3 * (tp - 1)]:
            c.wait_recv()
        slot = (dot_t(hg[e, :re, :], eg[e]) + dot_t(hu[e, :re, :], eu[e])).astype(BF)
        back_send[e, :, :, :dl] = dot(pick, slot).astype(BF).reshape(ep, cp, dl)
        back_send[e, :, :, dl:] = dot(pick, dgs[e, :re, :]).astype(BF).reshape(ep, cp, 128)
        for o in range(1, ep):
            peer = (me + o) % ep
            bks.append(
                remote(
                    back_send.at[e, peer],
                    back.at[e, me],
                    bk_s.at[e * ep + o],
                    bk_r.at[e * ep + o],
                    {"ep": peer},
                )
            )
        back[e, me] = back_send[e, me]

    shsum[...] = dot_t(sh_all[0, :tok, :], sg[...]) + dot_t(sh_all[1, :tok, :], su[...])
    for c in xts:
        c.wait_recv()
    flat = [
        jnp.concatenate([share_t[1, n, j] for j in range(ep)], axis=1) for n in range(3)
    ]
    tok_flat = all_tok[...].reshape(ep * tok, dl)
    osg[...] = dot(flat[0], tok_flat)
    osu[...] = dot(flat[1], tok_flat)
    osd[...] = dot(flat[2], all_cot[...].reshape(ep * tok, dl))

    width = ne * ep * cp
    home = all_meta[me].T.astype(jnp.int32)
    hcol = lax.broadcasted_iota(jnp.int32, (tok, width), 1)
    g0 = (hcol == home[:, 4:5]).astype(F32)
    g1 = (hcol == home[:, 5:6]).astype(F32)
    both = (g0 + g1).astype(BF)
    for c in bks:
        c.wait_recv()
    flat_back = back[...].reshape(width, dl + 128)
    gtok_out[...] = (dot(both, flat_back[:, :dl]) + shsum[...]).astype(BF)
    w0 = jnp.sum(dot(g0.astype(BF), flat_back[:, dl:]), axis=1, keepdims=True)
    w1 = jnp.sum(dot(g1.astype(BF), flat_back[:, dl:]), axis=1, keepdims=True)
    wl = lax.broadcasted_iota(jnp.int32, (tok, 128), 1)
    gw_out[...] = jnp.where(wl == 0, w0, w1).T[0:2, :]
    for group in pas:
        for c in group[3 * (tp - 1) :]:
            c.wait_recv()
    for c in sends:
        c.wait_send()


def rows_body(
    tokens,
    routes,
    route_weights,
    cotangent,
    expert_gate,
    expert_up,
    expert_down,
    shared_gate,
    shared_up,
    shared_down,
):
    tok, top = routes.shape
    dl = tokens.shape[1]
    ne, _, ff = expert_gate.shape
    sff = shared_gate.shape[1]
    ep, tp = lax.axis_size("ep"), lax.axis_size("tp")
    cap = max(2, 5 * tok * top // (4 * ep * ne))
    re = up_to(ep * cap, 16)
    rows = ne * re
    rpp = up_to(-(-re // tp), 8)
    rpt = up_to(-(-tok // tp), 16)
    cp = up_to(cap, 8)
    swid = sff // ep
    length = ep // CORES
    total = rpp * tp
    dims = (ep, tp, tok, dl, ne, ff, sff, cap, re, rows, rpp, rpt, cp, swid)

    picked = routes.T.reshape(-1)
    earlier = jnp.arange(top * tok)[None, :] < jnp.arange(top * tok)[:, None]
    same = picked[:, None] == picked[None, :]
    ranked = jnp.sum((same & earlier).astype(jnp.int32), axis=1)
    code = (picked * re + ranked).reshape(top, tok)
    home = (((picked % ne) * ep + picked // ne) * cp + ranked).reshape(top, tok)
    gate = route_weights.astype(BF).astype(F32).T
    meta = jnp.concatenate(
        [code.astype(F32), gate, home.astype(F32), jnp.zeros((8 - 3 * top, tok), F32)], axis=0
    )

    vm = pl.BlockSpec(memory_space=pltpu.VMEM)
    hbm = pl.BlockSpec(memory_space=pl.ANY)
    dma = pltpu.SemaphoreType.DMA
    n_ring = max(1, (length // 2) * 6)
    scratch = [
        pltpu.VMEM((ep, tok, dl), BF),
        pltpu.VMEM((ep, tok, dl), BF),
        pltpu.VMEM((ep, 8, tok), F32),
        pltpu.VMEM(expert_gate.shape, BF),
        pltpu.VMEM(expert_up.shape, BF),
        pltpu.VMEM(expert_down.shape, BF),
        pltpu.VMEM(shared_gate.shape, BF),
        pltpu.VMEM(shared_up.shape, BF),
        pltpu.VMEM(shared_down.shape, BF),
        pltpu.VMEM((rows, ep * tok), BF),
        pltpu.VMEM((ne, total, 128), F32),
        pltpu.VMEM((3, rpt * tp, sff), BF),
        pltpu.VMEM((tp, 3, rpt, sff), BF),
        pltpu.VMEM((3, rpt * tp, sff), BF),
        pltpu.VMEM((2, 3, ep, swid, tok), BF),
        pltpu.VMEM((ne, 3, total, ff), BF),
        pltpu.VMEM((ne, 3, total, ff), F32),
        pltpu.VMEM((tp, ne, 3, rpp, ff), BF),
        pltpu.VMEM((ne, total, 128), BF),
        pltpu.VMEM((ne, ep, cp, dl + 128), BF),
        pltpu.VMEM((ne, ep, cp, dl + 128), BF),
        pltpu.VMEM((tok, dl), F32),
        dma((6,)),
        dma((3,)),
        dma((n_ring,)),
        dma((n_ring,)),
        dma((3 * length,)),
        dma((3 * length,)),
        dma((tp,)),
        dma((tp,)),
        dma((tp,)),
        dma((tp,)),
        dma((3 * ne * tp,)),
        dma((3 * ne * tp,)),
        dma((4 * ne * tp,)),
        dma((4 * ne * tp,)),
        dma((ep,)),
        dma((ep,)),
        dma((ne * ep,)),
        dma((ne * ep,)),
    ]
    sds = jax.ShapeDtypeStruct
    outs = pl.pallas_call(
        functools.partial(rows_kernel, dims),
        out_shape=(
            sds((tok, dl), BF),
            sds((top, tok), F32),
            sds((swid, dl), F32),
            sds((swid, dl), F32),
            sds((swid, dl), F32),
            sds((rows, dl), BF),
            sds((rows, dl), BF),
            sds((ne, total, ff), BF),
            sds((ne, total, ff), BF),
            sds((ne, total, ff), BF),
        ),
        in_specs=[hbm] * 9,
        out_specs=tuple([vm] * 10),
        scratch_shapes=scratch,
        compiler_params=pltpu.CompilerParams(
            collective_id=0, has_side_effects=True, vmem_limit_bytes=60 * 1024 * 1024
        ),
    )(
        meta,
        tokens,
        cotangent,
        expert_gate,
        expert_up,
        expert_down,
        shared_gate,
        shared_up,
        shared_down,
    )
    gtok, gw, osg, osu, osd, stok, scot, hg, hu, hh = outs
    stok = stok.reshape(ne, re, dl)
    scot = scot.reshape(ne, re, dl)
    hg, hu, hh = (h[:, :re] for h in (hg, hu, hh))
    grad_gate = jnp.einsum("esd,esf->edf", stok, hg, preferred_element_type=F32)
    grad_up = jnp.einsum("esd,esf->edf", stok, hu, preferred_element_type=F32)
    grad_down = jnp.einsum("esf,esd->efd", hh, scot, preferred_element_type=F32)
    return gtok, gw.T, grad_gate, grad_up, grad_down, osg.T, osu.T, osd


def line_order(chip, length):
    high = (2 * chip) // length
    far = 1 - 2 * high
    edge = chip * (1 - high) + (length - 1 - chip) * high
    order = [(chip, None, None)]
    for p in range(1, length):
        two_sided = (2 * edge - p + 2 * length) // (2 * length)
        dist = two_sided * ((p + 1) // 2) + (1 - two_sided) * (p - edge)
        toward = far * (1 - 2 * two_sided * (p % 2))
        order.append((chip + toward * dist, chip - toward, two_sided))
    return order


def line_kernel(
    dims,
    routes_in,
    weights_in,
    tok_in,
    cot_in,
    eg_in,
    eu_in,
    ed_in,
    sg_in,
    su_in,
    sd_in,
    gtok_out,
    gw_out,
    osg_out,
    osu_out,
    osd_out,
    stok_out,
    scot_out,
    hg_out,
    hu_out,
    hh_out,
    routes,
    weights,
    gtok,
    gw,
    osg,
    osu,
    osd,
    stok,
    scot,
    hg,
    hu,
    hh,
    all_tok,
    all_cot,
    all_meta,
    eg,
    eu,
    ed,
    sg,
    su,
    sd,
    gates,
    sh_part,
    sh_exact,
    sh_recv,
    sh_all,
    share_t,
    part,
    exact,
    recv,
    hs,
    dgp,
    dgs,
    dgb,
    back_send,
    back,
    shsum,
    load_sem,
    own_sem,
    out_sem,
    own_s,
    line_s,
    line_r,
    mate_s,
    mate_r,
    shr_s,
    shr_r,
    sha_s,
    sha_r,
    pr_s,
    pr_r,
    pa_s,
    pa_r,
    xt_s,
    xt_r,
    xy_s,
    xy_r,
    bk_s,
    bk_r,
):
    ep, tp, tok, dl, ne, ff, sff, cap, rows, width, swidth, swid = dims
    me = lax.axis_index("ep")
    mt = lax.axis_index("tp")
    length = ep // CORES
    chip = me // CORES
    core = me % CORES
    mate = chip * CORES + (1 - core)
    pair = CORES * cap
    group = ne * pair
    home = ne * cap
    part_rows = swid // tp
    order = line_order(chip, length)
    bufs = (all_tok, all_meta, all_cot)

    owns = []
    for n, (src, dst) in enumerate(
        (
            (tok_in, all_tok.at[chip, core]),
            (cot_in, all_cot.at[chip, core]),
            (routes_in, routes),
            (weights_in, weights),
        )
    ):
        c = pltpu.make_async_copy(src, dst, own_sem.at[n])
        c.start()
        owns.append(c)
    loads = []
    for n, (src, dst) in enumerate(
        ((sg_in, sg), (su_in, su), (sd_in, sd), (eg_in, eg), (eu_in, eu), (ed_in, ed))
    ):
        c = pltpu.make_async_copy(src, dst, load_sem.at[n])
        c.start()
        loads.append(c)

    barrier = pltpu.get_barrier_semaphore()
    def greet(there):
        pl.semaphore_signal(barrier, inc=1, device_id={"ep": there * CORES + core})

    pl.semaphore_signal(barrier, inc=1, device_id={"ep": mate})
    for o in range(1, tp):
        pl.semaphore_signal(barrier, inc=1, device_id={"tp": (mt + o) % tp})
    pl.when(chip < length - 1)(lambda: greet(chip + 1))
    pl.when(chip > 0)(lambda: greet(chip - 1))
    above = (2 * length - 2 - chip) // length
    below = (chip + length - 1) // length

    pl.semaphore_wait(barrier, tp + above + below)

    sends = []

    def copy_of(src, dst, ssem, rsem, dev):
        return pltpu.make_async_remote_copy(
            src_ref=src, dst_ref=dst, send_sem=ssem, recv_sem=rsem, device_id=dev
        )

    def remote(src, dst, ssem, rsem, dev):
        c = copy_of(src, dst, ssem, rsem, dev)
        c.start()
        sends.append((None, c))
        return c

    def along_line(b, src, ssem, there):
        block = bufs[b].at[src, core]
        dest = ((there + length) % length) * CORES + core
        return copy_of(block, block, ssem, line_r.at[b * length + src], {"ep": dest})

    def to_mate(b, p):
        block = bufs[b].at[order[p][0], core]
        n = b * length + p
        return copy_of(block, block, mate_s.at[n], mate_r.at[n], {"ep": mate})

    def send_own(b):
        for d, there in enumerate((chip + 1, chip - 1)):
            c = along_line(b, chip, own_s.at[2 * b + d], there)
            inside = chip < length - 1 if d == 0 else chip > 0
            pl.when(inside)(c.start)
            sends.append((inside, c))

    def send_mate(b):
        c = to_mate(b, 0)
        c.start()
        sends.append((None, c))

    owns[0].wait()
    send_own(0)
    send_mate(0)
    owns[1].wait()
    send_mate(2)

    owns[2].wait()
    owns[3].wait()
    table = jnp.concatenate(
        [
            routes[...].astype(F32),
            weights[...].astype(BF).astype(F32),
            jnp.zeros((4, tok), F32),
        ],
        axis=0,
    )
    picked = table.T
    earlier = lax.broadcasted_iota(jnp.int32, (tok, tok), 0) < lax.broadcasted_iota(
        jnp.int32, (tok, tok), 1
    )

    def count(hits):
        return jnp.sum(hits.astype(F32), axis=0, keepdims=True)

    first, second = picked[:, 0:1], picked[:, 1:2]
    ranks = [
        count((first == table[0:1]) & earlier),
        count((second == table[1:2]) & earlier) + count(first == table[1:2]),
    ]
    ranked = jnp.concatenate(ranks, axis=0)
    named = table[0:2]
    owner = jnp.floor((named + 0.5) * (1.0 / ne))
    which = named - owner * ne
    all_meta[chip, core] = jnp.concatenate(
        [
            named * rows + ranked,
            table[2:4],
            owner * home + which * cap + ranked,
            owner * 128 + which * pair + ranked,
        ],
        axis=0,
    )
    send_own(1)
    send_mate(1)

    relays = {}
    mates = {}
    for p in range(1, length):
        src, there, _ = order[p]
        for b in range(3):
            relays[b, p] = along_line(b, src, line_s.at[b * length + p], there)
            mates[b, p] = to_mate(b, p)
            if p < length - 1 or b < 2:
                sends.append(((there >= 0) & (there < length), relays[b, p]))
            sends.append((None, mates[b, p]))

    def arrivals(p, which, cond=None):
        def run():
            _, there, _ = order[p]
            for b in which:
                relays[b, p].wait_recv()
                pl.when((there >= 0) & (there < length))(relays[b, p].start)
                mates[b, p].start()

        if cond is None:
            run()
        else:
            pl.when(cond)(run)

    def mate_wait(p, which):
        for b in which:
            to_mate(b, p).wait_recv()

    peers = [(mt + o) % tp for o in range(1, tp)]
    inner = chip * (length - 1 - chip) > 0
    outer = chip * (length - 1 - chip) < 1

    own_tok = all_tok[chip, core]
    own_cot = all_cot[chip, core]
    for n in range(3):
        loads[n].wait()
        val = dot(own_tok, (sg, su)[n][...]) if n < 2 else dot_t(own_cot, sd[...])
        for q in range(tp):
            piece = val[:, q * swidth : (q + 1) * swidth]
            sh_exact[q, n] = piece
            sh_part[q, n] = piece.astype(BF)
    sh_copies = []
    for o in range(1, tp):
        sh_copies.append(
            remote(
                sh_part.at[peers[o - 1]],
                sh_recv.at[o],
                shr_s.at[o],
                shr_r.at[o],
                {"tp": peers[o - 1]},
            )
        )

    row_id = lax.broadcasted_iota(jnp.int32, (ne * rows, tok), 0)
    sels = {}
    pr_copies = {}

    def selection(p):
        src = order[p][0]
        halves = []
        gate = jnp.zeros((ne * rows, 1), F32)
        for jj in range(CORES):
            m = all_meta[src, jj]
            code = m[0:2, :].astype(jnp.int32) + (jj * cap - me * (ne * rows))
            p0 = (row_id == code[0:1, :]).astype(F32)
            p1 = (row_id == code[1:2, :]).astype(F32)
            halves.append((p0 + p1).astype(BF))
            gate = gate + jnp.sum(p0 * m[2:3, :] + p1 * m[3:4, :], axis=1, keepdims=True)
        sels[p] = jnp.concatenate(halves, axis=1)
        gate = jnp.concatenate([gate[e * rows : e * rows + pair] for e in range(ne)], axis=0)
        gates[p] = jnp.broadcast_to(gate, (group, 128))

    def products(p, which):
        src = order[p][0]
        buf, out = (all_cot, scot) if which == (2,) else (all_tok, stok)
        picked = dot(sels[p], buf[src].reshape(CORES * tok, dl)).astype(BF)
        for e in range(ne):
            out[e, p * rows : (p + 1) * rows, :] = picked[e * rows : (e + 1) * rows]
        for n in which:
            vals = []
            for e in range(ne):
                x = picked[e * rows : (e + 1) * rows]
                val = dot_t(x, ed[e]) if n == 2 else dot(x, (eg, eu)[n][e])
                vals.append(val[:pair])
            val = jnp.concatenate(vals, axis=0)
            for q in range(tp):
                piece = val[:, q * width : (q + 1) * width]
                exact[p, q, n] = piece
                part[p, q, n] = piece.astype(BF)
        half = 1 if which == (2,) else 0
        span = pl.ds(which[0], len(which))
        for o in range(1, tp):
            k = (p * 2 + half) * tp + o
            pr_copies[p, half, o] = remote(
                part.at[p, peers[o - 1], span],
                recv.at[p, o, span],
                pr_s.at[k],
                pr_r.at[k],
                {"tp": peers[o - 1]},
            )

    def products_all(p):
        selection(p)
        products(p, (0, 1))
        products(p, (2,))

    pa_copies = {}

    def send_hidden(p, piece):
        for o in range(1, tp):
            k = (p * 3 + piece) * tp + o
            if piece < 2:
                block = hs.at[p, mt, pl.ds(2 * piece, 2 - piece)]
            else:
                block = dgp.at[p, mt]
            pa_copies[p, piece, o] = remote(
                block, block, pa_s.at[k], pa_r.at[k], {"tp": peers[o - 1]}
            )

    def hidden(p):
        for half in range(2):
            for o in range(1, tp):
                pr_copies[p, half, o].wait_recv()
        tot = [exact[p, mt, n] for n in range(3)]
        for o in range(1, tp):
            for n in range(3):
                tot[n] = tot[n] + recv[p, o, n].astype(F32)
        gate = gates[p][:, 0:1]
        logistic = jax.nn.sigmoid(tot[0])
        silu = tot[0] * logistic
        product = silu * tot[1]
        grad_act = gate * tot[2]
        hs[p, mt, 0] = (
            grad_act * tot[1] * logistic * (1.0 + tot[0] * (1.0 - logistic))
        ).astype(BF)
        hs[p, mt, 1] = (grad_act * silu).astype(BF)
        hs[p, mt, 2] = (gate * product).astype(BF)
        terms = tot[2] * product
        fill = jnp.zeros((128 - group, width), F32)
        cols = jnp.concatenate([terms, fill], axis=0).T
        dgp[p, mt] = jnp.broadcast_to(jnp.sum(cols, axis=0, keepdims=True), (8, 128))
        for piece in (2, 0) if p == length - 1 else (2, 0, 1):
            send_hidden(p, piece)

    def pick_rows():
        at = lax.broadcasted_iota(jnp.int32, (group, group), 0)
        col = lax.broadcasted_iota(jnp.int32, (group, group), 1)
        wanted = at * 0
        for jj in range(CORES):
            for e in range(ne):
                low = jj * home + e * cap
                inside = (at >= low) & (at < low + cap)
                wanted = jnp.where(inside, at - low + e * pair + jj * cap, wanted)
        return (col == wanted).astype(F32).astype(BF)

    pick = pick_rows()
    held = []

    def give(c, hold):
        sends.append((None, c))
        if hold:
            pl.when(outer)(c.start)
            held.append(c)
        else:
            c.start()

    def give_held():
        for c in held:
            c.start()

    def spread(p, n, out):
        full = jnp.concatenate([hs[p, q, n] for q in range(tp)], axis=1).astype(F32)
        fill = jnp.zeros((rows - pair, ff), F32)
        blocks = []
        for e in range(ne):
            block = full[e * pair : (e + 1) * pair]
            if rows > pair:
                block = jnp.concatenate([block, fill], axis=0)
            block = block.astype(BF)
            out[e, p * rows : (p + 1) * rows, :] = block
            blocks.append(block)
        return blocks

    def slots(p):
        src = order[p][0]
        for o in range(1, tp):
            pa_copies[p, 0, o].wait_recv()
        if p == length - 1:
            send_hidden(p, 1)
            share_columns()
        a = spread(p, 0, hg)
        b = spread(p, 1, hu)
        vals = [(dot_t(a[e], eg[e]) + dot_t(b[e], eu[e]))[:pair] for e in range(ne)]
        slot = jnp.concatenate(vals, axis=0).astype(BF)
        moved = dot(pick, slot)
        for jj in range(CORES):
            back_send[p, jj] = moved[jj * home : (jj + 1) * home].astype(BF)
        for o in range(1, tp):
            pa_copies[p, 2, o].wait_recv()
        total = dgp[p, 0]
        for q in range(1, tp):
            total = total + dgp[p, q]
        dgs[p] = total
        if p == 0:
            back[me] = back_send[0, core]
            dgb[me] = total
            targets = [(1 - core, mate)]
        else:
            targets = [(jj, src * CORES + jj) for jj in range(CORES)]
        for n, (jj, dest) in enumerate(targets):
            k = p * CORES + n
            for c in (
                copy_of(back_send.at[p, jj], back.at[me], bk_s.at[2 * k], bk_r.at[me], {"ep": dest}),
                copy_of(dgs.at[p], dgb.at[me], bk_s.at[2 * k + 1], bk_r.at[ep + me], {"ep": dest}),
            ):
                give(c, p == 1)

    def shared_hidden():
        for c in sh_copies:
            c.wait_recv()
        tot = [sh_exact[mt, n] for n in range(3)]
        for o in range(1, tp):
            for n in range(3):
                tot[n] = tot[n] + sh_recv[o, n].astype(F32)
        a, b, c3, _ = hidden_terms(tot[0], tot[1], tot[2], None)
        sh_all[mt, 0] = a
        sh_all[mt, 1] = b
        sh_all[mt, 2] = c3
        return [
            remote(sh_all.at[mt], sh_all.at[mt], sha_s.at[o], sha_r.at[o], {"tp": peers[o - 1]})
            for o in range(1, tp)
        ]

    spread_out = []

    def share_columns():
        for c in xts:
            c.wait_recv()
        for o in range(1, tp):
            block = share_t.at[1, :, :, mt]
            spread_out.append(
                remote(block, block, xy_s.at[o], xy_r.at[o], {"tp": peers[o - 1]})
            )

    def shared_full(n):
        return jnp.concatenate([sh_all[q, n] for q in range(tp)], axis=1)

    def shared_shares():
        for n in range(3):
            back_t = shared_full(n).astype(F32).T.astype(BF)
            for j in range(ep):
                for q in range(tp):
                    low = j * swid + q * part_rows
                    share_t[0, n, j, q] = back_t[low : low + part_rows, :]
        copies = []
        for o in range(1, ep):
            peer = (me + o) % ep
            c = copy_of(
                share_t.at[0, :, peer, mt],
                share_t.at[1, :, me, mt],
                xt_s.at[o],
                xt_r.at[o],
                {"ep": peer},
            )
            give(c, True)
            copies.append(c)
        for n in range(3):
            share_t[1, n, me, mt] = share_t[0, n, me, mt]
        return copies

    def homeward(p):
        src = order[p][0]
        for jj in range(CORES):
            if p == 0:
                j = me if jj == 0 else mate
            else:
                j = src * CORES + jj
            if p > 0 or jj > 0:
                copy_of(back.at[j], back.at[j], bk_s.at[0], bk_r.at[j], {"ep": j}).wait_recv()
                copy_of(dgb.at[j], dgb.at[j], bk_s.at[0], bk_r.at[ep + j], {"ep": j}).wait_recv()
            g0 = (hcol == where_home[:, 4:5] - j * home).astype(F32)
            g1 = (hcol == where_home[:, 5:6] - j * home).astype(F32)
            shsum[...] += dot((g0 + g1).astype(BF), back[j])

    outs = []

    def put(src, dst):
        c = pltpu.make_async_copy(src, dst, out_sem.at[len(outs)])
        c.start()
        outs.append(c)

    def hidden_rows(p):
        for o in range(1, tp):
            pa_copies[p, 1, o].wait_recv()
        spread(p, 2, hh)

    def first_arrivals(which):
        if length > 1:
            arrivals(1, which)
        if length > 2:
            arrivals(2, which, order[2][2] > 0)

    mate_wait(0, (0, 1))
    for n in range(3):
        loads[3 + n].wait()
    mate_wait(0, (2,))
    products_all(0)
    send_own(2)
    sha = shared_hidden()
    first_arrivals((0, 1))
    hidden(0)
    last = length - 1
    for p in range(1, length):
        split = p == last
        if p == 1:
            first_arrivals((2,))
        elif not split:
            far = order[p][2] < 1 if p % 2 == 0 or p == last else None
            arrivals(p, (0, 1, 2), far)
            if p % 2 == 1 and p + 1 < last:
                arrivals(p + 1, (0, 1, 2), order[p + 1][2] > 0)
        else:
            arrivals(p, (0, 1), outer)
        mate_wait(p, (0, 1))
        selection(p)
        products(p, (0, 1))
        if split:
            for c in sha:
                c.wait_recv()
            xts = shared_shares()
            arrivals(p, (2,), outer)
        mate_wait(p, (2,))
        products(p, (2,))
        if p + 1 == last and last > 2:
            arrivals(last, (2,), inner)
        slots(p - 1)
        hidden(p)
        if p + 2 == last and last > 2:
            arrivals(last, (0, 1), inner)
    if last > 0:
        there = order[last][1]
        pl.when((there >= 0) & (there < length))(relays[2, last].wait_send)
    pl.when(inner)(give_held)
    put(stok, stok_out)
    put(scot, scot_out)
    shsum[...] = dot_t(shared_full(0), sg[...]) + dot_t(shared_full(1), su[...])
    for p in range(last):
        hidden_rows(p)
    own_meta = all_meta[chip, core]
    where_home = own_meta.T.astype(jnp.int32)
    hcol = lax.broadcasted_iota(jnp.int32, (tok, home), 1)
    lane_at = lax.broadcasted_iota(jnp.int32, (ep * 128, tok), 0)
    lanes = own_meta[6:8, :].astype(jnp.int32) + core * cap
    spots = [(lane_at == lanes[k : k + 1, :]).astype(F32).astype(BF) for k in range(2)]
    spots = jnp.concatenate(spots, axis=1)
    slots(last)
    put(hg, hg_out)
    put(hu, hu_out)
    homeward(0)
    hidden_rows(last)
    put(hh, hh_out)

    homeward(1)
    homeward(2)
    for c in spread_out:
        c.wait_recv()
    flat = []
    for n in range(3):
        parts = [
            jnp.concatenate([share_t[1, n, j, q] for j in range(ep)], axis=1) for q in range(tp)
        ]
        flat.append(jnp.concatenate(parts, axis=0))
    tok_flat = all_tok[...].reshape(ep * tok, dl)
    osg[...] = dot(flat[0], tok_flat)
    put(osg, osg_out)
    osu[...] = dot(flat[1], tok_flat)
    put(osu, osu_out)
    osd[...] = dot(flat[2], all_cot[...].reshape(ep * tok, dl))
    put(osd, osd_out)

    for p in range(3, length):
        homeward(p)
    gtok[...] = shsum[...].astype(BF)
    put(gtok, gtok_out)
    dg = jnp.concatenate([dgb[j] for j in range(ep)], axis=1)
    high = dg.astype(BF)
    low = (dg - high.astype(F32)).astype(BF)
    total = dot(high, spots) + dot(low, spots)
    gw[...] = jnp.concatenate(
        [total[0:1, :tok], total[0:1, tok:], jnp.zeros((6, tok), F32)], axis=0
    )
    put(gw, gw_out)
    for cond, c in sends:
        if cond is None:
            c.wait_send()
        else:
            pl.when(cond)(c.wait_send)
    for c in outs:
        c.wait()


def grads_kernel(
    dims,
    gtok_in,
    gw_in,
    osg_in,
    osu_in,
    osd_in,
    stok_in,
    scot_in,
    hg_in,
    hu_in,
    hh_in,
    gtok_out,
    gw_out,
    grad_gate,
    grad_up,
    grad_down,
    osg_out,
    osu_out,
    osd_out,
    gtok,
    gw,
    osg,
    osu,
    osd,
    stok,
    scot,
    hg,
    hu,
    hh,
    gate_rows,
    up_rows,
    down_rows,
    in_sem,
    out_sem,
):
    ne, chunks = dims
    ins = []
    for n, (src, dst) in enumerate(
        (
            (stok_in, stok),
            (hg_in, hg),
            (hu_in, hu),
            (hh_in, hh),
            (scot_in, scot),
            (gtok_in, gtok),
            (gw_in, gw),
            (osg_in, osg),
            (osu_in, osu),
            (osd_in, osd),
        )
    ):
        c = pltpu.make_async_copy(src, dst, in_sem.at[n])
        c.start()
        ins.append(c)
    outs = []

    def put(src, dst):
        c = pltpu.make_async_copy(src, dst, out_sem.at[len(outs)])
        c.start()
        outs.append(c)

    def outer(a, b):
        return lax.dot_general(a, b, (((0,), (0,)), ((), ())), preferred_element_type=F32)

    def cut(size):
        step = size // chunks
        return [slice(i * step, (i + 1) * step) for i in range(chunks)]

    for n in range(3):
        ins[n].wait()
    for e in range(ne):
        for r in cut(stok.shape[2]):
            left = stok[e, :, r]
            gate_rows[e, r, :] = outer(left, hg[e])
            put(gate_rows.at[e, r], grad_gate.at[e, r])
            up_rows[e, r, :] = outer(left, hu[e])
            put(up_rows.at[e, r], grad_up.at[e, r])
    for n in range(3, 10):
        ins[n].wait()
    for src, dst in (
        (gtok, gtok_out),
        (gw.at[pl.ds(0, gw_out.shape[0])], gw_out),
        (osg, osg_out),
        (osu, osu_out),
        (osd, osd_out),
    ):
        put(src, dst)
    for e in range(ne):
        for r in cut(hh.shape[2]):
            down_rows[e, r, :] = outer(hh[e, :, r], scot[e])
            put(down_rows.at[e, r], grad_down.at[e, r])
    for c in outs:
        c.wait()


def line_body(
    tokens,
    routes,
    route_weights,
    cotangent,
    expert_gate,
    expert_up,
    expert_down,
    shared_gate,
    shared_up,
    shared_down,
):
    tok, top = routes.shape
    dl = tokens.shape[1]
    ne, _, ff = expert_gate.shape
    sff = shared_gate.shape[1]
    ep, tp = lax.axis_size("ep"), lax.axis_size("tp")
    cap = max(2, 5 * tok * top // (4 * ep * ne))
    length = ep // CORES
    pair = CORES * cap
    rows = up_to(pair, 16)
    group = ne * pair
    home = ne * cap
    width, swidth, swid = ff // tp, sff // tp, sff // ep
    dims = (ep, tp, tok, dl, ne, ff, sff, cap, rows, width, swidth, swid)

    hbm = pl.BlockSpec(memory_space=pltpu.HBM)
    dma = pltpu.SemaphoreType.DMA
    sds = jax.ShapeDtypeStruct
    shapes = (
        sds((tok, dl), BF),
        sds((8, tok), F32),
        sds((swid, dl), F32),
        sds((swid, dl), F32),
        sds((swid, dl), F32),
        sds((ne, length * rows, dl), BF),
        sds((ne, length * rows, dl), BF),
        sds((ne, length * rows, ff), BF),
        sds((ne, length * rows, ff), BF),
        sds((ne, length * rows, ff), BF),
    )
    scratch = [
        pltpu.VMEM((top, tok), jnp.int32),
        pltpu.VMEM((top, tok), F32),
        *[pltpu.VMEM(s.shape, s.dtype) for s in shapes],
        pltpu.VMEM((length, CORES, tok, dl), BF),
        pltpu.VMEM((length, CORES, tok, dl), BF),
        pltpu.VMEM((length, CORES, 8, tok), F32),
        pltpu.VMEM(expert_gate.shape, BF),
        pltpu.VMEM(expert_up.shape, BF),
        pltpu.VMEM(expert_down.shape, BF),
        pltpu.VMEM(shared_gate.shape, BF),
        pltpu.VMEM(shared_up.shape, BF),
        pltpu.VMEM(shared_down.shape, BF),
        pltpu.VMEM((length, group, 128), F32),
        pltpu.VMEM((tp, 3, tok, swidth), BF),
        pltpu.VMEM((tp, 3, tok, swidth), F32),
        pltpu.VMEM((tp, 3, tok, swidth), BF),
        pltpu.VMEM((tp, 3, tok, swidth), BF),
        pltpu.VMEM((2, 3, ep, tp, swid // tp, tok), BF),
        pltpu.VMEM((length, tp, 3, group, width), BF),
        pltpu.VMEM((length, tp, 3, group, width), F32),
        pltpu.VMEM((length, tp, 3, group, width), BF),
        pltpu.VMEM((length, tp, 3, group, width), BF),
        pltpu.VMEM((length, tp, 8, 128), F32),
        pltpu.VMEM((length, 8, 128), F32),
        pltpu.VMEM((ep, 8, 128), F32),
        pltpu.VMEM((length, CORES, home, dl), BF),
        pltpu.VMEM((ep, home, dl), BF),
        pltpu.VMEM((tok, dl), F32),
        dma((6,)),
        dma((4,)),
        dma((len(shapes),)),
        dma((6,)),
        dma((3 * length,)),
        dma((3 * length,)),
        dma((3 * length,)),
        dma((3 * length,)),
        dma((tp,)),
        dma((tp,)),
        dma((tp,)),
        dma((tp,)),
        dma((2 * length * tp,)),
        dma((2 * length * tp,)),
        dma((3 * length * tp,)),
        dma((3 * length * tp,)),
        dma((ep,)),
        dma((ep,)),
        dma((tp,)),
        dma((tp,)),
        dma((2 * CORES * length,)),
        dma((2 * ep,)),
    ]
    outs = pl.pallas_call(
        functools.partial(line_kernel, dims),
        out_shape=shapes,
        in_specs=[hbm] * 10,
        out_specs=tuple([hbm] * len(shapes)),
        scratch_shapes=scratch,
        compiler_params=pltpu.CompilerParams(
            collective_id=0, has_side_effects=True, vmem_limit_bytes=60 * 1024 * 1024
        ),
    )(
        routes.T,
        route_weights.T,
        tokens,
        cotangent,
        expert_gate,
        expert_up,
        expert_down,
        shared_gate,
        shared_up,
        shared_down,
    )
    chunks = 4
    results = (
        sds((tok, dl), BF),
        sds((top, tok), F32),
        sds((ne, dl, ff), F32),
        sds((ne, dl, ff), F32),
        sds((ne, ff, dl), F32),
        sds((swid, dl), F32),
        sds((swid, dl), F32),
        sds((swid, dl), F32),
    )
    gtok, gw, grad_gate, grad_up, grad_down, osg, osu, osd = pl.pallas_call(
        functools.partial(grads_kernel, (ne, chunks)),
        out_shape=results,
        in_specs=[hbm] * len(shapes),
        out_specs=tuple([hbm] * len(results)),
        scratch_shapes=[
            *[pltpu.VMEM(s.shape, s.dtype) for s in shapes],
            *[pltpu.VMEM(s.shape, s.dtype) for s in results[2:5]],
            dma((len(shapes),)),
            dma((3 * ne * chunks + 5,)),
        ],
        compiler_params=pltpu.CompilerParams(vmem_limit_bytes=60 * 1024 * 1024),
        name="grads",
    )(*outs)
    return gtok, gw.T, grad_gate, grad_up, grad_down, osg.T, osu.T, osd


def body(tokens, routes, *rest):
    tok, top = routes.shape
    ne, _, ff = rest[2].shape
    sff = rest[5].shape[1]
    ep, tp = lax.axis_size("ep"), lax.axis_size("tp")
    cap = max(2, 5 * tok * top // (4 * ep * ne))
    lines = (
        ep == 4 * CORES
        and ff == tp * 128
        and sff == tp * 128
        and (CORES * cap) % 8 == 0
        and (ne * cap) % 8 == 0
        and (ne * CORES * cap) % 16 == 0
        and ne * CORES * cap <= 128
        and tok == 128
        and sff % (ep * tp * 16) == 0
        and top == 2
    )
    return (line_body if lines else rows_body)(tokens, routes, *rest)


def solution(mesh):
    return jax.shard_map(
        body,
        mesh=mesh,
        in_specs=(
            P("ep", "tp"),
            P("ep", None),
            P("ep", None),
            P("ep", "tp"),
            P("ep", "tp", None),
            P("ep", "tp", None),
            P("ep", None, "tp"),
            P("tp", None),
            P("tp", None),
            P(None, "tp"),
        ),
        out_specs=(
            P("ep", "tp"),
            P("ep", None),
            P("ep", "tp", None),
            P("ep", "tp", None),
            P("ep", None, "tp"),
            P("tp", "ep"),
            P("tp", "ep"),
            P("ep", "tp"),
        ),
        check_vma=False,
    )
```

```python
import functools

import jax
import jax.numpy as jnp
from jax import lax
from jax.experimental import pallas as pl
from jax.experimental.pallas import tpu as pltpu
from jax.sharding import PartitionSpec as P

CORES = 2
BF = jnp.bfloat16
F32 = jnp.float32


def up_to(value, unit):
    return -(-value // unit) * unit


def dot(a, b):
    return jnp.dot(a, b, preferred_element_type=F32)


def dot_t(a, b):
    return lax.dot_general(a, b, (((1,), (1,)), ((), ())), preferred_element_type=F32)


def hidden_terms(gate_pre, up_pre, back_grad, scaling):
    logistic = jax.nn.sigmoid(gate_pre)
    silu = gate_pre * logistic
    product = silu * up_pre
    grad_act = back_grad if scaling is None else scaling * back_grad
    gate_grad = grad_act * up_pre * logistic * (1.0 + gate_pre * (1.0 - logistic))
    hidden = product if scaling is None else scaling * product
    return (
        gate_grad.astype(BF),
        (grad_act * silu).astype(BF),
        hidden.astype(BF),
        jnp.sum(back_grad * product, axis=-1, keepdims=True),
    )


def ring_plan(length):
    plan = []
    for step in range(1, length // 2 + 1):
        last_even = length % 2 == 0 and step == length // 2
        plan.append((step, 0, (0,) if last_even else (0, 1)))
        plan.append((step, 1, (1,) if last_even else (1, 0)))
    return plan


def rows_kernel(
    dims,
    meta_in,
    tok_in,
    cot_in,
    eg_in,
    eu_in,
    ed_in,
    sg_in,
    su_in,
    sd_in,
    gtok_out,
    gw_out,
    osg,
    osu,
    osd,
    stok,
    scot,
    hg,
    hu,
    hh,
    all_tok,
    all_cot,
    all_meta,
    eg,
    eu,
    ed,
    sg,
    su,
    sd,
    sel,
    gates,
    sh_part,
    sh_recv,
    sh_all,
    share_t,
    part,
    exact,
    recv,
    dgs,
    back_send,
    back,
    shsum,
    load_sem,
    own_sem,
    ring_s,
    ring_r,
    mate_s,
    mate_r,
    shr_s,
    shr_r,
    sha_s,
    sha_r,
    pr_s,
    pr_r,
    pa_s,
    pa_r,
    xt_s,
    xt_r,
    bk_s,
    bk_r,
):
    ep, tp, tok, dl, ne, ff, sff, cap, re, rows, rpp, rpt, cp, swid = dims
    me = lax.axis_index("ep")
    mt = lax.axis_index("tp")
    length = ep // CORES
    chip = me // CORES
    core = me % CORES
    mate = chip * CORES + (1 - core)
    nxt = ((chip + 1) % length) * CORES + core
    prv = ((chip + length - 1) % length) * CORES + core

    owns = []
    for n, (src, dst) in enumerate(((tok_in, all_tok), (cot_in, all_cot), (meta_in, all_meta))):
        c = pltpu.make_async_copy(src, dst.at[me], own_sem.at[n])
        c.start()
        owns.append(c)
    loads = []
    for n, (src, dst) in enumerate(
        ((sg_in, sg), (su_in, su), (sd_in, sd), (eg_in, eg), (eu_in, eu), (ed_in, ed))
    ):
        c = pltpu.make_async_copy(src, dst, load_sem.at[n])
        c.start()
        loads.append(c)

    barrier = pltpu.get_barrier_semaphore()
    for o in range(1, ep):
        pl.semaphore_signal(barrier, inc=1, device_id={"ep": (me + o) % ep})
    for o in range(1, tp):
        pl.semaphore_signal(barrier, inc=1, device_id={"tp": (mt + o) % tp})
    pl.semaphore_wait(barrier, ep + tp - 2)

    sends = []

    def remote(src, dst, ssem, rsem, dev):
        c = pltpu.make_async_remote_copy(
            src_ref=src, dst_ref=dst, send_sem=ssem, recv_sem=rsem, device_id=dev
        )
        c.start()
        sends.append(c)
        return c

    bufs = (all_tok, all_cot, all_meta)
    ring_copies = {}
    mate_copies = []
    plan = {(step, d): items for step, d, items in ring_plan(length)}

    def ring_send(step, d, item, src):
        dest = nxt if d == 0 else prv
        subs = (0, 2) if item == 0 else (1,)
        for b in subs:
            n = ((step - 1) * 2 + d) * 3 + b
            ring_copies[step, d, b] = remote(
                bufs[b].at[src], bufs[b].at[src], ring_s.at[n], ring_r.at[n], {"ep": dest}
            )

    def mate_send(item, src):
        for b in (0, 2) if item == 0 else (1,):
            n = len(mate_copies)
            mate_copies.append(
                remote(
                    bufs[b].at[src], bufs[b].at[src], mate_s.at[n], mate_r.at[n], {"ep": mate}
                )
            )

    for c in owns:
        c.wait()
    for pos in range(2):
        for d in range(2):
            items = plan.get((1, d), ())
            if pos < len(items):
                ring_send(1, d, items[pos], me)
    mate_send(0, me)
    mate_send(1, me)

    tp_order = [(mt + o) % tp for o in range(1, tp)]
    if rpt * tp > tok:
        sh_part[:, tok:, :] = jnp.zeros((3, rpt * tp - tok, sff), BF)
    for n in range(3):
        loads[n].wait()
        if n < 2:
            val = dot(all_tok[me], (sg, su)[n][...])
        else:
            val = dot_t(all_cot[me], sd[...])
        sh_part[n, :tok, :] = val.astype(BF)
    sh_copies = []
    for o in range(1, tp):
        peer = tp_order[o - 1]
        sh_copies.append(
            remote(
                sh_part.at[:, pl.ds(pl.multiple_of(peer * rpt, 16), rpt), :],
                sh_recv.at[o],
                shr_s.at[o],
                shr_r.at[o],
                {"tp": peer},
            )
        )

    def ring_arrivals(step):
        for pos in range(2):
            for d in range(2):
                items = plan.get((step, d), ())
                if pos >= len(items):
                    continue
                item = items[pos]
                away = length - step if d == 0 else step
                src = ((chip + away) % length) * CORES + core
                for b in (0, 2) if item == 0 else (1,):
                    ring_copies[step, d, b].wait_recv()
                if item in plan.get((step + 1, d), ()):
                    ring_send(step + 1, d, item, src)
                mate_send(item, src)

    if length > 1:
        ring_arrivals(1)

    for c in sh_copies:
        c.wait_recv()
    mine_t = pl.ds(pl.multiple_of(mt * rpt, 16), rpt)
    tot = [sh_part[n, mine_t, :].astype(F32) for n in range(3)]
    for o in range(1, tp):
        for n in range(3):
            tot[n] = tot[n] + sh_recv[o, n].astype(F32)
    a, b, c3, _ = hidden_terms(tot[0], tot[1], tot[2], None)
    sh_all[0, mine_t, :] = a
    sh_all[1, mine_t, :] = b
    sh_all[2, mine_t, :] = c3
    sha = []
    for o in range(1, tp):
        sha.append(
            remote(
                sh_all.at[:, mine_t, :],
                sh_all.at[:, mine_t, :],
                sha_s.at[o],
                sha_r.at[o],
                {"tp": tp_order[o - 1]},
            )
        )

    for step in range(2, length // 2 + 1):
        ring_arrivals(step)
    for c in mate_copies:
        c.wait_recv()

    row_id = lax.broadcasted_iota(jnp.int32, (rows, tok), 0)
    gate = jnp.zeros((rows, 1), F32)
    for j in range(ep):
        m = all_meta[j]
        code = m[0:2, :].astype(jnp.int32) + (j * cap - me * (ne * re))
        p0 = (row_id == code[0:1, :]).astype(F32)
        p1 = (row_id == code[1:2, :]).astype(F32)
        sel[:, j * tok : (j + 1) * tok] = (p0 + p1).astype(BF)
        gate = gate + jnp.sum(p0 * m[2:3, :] + p1 * m[3:4, :], axis=1, keepdims=True)
    te = rpp * tp
    for e in range(ne):
        gates[e, :re, :] = jnp.broadcast_to(gate[e * re : (e + 1) * re, :], (re, 128))
        if te > re:
            gates[e, re:, :] = jnp.zeros((te - re, 128), F32)
            part[e, :, re:, :] = jnp.zeros((3, te - re, ff), BF)
            exact[e, :, re:, :] = jnp.zeros((3, te - re, ff), F32)

    stok[...] = dot(sel[...], all_tok[...].reshape(ep * tok, dl)).astype(BF)
    scot[...] = dot(sel[...], all_cot[...].reshape(ep * tok, dl)).astype(BF)
    for n in range(3):
        loads[3 + n].wait()
    p_copies = [[] for _ in range(ne)]
    for e in range(ne):
        for n in range(3):
            r = slice(e * re, (e + 1) * re)
            val = dot_t(scot[r, :], ed[e]) if n == 2 else dot(stok[r, :], (eg, eu)[n][e])
            exact[e, n, :re, :] = val
            part[e, n, :re, :] = val.astype(BF)
            for o in range(1, tp):
                peer = tp_order[o - 1]
                k = (e * 3 + n) * tp + o
                p_copies[e].append(
                    remote(
                        part.at[e, n, pl.ds(pl.multiple_of(peer * rpp, 8), rpp), :],
                        recv.at[o, e, n],
                        pr_s.at[k],
                        pr_r.at[k],
                        {"tp": peer},
                    )
                )

    for c in sha:
        c.wait_recv()
    for n in range(3):
        back_t = sh_all[n, :tok, :].astype(F32).T.astype(BF)
        for j in range(ep):
            share_t[0, n, j] = back_t[j * swid : (j + 1) * swid, :]
    xts = []
    for o in range(1, ep):
        peer = (me + o) % ep
        xts.append(
            remote(
                share_t.at[0, :, peer],
                share_t.at[1, :, me],
                xt_s.at[o],
                xt_r.at[o],
                {"ep": peer},
            )
        )
    for n in range(3):
        share_t[1, n, me] = share_t[0, n, me]
    mine = pl.ds(pl.multiple_of(mt * rpp, 8), rpp)
    lane = lax.broadcasted_iota(jnp.int32, (rpp, 128), 1)
    pas = []
    for e in range(ne):
        for c in p_copies[e]:
            c.wait_recv()
        tot = [exact[e, n, mine, :] for n in range(3)]
        for o in range(1, tp):
            for n in range(3):
                tot[n] = tot[n] + recv[o, e, n].astype(F32)
        a, b, c3, dg = hidden_terms(tot[0], tot[1], tot[2], gates[e, mine, :][:, 0:1])
        hg[e, mine, :] = a
        hu[e, mine, :] = b
        hh[e, mine, :] = c3
        high = dg.astype(BF).astype(F32)
        dgs[e, mine, :] = jnp.where(
            lane == 0, high, jnp.where(lane == 1, dg - high, 0.0)
        ).astype(BF)
        group = []
        for k, buf in enumerate((hg, hu, dgs, hh)):
            for o in range(1, tp):
                n = (e * 4 + k) * tp + o
                group.append(
                    remote(
                        buf.at[e, mine, :],
                        buf.at[e, mine, :],
                        pa_s.at[n],
                        pa_r.at[n],
                        {"tp": tp_order[o - 1]},
                    )
                )
        pas.append(group)

    col = lax.broadcasted_iota(jnp.int32, (8, re), 1)
    block = jnp.zeros((8, re), jnp.int32)
    for j in range(1, ep):
        block = block + (col >= j * cap).astype(jnp.int32)
    target = block * cp + (col - block * cap)
    target = jnp.where(col < ep * cap, target, -1)
    pick = (
        (lax.broadcasted_iota(jnp.int32, (ep * cp, re), 0) == target[0:1, :])
        .astype(F32)
        .astype(BF)
    )
    bks = []
    for e in range(ne):
        for c in pas[e][: 3 * (tp - 1)]:
            c.wait_recv()
        slot = (dot_t(hg[e, :re, :], eg[e]) + dot_t(hu[e, :re, :], eu[e])).astype(BF)
        back_send[e, :, :, :dl] = dot(pick, slot).astype(BF).reshape(ep, cp, dl)
        back_send[e, :, :, dl:] = dot(pick, dgs[e, :re, :]).astype(BF).reshape(ep, cp, 128)
        for o in range(1, ep):
            peer = (me + o) % ep
            bks.append(
                remote(
                    back_send.at[e, peer],
                    back.at[e, me],
                    bk_s.at[e * ep + o],
                    bk_r.at[e * ep + o],
                    {"ep": peer},
                )
            )
        back[e, me] = back_send[e, me]

    shsum[...] = dot_t(sh_all[0, :tok, :], sg[...]) + dot_t(sh_all[1, :tok, :], su[...])
    for c in xts:
        c.wait_recv()
    flat = [
        jnp.concatenate([share_t[1, n, j] for j in range(ep)], axis=1) for n in range(3)
    ]
    tok_flat = all_tok[...].reshape(ep * tok, dl)
    osg[...] = dot(flat[0], tok_flat)
    osu[...] = dot(flat[1], tok_flat)
    osd[...] = dot(flat[2], all_cot[...].reshape(ep * tok, dl))

    width = ne * ep * cp
    home = all_meta[me].T.astype(jnp.int32)
    hcol = lax.broadcasted_iota(jnp.int32, (tok, width), 1)
    g0 = (hcol == home[:, 4:5]).astype(F32)
    g1 = (hcol == home[:, 5:6]).astype(F32)
    both = (g0 + g1).astype(BF)
    for c in bks:
        c.wait_recv()
    flat_back = back[...].reshape(width, dl + 128)
    gtok_out[...] = (dot(both, flat_back[:, :dl]) + shsum[...]).astype(BF)
    w0 = jnp.sum(dot(g0.astype(BF), flat_back[:, dl:]), axis=1, keepdims=True)
    w1 = jnp.sum(dot(g1.astype(BF), flat_back[:, dl:]), axis=1, keepdims=True)
    wl = lax.broadcasted_iota(jnp.int32, (tok, 128), 1)
    gw_out[...] = jnp.where(wl == 0, w0, w1).T[0:2, :]
    for group in pas:
        for c in group[3 * (tp - 1) :]:
            c.wait_recv()
    for c in sends:
        c.wait_send()


def rows_body(
    tokens,
    routes,
    route_weights,
    cotangent,
    expert_gate,
    expert_up,
    expert_down,
    shared_gate,
    shared_up,
    shared_down,
):
    tok, top = routes.shape
    dl = tokens.shape[1]
    ne, _, ff = expert_gate.shape
    sff = shared_gate.shape[1]
    ep, tp = lax.axis_size("ep"), lax.axis_size("tp")
    cap = max(2, 5 * tok * top // (4 * ep * ne))
    re = up_to(ep * cap, 16)
    rows = ne * re
    rpp = up_to(-(-re // tp), 8)
    rpt = up_to(-(-tok // tp), 16)
    cp = up_to(cap, 8)
    swid = sff // ep
    length = ep // CORES
    total = rpp * tp
    dims = (ep, tp, tok, dl, ne, ff, sff, cap, re, rows, rpp, rpt, cp, swid)

    picked = routes.T.reshape(-1)
    earlier = jnp.arange(top * tok)[None, :] < jnp.arange(top * tok)[:, None]
    same = picked[:, None] == picked[None, :]
    ranked = jnp.sum((same & earlier).astype(jnp.int32), axis=1)
    code = (picked * re + ranked).reshape(top, tok)
    home = (((picked % ne) * ep + picked // ne) * cp + ranked).reshape(top, tok)
    gate = route_weights.astype(BF).astype(F32).T
    meta = jnp.concatenate(
        [code.astype(F32), gate, home.astype(F32), jnp.zeros((8 - 3 * top, tok), F32)], axis=0
    )

    vm = pl.BlockSpec(memory_space=pltpu.VMEM)
    hbm = pl.BlockSpec(memory_space=pl.ANY)
    dma = pltpu.SemaphoreType.DMA
    n_ring = max(1, (length // 2) * 6)
    scratch = [
        pltpu.VMEM((ep, tok, dl), BF),
        pltpu.VMEM((ep, tok, dl), BF),
        pltpu.VMEM((ep, 8, tok), F32),
        pltpu.VMEM(expert_gate.shape, BF),
        pltpu.VMEM(expert_up.shape, BF),
        pltpu.VMEM(expert_down.shape, BF),
        pltpu.VMEM(shared_gate.shape, BF),
        pltpu.VMEM(shared_up.shape, BF),
        pltpu.VMEM(shared_down.shape, BF),
        pltpu.VMEM((rows, ep * tok), BF),
        pltpu.VMEM((ne, total, 128), F32),
        pltpu.VMEM((3, rpt * tp, sff), BF),
        pltpu.VMEM((tp, 3, rpt, sff), BF),
        pltpu.VMEM((3, rpt * tp, sff), BF),
        pltpu.VMEM((2, 3, ep, swid, tok), BF),
        pltpu.VMEM((ne, 3, total, ff), BF),
        pltpu.VMEM((ne, 3, total, ff), F32),
        pltpu.VMEM((tp, ne, 3, rpp, ff), BF),
        pltpu.VMEM((ne, total, 128), BF),
        pltpu.VMEM((ne, ep, cp, dl + 128), BF),
        pltpu.VMEM((ne, ep, cp, dl + 128), BF),
        pltpu.VMEM((tok, dl), F32),
        dma((6,)),
        dma((3,)),
        dma((n_ring,)),
        dma((n_ring,)),
        dma((3 * length,)),
        dma((3 * length,)),
        dma((tp,)),
        dma((tp,)),
        dma((tp,)),
        dma((tp,)),
        dma((3 * ne * tp,)),
        dma((3 * ne * tp,)),
        dma((4 * ne * tp,)),
        dma((4 * ne * tp,)),
        dma((ep,)),
        dma((ep,)),
        dma((ne * ep,)),
        dma((ne * ep,)),
    ]
    sds = jax.ShapeDtypeStruct
    outs = pl.pallas_call(
        functools.partial(rows_kernel, dims),
        out_shape=(
            sds((tok, dl), BF),
            sds((top, tok), F32),
            sds((swid, dl), F32),
            sds((swid, dl), F32),
            sds((swid, dl), F32),
            sds((rows, dl), BF),
            sds((rows, dl), BF),
            sds((ne, total, ff), BF),
            sds((ne, total, ff), BF),
            sds((ne, total, ff), BF),
        ),
        in_specs=[hbm] * 9,
        out_specs=tuple([vm] * 10),
        scratch_shapes=scratch,
        compiler_params=pltpu.CompilerParams(
            collective_id=0, has_side_effects=True, vmem_limit_bytes=60 * 1024 * 1024
        ),
    )(
        meta,
        tokens,
        cotangent,
        expert_gate,
        expert_up,
        expert_down,
        shared_gate,
        shared_up,
        shared_down,
    )
    gtok, gw, osg, osu, osd, stok, scot, hg, hu, hh = outs
    stok = stok.reshape(ne, re, dl)
    scot = scot.reshape(ne, re, dl)
    hg, hu, hh = (h[:, :re] for h in (hg, hu, hh))
    grad_gate = jnp.einsum("esd,esf->edf", stok, hg, preferred_element_type=F32)
    grad_up = jnp.einsum("esd,esf->edf", stok, hu, preferred_element_type=F32)
    grad_down = jnp.einsum("esf,esd->efd", hh, scot, preferred_element_type=F32)
    return gtok, gw.T, grad_gate, grad_up, grad_down, osg.T, osu.T, osd


def line_order(chip, length):
    high = (2 * chip) // length
    far = 1 - 2 * high
    edge = chip * (1 - high) + (length - 1 - chip) * high
    order = [(chip, None, None)]
    for p in range(1, length):
        two_sided = (2 * edge - p + 2 * length) // (2 * length)
        dist = two_sided * ((p + 1) // 2) + (1 - two_sided) * (p - edge)
        toward = far * (1 - 2 * two_sided * (p % 2))
        order.append((chip + toward * dist, chip - toward, two_sided))
    return order


def line_kernel(
    dims,
    routes_in,
    weights_in,
    tok_in,
    cot_in,
    eg_in,
    eu_in,
    ed_in,
    sg_in,
    su_in,
    sd_in,
    gtok_out,
    gw_out,
    osg_out,
    osu_out,
    osd_out,
    stok_out,
    scot_out,
    hg_out,
    hu_out,
    hh_out,
    routes,
    weights,
    gtok,
    gw,
    osg,
    osu,
    osd,
    stok,
    scot,
    hg,
    hu,
    hh,
    all_tok,
    all_cot,
    all_meta,
    eg,
    eu,
    ed,
    sg,
    su,
    sd,
    gates,
    sh_part,
    sh_exact,
    sh_recv,
    sh_all,
    share_t,
    part,
    exact,
    recv,
    hs,
    dgp,
    dgs,
    dgb,
    back_send,
    back,
    shsum,
    load_sem,
    own_sem,
    out_sem,
    own_s,
    line_s,
    line_r,
    mate_s,
    mate_r,
    shr_s,
    shr_r,
    sha_s,
    sha_r,
    pr_s,
    pr_r,
    pa_s,
    pa_r,
    xt_s,
    xt_r,
    xy_s,
    xy_r,
    bk_s,
    bk_r,
):
    ep, tp, tok, dl, ne, ff, sff, cap, rows, width, swidth, swid = dims
    me = lax.axis_index("ep")
    mt = lax.axis_index("tp")
    length = ep // CORES
    chip = me // CORES
    core = me % CORES
    mate = chip * CORES + (1 - core)
    pair = CORES * cap
    group = ne * pair
    home = ne * cap
    part_rows = swid // tp
    order = line_order(chip, length)
    bufs = (all_tok, all_meta, all_cot)

    owns = []
    for n, (src, dst) in enumerate(
        (
            (tok_in, all_tok.at[chip, core]),
            (cot_in, all_cot.at[chip, core]),
            (routes_in, routes),
            (weights_in, weights),
        )
    ):
        c = pltpu.make_async_copy(src, dst, own_sem.at[n])
        c.start()
        owns.append(c)
    loads = []
    for n, (src, dst) in enumerate(
        ((sg_in, sg), (su_in, su), (sd_in, sd), (eg_in, eg), (eu_in, eu), (ed_in, ed))
    ):
        c = pltpu.make_async_copy(src, dst, load_sem.at[n])
        c.start()
        loads.append(c)

    barrier = pltpu.get_barrier_semaphore()
    def greet(there):
        pl.semaphore_signal(barrier, inc=1, device_id={"ep": there * CORES + core})

    pl.semaphore_signal(barrier, inc=1, device_id={"ep": mate})
    for o in range(1, tp):
        pl.semaphore_signal(barrier, inc=1, device_id={"tp": (mt + o) % tp})
    pl.when(chip < length - 1)(lambda: greet(chip + 1))
    pl.when(chip > 0)(lambda: greet(chip - 1))
    above = (2 * length - 2 - chip) // length
    below = (chip + length - 1) // length

    pl.semaphore_wait(barrier, tp + above + below)

    sends = []

    def copy_of(src, dst, ssem, rsem, dev):
        return pltpu.make_async_remote_copy(
            src_ref=src, dst_ref=dst, send_sem=ssem, recv_sem=rsem, device_id=dev
        )

    def remote(src, dst, ssem, rsem, dev):
        copy_of(src, dst, ssem, rsem, dev).start()

    def got(block, sem):
        copy_of(block, block, own_s.at[0], sem, {"ep": mate}).wait_recv()

    def left(block, sem):
        copy_of(block, block, sem, own_s.at[0], {"ep": mate}).wait_send()

    def along_line(b, src, ssem, there):
        block = bufs[b].at[src, core]
        dest = ((there + length) % length) * CORES + core
        return copy_of(block, block, ssem, line_r.at[b * length + src], {"ep": dest})

    def to_mate(b, p):
        block = bufs[b].at[order[p][0], core]
        n = b * length + p
        return copy_of(block, block, mate_s.at[b], mate_r.at[n], {"ep": mate})

    def send_own(b):
        for d, there in enumerate((chip + 1, chip - 1)):
            c = along_line(b, chip, own_s.at[2 * b + d], there)
            inside = chip < length - 1 if d == 0 else chip > 0
            pl.when(inside)(c.start)
            sends.append((inside, c))

    def send_mate(b):
        to_mate(b, 0).start()

    owns[0].wait()
    send_own(0)
    send_mate(0)
    owns[1].wait()
    send_mate(2)

    owns[2].wait()
    owns[3].wait()
    table = jnp.concatenate(
        [
            routes[...].astype(F32),
            weights[...].astype(BF).astype(F32),
            jnp.zeros((4, tok), F32),
        ],
        axis=0,
    )
    picked = table.T
    earlier = lax.broadcasted_iota(jnp.int32, (tok, tok), 0) < lax.broadcasted_iota(
        jnp.int32, (tok, tok), 1
    )

    def count(hits):
        return jnp.sum(hits.astype(F32), axis=0, keepdims=True)

    first, second = picked[:, 0:1], picked[:, 1:2]
    ranks = [
        count((first == table[0:1]) & earlier),
        count((second == table[1:2]) & earlier) + count(first == table[1:2]),
    ]
    ranked = jnp.concatenate(ranks, axis=0)
    named = table[0:2]
    owner = jnp.floor((named + 0.5) * (1.0 / ne))
    which = named - owner * ne
    all_meta[chip, core] = jnp.concatenate(
        [
            named * rows + ranked,
            table[2:4],
            owner * home + which * cap + ranked,
            owner * 128 + which * pair + ranked,
        ],
        axis=0,
    )
    send_own(1)
    send_mate(1)

    relays = {}
    mates = {}
    for p in range(1, length):
        src, there, _ = order[p]
        for b in range(3):
            relays[b, p] = along_line(b, src, line_s.at[b * length + p], there)
            mates[b, p] = to_mate(b, p)
            if p < length - 1 or b < 2:
                sends.append(((there >= 0) & (there < length), relays[b, p]))

    def arrivals(p, which, cond=None):
        def run():
            _, there, _ = order[p]
            for b in which:
                relays[b, p].wait_recv()
                pl.when((there >= 0) & (there < length))(relays[b, p].start)
                mates[b, p].start()

        if cond is None:
            run()
        else:
            pl.when(cond)(run)

    def mate_wait(p, which):
        for b in which:
            to_mate(b, p).wait_recv()

    peers = [(mt + o) % tp for o in range(1, tp)]
    inner = chip * (length - 1 - chip) > 0
    outer = chip * (length - 1 - chip) < 1

    own_tok = all_tok[chip, core]
    own_cot = all_cot[chip, core]
    for n in range(3):
        loads[n].wait()
        val = dot(own_tok, (sg, su)[n][...]) if n < 2 else dot_t(own_cot, sd[...])
        for q in range(tp):
            piece = val[:, q * swidth : (q + 1) * swidth]
            sh_exact[q, n] = piece
            sh_part[q, n] = piece.astype(BF)
    for o in range(1, tp):
        peer = peers[o - 1]
        remote(sh_part.at[peer], sh_recv.at[o], shr_s.at[0], shr_r.at[0], {"tp": peer})
    others = pl.ds(1, tp - 1)
    any_tp = pl.ds(0, tp - 1)

    row_id = lax.broadcasted_iota(jnp.int32, (ne * rows, tok), 0)
    sels = {}

    def selection(p):
        src = order[p][0]
        halves = []
        gate = jnp.zeros((ne * rows, 1), F32)
        for jj in range(CORES):
            m = all_meta[src, jj]
            code = m[0:2, :].astype(jnp.int32) + (jj * cap - me * (ne * rows))
            p0 = (row_id == code[0:1, :]).astype(F32)
            p1 = (row_id == code[1:2, :]).astype(F32)
            halves.append((p0 + p1).astype(BF))
            gate = gate + jnp.sum(p0 * m[2:3, :] + p1 * m[3:4, :], axis=1, keepdims=True)
        sels[p] = jnp.concatenate(halves, axis=1)
        gate = jnp.concatenate([gate[e * rows : e * rows + pair] for e in range(ne)], axis=0)
        gates[p] = jnp.broadcast_to(gate, (group, 128))

    def products(p, which):
        src = order[p][0]
        buf, out = (all_cot, scot) if which == (2,) else (all_tok, stok)
        picked = dot(sels[p], buf[src].reshape(CORES * tok, dl)).astype(BF)
        for e in range(ne):
            out[e, p * rows : (p + 1) * rows, :] = picked[e * rows : (e + 1) * rows]
        for n in which:
            vals = []
            for e in range(ne):
                x = picked[e * rows : (e + 1) * rows]
                val = dot_t(x, ed[e]) if n == 2 else dot(x, (eg, eu)[n][e])
                vals.append(val[:pair])
            val = jnp.concatenate(vals, axis=0)
            for q in range(tp):
                piece = val[:, q * width : (q + 1) * width]
                exact[p, q, n] = piece
                part[p, q, n] = piece.astype(BF)
        half = 1 if which == (2,) else 0
        span = pl.ds(which[0], len(which))
        for o in range(1, tp):
            remote(
                part.at[p, peers[o - 1], span],
                recv.at[p, o, span],
                pr_s.at[0],
                pr_r.at[2 * p + half],
                {"tp": peers[o - 1]},
            )

    def products_all(p):
        selection(p)
        products(p, (0, 1))
        products(p, (2,))

    def send_hidden(p, piece):
        for o in range(1, tp):
            if piece < 2:
                block = hs.at[p, mt, pl.ds(2 * piece, 2 - piece)]
            else:
                block = dgp.at[p, mt]
            remote(
                block, block, pa_s.at[piece // 2], pa_r.at[3 * p + piece], {"tp": peers[o - 1]}
            )

    def hidden_got(p, piece):
        if piece < 2:
            got(hs.at[p, any_tp, pl.ds(2 * piece, 2 - piece)], pa_r.at[3 * p + piece])
        else:
            got(dgp.at[p, any_tp], pa_r.at[3 * p + piece])

    def hidden(p):
        got(recv.at[p, others, pl.ds(0, 2)], pr_r.at[2 * p])
        got(recv.at[p, others, pl.ds(2, 1)], pr_r.at[2 * p + 1])
        tot = [exact[p, mt, n] for n in range(3)]
        for o in range(1, tp):
            for n in range(3):
                tot[n] = tot[n] + recv[p, o, n].astype(F32)
        gate = gates[p][:, 0:1]
        logistic = jax.nn.sigmoid(tot[0])
        silu = tot[0] * logistic
        product = silu * tot[1]
        grad_act = gate * tot[2]
        hs[p, mt, 0] = (
            grad_act * tot[1] * logistic * (1.0 + tot[0] * (1.0 - logistic))
        ).astype(BF)
        hs[p, mt, 1] = (grad_act * silu).astype(BF)
        hs[p, mt, 2] = (gate * product).astype(BF)
        terms = tot[2] * product
        fill = jnp.zeros((128 - group, width), F32)
        cols = jnp.concatenate([terms, fill], axis=0).T
        dgp[p, mt] = jnp.broadcast_to(jnp.sum(cols, axis=0, keepdims=True), (8, 128))
        for piece in (2, 0) if p == length - 1 else (2, 0, 1):
            send_hidden(p, piece)

    def pick_rows():
        at = lax.broadcasted_iota(jnp.int32, (group, group), 0)
        col = lax.broadcasted_iota(jnp.int32, (group, group), 1)
        wanted = at * 0
        for jj in range(CORES):
            for e in range(ne):
                low = jj * home + e * cap
                inside = (at >= low) & (at < low + cap)
                wanted = jnp.where(inside, at - low + e * pair + jj * cap, wanted)
        return (col == wanted).astype(F32).astype(BF)

    pick = pick_rows()
    held = []

    def give(c, hold):
        if hold:
            pl.when(outer)(c.start)
            held.append(c)
        else:
            c.start()

    def give_held():
        for c in held:
            c.start()

    def spread(p, n, out):
        full = jnp.concatenate([hs[p, q, n] for q in range(tp)], axis=1).astype(F32)
        fill = jnp.zeros((rows - pair, ff), F32)
        blocks = []
        for e in range(ne):
            block = full[e * pair : (e + 1) * pair]
            if rows > pair:
                block = jnp.concatenate([block, fill], axis=0)
            block = block.astype(BF)
            out[e, p * rows : (p + 1) * rows, :] = block
            blocks.append(block)
        return blocks

    def slots(p):
        src = order[p][0]
        hidden_got(p, 0)
        if p == length - 1:
            send_hidden(p, 1)
            share_columns()
        a = spread(p, 0, hg)
        b = spread(p, 1, hu)
        vals = [(dot_t(a[e], eg[e]) + dot_t(b[e], eu[e]))[:pair] for e in range(ne)]
        slot = jnp.concatenate(vals, axis=0).astype(BF)
        moved = dot(pick, slot)
        for jj in range(CORES):
            back_send[p, jj] = moved[jj * home : (jj + 1) * home].astype(BF)
        hidden_got(p, 2)
        total = dgp[p, 0]
        for q in range(1, tp):
            total = total + dgp[p, q]
        dgs[p] = total
        if p == 0:
            back[me] = back_send[0, core]
            dgb[me] = total
            targets = [(1 - core, mate)]
        else:
            targets = [(jj, src * CORES + jj) for jj in range(CORES)]
        for jj, dest in targets:
            for c in (
                copy_of(
                    back_send.at[p, jj], back.at[me], bk_s.at[0], bk_r.at[chip], {"ep": dest}
                ),
                copy_of(dgs.at[p], dgb.at[me], bk_s.at[1], bk_r.at[length + chip], {"ep": dest}),
            ):
                give(c, p == 1)

    def shared_hidden():
        got(sh_recv.at[others], shr_r.at[0])
        tot = [sh_exact[mt, n] for n in range(3)]
        for o in range(1, tp):
            for n in range(3):
                tot[n] = tot[n] + sh_recv[o, n].astype(F32)
        a, b, c3, _ = hidden_terms(tot[0], tot[1], tot[2], None)
        sh_all[mt, 0] = a
        sh_all[mt, 1] = b
        sh_all[mt, 2] = c3
        for o in range(1, tp):
            remote(
                sh_all.at[mt], sh_all.at[mt], sha_s.at[0], sha_r.at[0], {"tp": peers[o - 1]}
            )

    def share_columns():
        got(share_t.at[1, :, pl.ds(0, ep - 1), 0], xt_r.at[0])
        for o in range(1, tp):
            block = share_t.at[1, :, :, mt]
            remote(block, block, xy_s.at[0], xy_r.at[0], {"tp": peers[o - 1]})

    def shared_full(n):
        return jnp.concatenate([sh_all[q, n] for q in range(tp)], axis=1)

    def shared_shares():
        for n in range(3):
            back_t = shared_full(n).astype(F32).T.astype(BF)
            for j in range(ep):
                for q in range(tp):
                    low = j * swid + q * part_rows
                    share_t[0, n, j, q] = back_t[low : low + part_rows, :]
        for o in range(1, ep):
            peer = (me + o) % ep
            c = copy_of(
                share_t.at[0, :, peer, mt],
                share_t.at[1, :, me, mt],
                xt_s.at[0],
                xt_r.at[0],
                {"ep": peer},
            )
            give(c, True)
        for n in range(3):
            share_t[1, n, me, mt] = share_t[0, n, me, mt]

    def homeward(p):
        src = order[p][0]
        from_there = pl.ds(src * CORES, CORES) if p else pl.ds(mate, 1)
        got(back.at[from_there], bk_r.at[src])
        got(dgb.at[from_there], bk_r.at[length + src])
        for jj in range(CORES):
            j = src * CORES + jj
            g0 = (hcol == where_home[:, 4:5] - j * home).astype(F32)
            g1 = (hcol == where_home[:, 5:6] - j * home).astype(F32)
            shsum[...] += dot((g0 + g1).astype(BF), back[j])

    outs = []

    def put(src, dst):
        c = pltpu.make_async_copy(src, dst, out_sem.at[len(outs)])
        c.start()
        outs.append(c)

    def hidden_rows(p):
        hidden_got(p, 1)
        spread(p, 2, hh)

    def first_arrivals(which):
        if length > 1:
            arrivals(1, which)
        if length > 2:
            arrivals(2, which, order[2][2] > 0)

    mate_wait(0, (0, 1))
    for n in range(3):
        loads[3 + n].wait()
    mate_wait(0, (2,))
    products_all(0)
    send_own(2)
    shared_hidden()
    first_arrivals((0, 1))
    hidden(0)
    last = length - 1
    for p in range(1, length):
        split = p == last
        if p == 1:
            first_arrivals((2,))
        elif not split:
            far = order[p][2] < 1 if p % 2 == 0 or p == last else None
            arrivals(p, (0, 1, 2), far)
            if p % 2 == 1 and p + 1 < last:
                arrivals(p + 1, (0, 1, 2), order[p + 1][2] > 0)
        else:
            arrivals(p, (0, 1), outer)
        mate_wait(p, (0, 1))
        selection(p)
        products(p, (0, 1))
        if split:
            got(sh_all.at[any_tp], sha_r.at[0])
            shared_shares()
            arrivals(p, (2,), outer)
        mate_wait(p, (2,))
        products(p, (2,))
        if p + 1 == last and last > 2:
            arrivals(last, (2,), inner)
        slots(p - 1)
        hidden(p)
        if p + 2 == last and last > 2:
            arrivals(last, (0, 1), inner)
    if last > 0:
        there = order[last][1]
        pl.when((there >= 0) & (there < length))(relays[2, last].wait_send)
    pl.when(inner)(give_held)
    put(stok, stok_out)
    put(scot, scot_out)
    shsum[...] = dot_t(shared_full(0), sg[...]) + dot_t(shared_full(1), su[...])
    for p in range(last):
        hidden_rows(p)
    own_meta = all_meta[chip, core]
    where_home = own_meta.T.astype(jnp.int32)
    hcol = lax.broadcasted_iota(jnp.int32, (tok, home), 1)
    lane_at = lax.broadcasted_iota(jnp.int32, (ep * 128, tok), 0)
    lanes = own_meta[6:8, :].astype(jnp.int32) + core * cap
    spots = [(lane_at == lanes[k : k + 1, :]).astype(F32).astype(BF) for k in range(2)]
    spots = jnp.concatenate(spots, axis=1)
    slots(last)
    put(hg, hg_out)
    put(hu, hu_out)
    homeward(0)
    hidden_rows(last)
    put(hh, hh_out)

    homeward(1)
    homeward(2)
    got(share_t.at[1, :, :, any_tp], xy_r.at[0])
    flat = []
    for n in range(3):
        parts = [
            jnp.concatenate([share_t[1, n, j, q] for j in range(ep)], axis=1) for q in range(tp)
        ]
        flat.append(jnp.concatenate(parts, axis=0))
    tok_flat = all_tok[...].reshape(ep * tok, dl)
    osg[...] = dot(flat[0], tok_flat)
    put(osg, osg_out)
    osu[...] = dot(flat[1], tok_flat)
    put(osu, osu_out)
    osd[...] = dot(flat[2], all_cot[...].reshape(ep * tok, dl))
    put(osd, osd_out)

    for p in range(3, length):
        homeward(p)
    gtok[...] = shsum[...].astype(BF)
    put(gtok, gtok_out)
    dg = jnp.concatenate([dgb[j] for j in range(ep)], axis=1)
    high = dg.astype(BF)
    low = (dg - high.astype(F32)).astype(BF)
    total = dot(high, spots) + dot(low, spots)
    gw[...] = jnp.concatenate(
        [total[0:1, :tok], total[0:1, tok:], jnp.zeros((6, tok), F32)], axis=0
    )
    put(gw, gw_out)
    for cond, c in sends:
        pl.when(cond)(c.wait_send)
    for b in range(3):
        left(bufs[b].at[:, 0], mate_s.at[b])
    left(sh_part.at[any_tp], shr_s.at[0])
    left(sh_all.at[any_tp], sha_s.at[0])
    left(part.at[:, any_tp], pr_s.at[0])
    left(hs.at[:, any_tp], pa_s.at[0])
    left(dgp.at[:, any_tp], pa_s.at[1])
    left(share_t.at[0, :, pl.ds(0, ep - 1), 0], xt_s.at[0])
    left(share_t.at[1, :, :, any_tp], xy_s.at[0])
    left(back.at[pl.ds(0, ep - 1)], bk_s.at[0])
    left(dgb.at[pl.ds(0, ep - 1)], bk_s.at[1])
    for c in outs:
        c.wait()


def grads_kernel(
    dims,
    gtok_in,
    gw_in,
    osg_in,
    osu_in,
    osd_in,
    stok_in,
    scot_in,
    hg_in,
    hu_in,
    hh_in,
    gtok_out,
    gw_out,
    grad_gate,
    grad_up,
    grad_down,
    osg_out,
    osu_out,
    osd_out,
    gtok,
    gw,
    osg,
    osu,
    osd,
    stok,
    scot,
    hg,
    hu,
    hh,
    gate_rows,
    up_rows,
    down_rows,
    in_sem,
    out_sem,
):
    ne, chunks = dims
    ins = []
    for n, (src, dst) in enumerate(
        (
            (stok_in, stok),
            (hg_in, hg),
            (hu_in, hu),
            (hh_in, hh),
            (scot_in, scot),
            (gtok_in, gtok),
            (gw_in, gw),
            (osg_in, osg),
            (osu_in, osu),
            (osd_in, osd),
        )
    ):
        c = pltpu.make_async_copy(src, dst, in_sem.at[n])
        c.start()
        ins.append(c)
    outs = []

    def put(src, dst):
        c = pltpu.make_async_copy(src, dst, out_sem.at[len(outs)])
        c.start()
        outs.append(c)

    def outer(a, b):
        return lax.dot_general(a, b, (((0,), (0,)), ((), ())), preferred_element_type=F32)

    def cut(size):
        step = size // chunks
        return [slice(i * step, (i + 1) * step) for i in range(chunks)]

    for n in range(3):
        ins[n].wait()
    for e in range(ne):
        for r in cut(stok.shape[2]):
            left = stok[e, :, r]
            gate_rows[e, r, :] = outer(left, hg[e])
            put(gate_rows.at[e, r], grad_gate.at[e, r])
            up_rows[e, r, :] = outer(left, hu[e])
            put(up_rows.at[e, r], grad_up.at[e, r])
    for n in range(3, 10):
        ins[n].wait()
    for src, dst in (
        (gtok, gtok_out),
        (gw.at[pl.ds(0, gw_out.shape[0])], gw_out),
        (osg, osg_out),
        (osu, osu_out),
        (osd, osd_out),
    ):
        put(src, dst)
    for e in range(ne):
        for r in cut(hh.shape[2]):
            down_rows[e, r, :] = outer(hh[e, :, r], scot[e])
            put(down_rows.at[e, r], grad_down.at[e, r])
    for c in outs:
        c.wait()


def line_body(
    tokens,
    routes,
    route_weights,
    cotangent,
    expert_gate,
    expert_up,
    expert_down,
    shared_gate,
    shared_up,
    shared_down,
):
    tok, top = routes.shape
    dl = tokens.shape[1]
    ne, _, ff = expert_gate.shape
    sff = shared_gate.shape[1]
    ep, tp = lax.axis_size("ep"), lax.axis_size("tp")
    cap = max(2, 5 * tok * top // (4 * ep * ne))
    length = ep // CORES
    pair = CORES * cap
    rows = up_to(pair, 16)
    group = ne * pair
    home = ne * cap
    width, swidth, swid = ff // tp, sff // tp, sff // ep
    dims = (ep, tp, tok, dl, ne, ff, sff, cap, rows, width, swidth, swid)

    hbm = pl.BlockSpec(memory_space=pltpu.HBM)
    dma = pltpu.SemaphoreType.DMA
    sds = jax.ShapeDtypeStruct
    shapes = (
        sds((tok, dl), BF),
        sds((8, tok), F32),
        sds((swid, dl), F32),
        sds((swid, dl), F32),
        sds((swid, dl), F32),
        sds((ne, length * rows, dl), BF),
        sds((ne, length * rows, dl), BF),
        sds((ne, length * rows, ff), BF),
        sds((ne, length * rows, ff), BF),
        sds((ne, length * rows, ff), BF),
    )
    scratch = [
        pltpu.VMEM((top, tok), jnp.int32),
        pltpu.VMEM((top, tok), F32),
        *[pltpu.VMEM(s.shape, s.dtype) for s in shapes],
        pltpu.VMEM((length, CORES, tok, dl), BF),
        pltpu.VMEM((length, CORES, tok, dl), BF),
        pltpu.VMEM((length, CORES, 8, tok), F32),
        pltpu.VMEM(expert_gate.shape, BF),
        pltpu.VMEM(expert_up.shape, BF),
        pltpu.VMEM(expert_down.shape, BF),
        pltpu.VMEM(shared_gate.shape, BF),
        pltpu.VMEM(shared_up.shape, BF),
        pltpu.VMEM(shared_down.shape, BF),
        pltpu.VMEM((length, group, 128), F32),
        pltpu.VMEM((tp, 3, tok, swidth), BF),
        pltpu.VMEM((tp, 3, tok, swidth), F32),
        pltpu.VMEM((tp, 3, tok, swidth), BF),
        pltpu.VMEM((tp, 3, tok, swidth), BF),
        pltpu.VMEM((2, 3, ep, tp, swid // tp, tok), BF),
        pltpu.VMEM((length, tp, 3, group, width), BF),
        pltpu.VMEM((length, tp, 3, group, width), F32),
        pltpu.VMEM((length, tp, 3, group, width), BF),
        pltpu.VMEM((length, tp, 3, group, width), BF),
        pltpu.VMEM((length, tp, 8, 128), F32),
        pltpu.VMEM((length, 8, 128), F32),
        pltpu.VMEM((ep, 8, 128), F32),
        pltpu.VMEM((length, CORES, home, dl), BF),
        pltpu.VMEM((ep, home, dl), BF),
        pltpu.VMEM((tok, dl), F32),
        dma((6,)),
        dma((4,)),
        dma((len(shapes),)),
        dma((6,)),
        dma((3 * length,)),
        dma((3 * length,)),
        dma((3,)),
        dma((3 * length,)),
        *[dma((1,))] * 5,
        dma((2 * length,)),
        dma((2,)),
        dma((3 * length,)),
        *[dma((1,))] * 4,
        dma((2,)),
        dma((2 * length,)),
    ]
    outs = pl.pallas_call(
        functools.partial(line_kernel, dims),
        out_shape=shapes,
        in_specs=[hbm] * 10,
        out_specs=tuple([hbm] * len(shapes)),
        scratch_shapes=scratch,
        compiler_params=pltpu.CompilerParams(
            collective_id=0, has_side_effects=True, vmem_limit_bytes=60 * 1024 * 1024
        ),
    )(
        routes.T,
        route_weights.T,
        tokens,
        cotangent,
        expert_gate,
        expert_up,
        expert_down,
        shared_gate,
        shared_up,
        shared_down,
    )
    chunks = 4
    results = (
        sds((tok, dl), BF),
        sds((top, tok), F32),
        sds((ne, dl, ff), F32),
        sds((ne, dl, ff), F32),
        sds((ne, ff, dl), F32),
        sds((swid, dl), F32),
        sds((swid, dl), F32),
        sds((swid, dl), F32),
    )
    gtok, gw, grad_gate, grad_up, grad_down, osg, osu, osd = pl.pallas_call(
        functools.partial(grads_kernel, (ne, chunks)),
        out_shape=results,
        in_specs=[hbm] * len(shapes),
        out_specs=tuple([hbm] * len(results)),
        scratch_shapes=[
            *[pltpu.VMEM(s.shape, s.dtype) for s in shapes],
            *[pltpu.VMEM(s.shape, s.dtype) for s in results[2:5]],
            dma((len(shapes),)),
            dma((3 * ne * chunks + 5,)),
        ],
        compiler_params=pltpu.CompilerParams(vmem_limit_bytes=60 * 1024 * 1024),
        name="grads",
    )(*outs)
    return gtok, gw.T, grad_gate, grad_up, grad_down, osg.T, osu.T, osd


def body(tokens, routes, *rest):
    tok, top = routes.shape
    ne, _, ff = rest[2].shape
    sff = rest[5].shape[1]
    ep, tp = lax.axis_size("ep"), lax.axis_size("tp")
    cap = max(2, 5 * tok * top // (4 * ep * ne))
    lines = (
        ep == 4 * CORES
        and ff == tp * 128
        and sff == tp * 128
        and (CORES * cap) % 8 == 0
        and (ne * cap) % 8 == 0
        and (ne * CORES * cap) % 16 == 0
        and ne * CORES * cap <= 128
        and tok == 128
        and sff % (ep * tp * 16) == 0
        and top == 2
    )
    return (line_body if lines else rows_body)(tokens, routes, *rest)


def solution(mesh):
    return jax.shard_map(
        body,
        mesh=mesh,
        in_specs=(
            P("ep", "tp"),
            P("ep", None),
            P("ep", None),
            P("ep", "tp"),
            P("ep", "tp", None),
            P("ep", "tp", None),
            P("ep", None, "tp"),
            P("tp", None),
            P("tp", None),
            P(None, "tp"),
        ),
        out_specs=(
            P("ep", "tp"),
            P("ep", None),
            P("ep", "tp", None),
            P("ep", "tp", None),
            P("ep", None, "tp"),
            P("tp", "ep"),
            P("tp", "ep"),
            P("ep", "tp"),
        ),
        check_vma=False,
    )
```

```python
import functools

import jax
import jax.numpy as jnp
from jax import lax
from jax.experimental import pallas as pl
from jax.experimental.pallas import tpu as pltpu
from jax.sharding import PartitionSpec as P

CORES = 2
BF = jnp.bfloat16
F32 = jnp.float32


def up_to(value, unit):
    return -(-value // unit) * unit


def dot(a, b):
    return jnp.dot(a, b, preferred_element_type=F32)


def dot_t(a, b):
    return lax.dot_general(a, b, (((1,), (1,)), ((), ())), preferred_element_type=F32)


def hidden_terms(gate_pre, up_pre, back_grad, scaling):
    logistic = jax.nn.sigmoid(gate_pre)
    silu = gate_pre * logistic
    product = silu * up_pre
    grad_act = back_grad if scaling is None else scaling * back_grad
    gate_grad = grad_act * up_pre * logistic * (1.0 + gate_pre * (1.0 - logistic))
    hidden = product if scaling is None else scaling * product
    return (
        gate_grad.astype(BF),
        (grad_act * silu).astype(BF),
        hidden.astype(BF),
        jnp.sum(back_grad * product, axis=-1, keepdims=True),
    )


def ring_plan(length):
    plan = []
    for step in range(1, length // 2 + 1):
        last_even = length % 2 == 0 and step == length // 2
        plan.append((step, 0, (0,) if last_even else (0, 1)))
        plan.append((step, 1, (1,) if last_even else (1, 0)))
    return plan


def rows_kernel(
    dims,
    meta_in,
    tok_in,
    cot_in,
    eg_in,
    eu_in,
    ed_in,
    sg_in,
    su_in,
    sd_in,
    gtok_out,
    gw_out,
    osg,
    osu,
    osd,
    stok,
    scot,
    hg,
    hu,
    hh,
    all_tok,
    all_cot,
    all_meta,
    eg,
    eu,
    ed,
    sg,
    su,
    sd,
    sel,
    gates,
    sh_part,
    sh_recv,
    sh_all,
    share_t,
    part,
    exact,
    recv,
    dgs,
    back_send,
    back,
    shsum,
    load_sem,
    own_sem,
    ring_s,
    ring_r,
    mate_s,
    mate_r,
    shr_s,
    shr_r,
    sha_s,
    sha_r,
    pr_s,
    pr_r,
    pa_s,
    pa_r,
    xt_s,
    xt_r,
    bk_s,
    bk_r,
):
    ep, tp, tok, dl, ne, ff, sff, cap, re, rows, rpp, rpt, cp, swid = dims
    me = lax.axis_index("ep")
    mt = lax.axis_index("tp")
    length = ep // CORES
    chip = me // CORES
    core = me % CORES
    mate = chip * CORES + (1 - core)
    nxt = ((chip + 1) % length) * CORES + core
    prv = ((chip + length - 1) % length) * CORES + core

    owns = []
    for n, (src, dst) in enumerate(((tok_in, all_tok), (cot_in, all_cot), (meta_in, all_meta))):
        c = pltpu.make_async_copy(src, dst.at[me], own_sem.at[n])
        c.start()
        owns.append(c)
    loads = []
    for n, (src, dst) in enumerate(
        ((sg_in, sg), (su_in, su), (sd_in, sd), (eg_in, eg), (eu_in, eu), (ed_in, ed))
    ):
        c = pltpu.make_async_copy(src, dst, load_sem.at[n])
        c.start()
        loads.append(c)

    barrier = pltpu.get_barrier_semaphore()
    for o in range(1, ep):
        pl.semaphore_signal(barrier, inc=1, device_id={"ep": (me + o) % ep})
    for o in range(1, tp):
        pl.semaphore_signal(barrier, inc=1, device_id={"tp": (mt + o) % tp})
    pl.semaphore_wait(barrier, ep + tp - 2)

    sends = []

    def remote(src, dst, ssem, rsem, dev):
        c = pltpu.make_async_remote_copy(
            src_ref=src, dst_ref=dst, send_sem=ssem, recv_sem=rsem, device_id=dev
        )
        c.start()
        sends.append(c)
        return c

    bufs = (all_tok, all_cot, all_meta)
    ring_copies = {}
    mate_copies = []
    plan = {(step, d): items for step, d, items in ring_plan(length)}

    def ring_send(step, d, item, src):
        dest = nxt if d == 0 else prv
        subs = (0, 2) if item == 0 else (1,)
        for b in subs:
            n = ((step - 1) * 2 + d) * 3 + b
            ring_copies[step, d, b] = remote(
                bufs[b].at[src], bufs[b].at[src], ring_s.at[n], ring_r.at[n], {"ep": dest}
            )

    def mate_send(item, src):
        for b in (0, 2) if item == 0 else (1,):
            n = len(mate_copies)
            mate_copies.append(
                remote(
                    bufs[b].at[src], bufs[b].at[src], mate_s.at[n], mate_r.at[n], {"ep": mate}
                )
            )

    for c in owns:
        c.wait()
    for pos in range(2):
        for d in range(2):
            items = plan.get((1, d), ())
            if pos < len(items):
                ring_send(1, d, items[pos], me)
    mate_send(0, me)
    mate_send(1, me)

    tp_order = [(mt + o) % tp for o in range(1, tp)]
    if rpt * tp > tok:
        sh_part[:, tok:, :] = jnp.zeros((3, rpt * tp - tok, sff), BF)
    for n in range(3):
        loads[n].wait()
        if n < 2:
            val = dot(all_tok[me], (sg, su)[n][...])
        else:
            val = dot_t(all_cot[me], sd[...])
        sh_part[n, :tok, :] = val.astype(BF)
    sh_copies = []
    for o in range(1, tp):
        peer = tp_order[o - 1]
        sh_copies.append(
            remote(
                sh_part.at[:, pl.ds(pl.multiple_of(peer * rpt, 16), rpt), :],
                sh_recv.at[o],
                shr_s.at[o],
                shr_r.at[o],
                {"tp": peer},
            )
        )

    def ring_arrivals(step):
        for pos in range(2):
            for d in range(2):
                items = plan.get((step, d), ())
                if pos >= len(items):
                    continue
                item = items[pos]
                away = length - step if d == 0 else step
                src = ((chip + away) % length) * CORES + core
                for b in (0, 2) if item == 0 else (1,):
                    ring_copies[step, d, b].wait_recv()
                if item in plan.get((step + 1, d), ()):
                    ring_send(step + 1, d, item, src)
                mate_send(item, src)

    if length > 1:
        ring_arrivals(1)

    for c in sh_copies:
        c.wait_recv()
    mine_t = pl.ds(pl.multiple_of(mt * rpt, 16), rpt)
    tot = [sh_part[n, mine_t, :].astype(F32) for n in range(3)]
    for o in range(1, tp):
        for n in range(3):
            tot[n] = tot[n] + sh_recv[o, n].astype(F32)
    a, b, c3, _ = hidden_terms(tot[0], tot[1], tot[2], None)
    sh_all[0, mine_t, :] = a
    sh_all[1, mine_t, :] = b
    sh_all[2, mine_t, :] = c3
    sha = []
    for o in range(1, tp):
        sha.append(
            remote(
                sh_all.at[:, mine_t, :],
                sh_all.at[:, mine_t, :],
                sha_s.at[o],
                sha_r.at[o],
                {"tp": tp_order[o - 1]},
            )
        )

    for step in range(2, length // 2 + 1):
        ring_arrivals(step)
    for c in mate_copies:
        c.wait_recv()

    row_id = lax.broadcasted_iota(jnp.int32, (rows, tok), 0)
    gate = jnp.zeros((rows, 1), F32)
    for j in range(ep):
        m = all_meta[j]
        code = m[0:2, :].astype(jnp.int32) + (j * cap - me * (ne * re))
        p0 = (row_id == code[0:1, :]).astype(F32)
        p1 = (row_id == code[1:2, :]).astype(F32)
        sel[:, j * tok : (j + 1) * tok] = (p0 + p1).astype(BF)
        gate = gate + jnp.sum(p0 * m[2:3, :] + p1 * m[3:4, :], axis=1, keepdims=True)
    te = rpp * tp
    for e in range(ne):
        gates[e, :re, :] = jnp.broadcast_to(gate[e * re : (e + 1) * re, :], (re, 128))
        if te > re:
            gates[e, re:, :] = jnp.zeros((te - re, 128), F32)
            part[e, :, re:, :] = jnp.zeros((3, te - re, ff), BF)
            exact[e, :, re:, :] = jnp.zeros((3, te - re, ff), F32)

    stok[...] = dot(sel[...], all_tok[...].reshape(ep * tok, dl)).astype(BF)
    scot[...] = dot(sel[...], all_cot[...].reshape(ep * tok, dl)).astype(BF)
    for n in range(3):
        loads[3 + n].wait()
    p_copies = [[] for _ in range(ne)]
    for e in range(ne):
        for n in range(3):
            r = slice(e * re, (e + 1) * re)
            val = dot_t(scot[r, :], ed[e]) if n == 2 else dot(stok[r, :], (eg, eu)[n][e])
            exact[e, n, :re, :] = val
            part[e, n, :re, :] = val.astype(BF)
            for o in range(1, tp):
                peer = tp_order[o - 1]
                k = (e * 3 + n) * tp + o
                p_copies[e].append(
                    remote(
                        part.at[e, n, pl.ds(pl.multiple_of(peer * rpp, 8), rpp), :],
                        recv.at[o, e, n],
                        pr_s.at[k],
                        pr_r.at[k],
                        {"tp": peer},
                    )
                )

    for c in sha:
        c.wait_recv()
    for n in range(3):
        back_t = sh_all[n, :tok, :].astype(F32).T.astype(BF)
        for j in range(ep):
            share_t[0, n, j] = back_t[j * swid : (j + 1) * swid, :]
    xts = []
    for o in range(1, ep):
        peer = (me + o) % ep
        xts.append(
            remote(
                share_t.at[0, :, peer],
                share_t.at[1, :, me],
                xt_s.at[o],
                xt_r.at[o],
                {"ep": peer},
            )
        )
    for n in range(3):
        share_t[1, n, me] = share_t[0, n, me]
    mine = pl.ds(pl.multiple_of(mt * rpp, 8), rpp)
    lane = lax.broadcasted_iota(jnp.int32, (rpp, 128), 1)
    pas = []
    for e in range(ne):
        for c in p_copies[e]:
            c.wait_recv()
        tot = [exact[e, n, mine, :] for n in range(3)]
        for o in range(1, tp):
            for n in range(3):
                tot[n] = tot[n] + recv[o, e, n].astype(F32)
        a, b, c3, dg = hidden_terms(tot[0], tot[1], tot[2], gates[e, mine, :][:, 0:1])
        hg[e, mine, :] = a
        hu[e, mine, :] = b
        hh[e, mine, :] = c3
        high = dg.astype(BF).astype(F32)
        dgs[e, mine, :] = jnp.where(
            lane == 0, high, jnp.where(lane == 1, dg - high, 0.0)
        ).astype(BF)
        group = []
        for k, buf in enumerate((hg, hu, dgs, hh)):
            for o in range(1, tp):
                n = (e * 4 + k) * tp + o
                group.append(
                    remote(
                        buf.at[e, mine, :],
                        buf.at[e, mine, :],
                        pa_s.at[n],
                        pa_r.at[n],
                        {"tp": tp_order[o - 1]},
                    )
                )
        pas.append(group)

    col = lax.broadcasted_iota(jnp.int32, (8, re), 1)
    block = jnp.zeros((8, re), jnp.int32)
    for j in range(1, ep):
        block = block + (col >= j * cap).astype(jnp.int32)
    target = block * cp + (col - block * cap)
    target = jnp.where(col < ep * cap, target, -1)
    pick = (
        (lax.broadcasted_iota(jnp.int32, (ep * cp, re), 0) == target[0:1, :])
        .astype(F32)
        .astype(BF)
    )
    bks = []
    for e in range(ne):
        for c in pas[e][: 3 * (tp - 1)]:
            c.wait_recv()
        slot = (dot_t(hg[e, :re, :], eg[e]) + dot_t(hu[e, :re, :], eu[e])).astype(BF)
        back_send[e, :, :, :dl] = dot(pick, slot).astype(BF).reshape(ep, cp, dl)
        back_send[e, :, :, dl:] = dot(pick, dgs[e, :re, :]).astype(BF).reshape(ep, cp, 128)
        for o in range(1, ep):
            peer = (me + o) % ep
            bks.append(
                remote(
                    back_send.at[e, peer],
                    back.at[e, me],
                    bk_s.at[e * ep + o],
                    bk_r.at[e * ep + o],
                    {"ep": peer},
                )
            )
        back[e, me] = back_send[e, me]

    shsum[...] = dot_t(sh_all[0, :tok, :], sg[...]) + dot_t(sh_all[1, :tok, :], su[...])
    for c in xts:
        c.wait_recv()
    flat = [
        jnp.concatenate([share_t[1, n, j] for j in range(ep)], axis=1) for n in range(3)
    ]
    tok_flat = all_tok[...].reshape(ep * tok, dl)
    osg[...] = dot(flat[0], tok_flat)
    osu[...] = dot(flat[1], tok_flat)
    osd[...] = dot(flat[2], all_cot[...].reshape(ep * tok, dl))

    width = ne * ep * cp
    home = all_meta[me].T.astype(jnp.int32)
    hcol = lax.broadcasted_iota(jnp.int32, (tok, width), 1)
    g0 = (hcol == home[:, 4:5]).astype(F32)
    g1 = (hcol == home[:, 5:6]).astype(F32)
    both = (g0 + g1).astype(BF)
    for c in bks:
        c.wait_recv()
    flat_back = back[...].reshape(width, dl + 128)
    gtok_out[...] = (dot(both, flat_back[:, :dl]) + shsum[...]).astype(BF)
    w0 = jnp.sum(dot(g0.astype(BF), flat_back[:, dl:]), axis=1, keepdims=True)
    w1 = jnp.sum(dot(g1.astype(BF), flat_back[:, dl:]), axis=1, keepdims=True)
    wl = lax.broadcasted_iota(jnp.int32, (tok, 128), 1)
    gw_out[...] = jnp.where(wl == 0, w0, w1).T[0:2, :]
    for group in pas:
        for c in group[3 * (tp - 1) :]:
            c.wait_recv()
    for c in sends:
        c.wait_send()


def rows_body(
    tokens,
    routes,
    route_weights,
    cotangent,
    expert_gate,
    expert_up,
    expert_down,
    shared_gate,
    shared_up,
    shared_down,
):
    tok, top = routes.shape
    dl = tokens.shape[1]
    ne, _, ff = expert_gate.shape
    sff = shared_gate.shape[1]
    ep, tp = lax.axis_size("ep"), lax.axis_size("tp")
    cap = max(2, 5 * tok * top // (4 * ep * ne))
    re = up_to(ep * cap, 16)
    rows = ne * re
    rpp = up_to(-(-re // tp), 8)
    rpt = up_to(-(-tok // tp), 16)
    cp = up_to(cap, 8)
    swid = sff // ep
    length = ep // CORES
    total = rpp * tp
    dims = (ep, tp, tok, dl, ne, ff, sff, cap, re, rows, rpp, rpt, cp, swid)

    picked = routes.T.reshape(-1)
    earlier = jnp.arange(top * tok)[None, :] < jnp.arange(top * tok)[:, None]
    same = picked[:, None] == picked[None, :]
    ranked = jnp.sum((same & earlier).astype(jnp.int32), axis=1)
    code = (picked * re + ranked).reshape(top, tok)
    home = (((picked % ne) * ep + picked // ne) * cp + ranked).reshape(top, tok)
    gate = route_weights.astype(BF).astype(F32).T
    meta = jnp.concatenate(
        [code.astype(F32), gate, home.astype(F32), jnp.zeros((8 - 3 * top, tok), F32)], axis=0
    )

    vm = pl.BlockSpec(memory_space=pltpu.VMEM)
    hbm = pl.BlockSpec(memory_space=pl.ANY)
    dma = pltpu.SemaphoreType.DMA
    n_ring = max(1, (length // 2) * 6)
    scratch = [
        pltpu.VMEM((ep, tok, dl), BF),
        pltpu.VMEM((ep, tok, dl), BF),
        pltpu.VMEM((ep, 8, tok), F32),
        pltpu.VMEM(expert_gate.shape, BF),
        pltpu.VMEM(expert_up.shape, BF),
        pltpu.VMEM(expert_down.shape, BF),
        pltpu.VMEM(shared_gate.shape, BF),
        pltpu.VMEM(shared_up.shape, BF),
        pltpu.VMEM(shared_down.shape, BF),
        pltpu.VMEM((rows, ep * tok), BF),
        pltpu.VMEM((ne, total, 128), F32),
        pltpu.VMEM((3, rpt * tp, sff), BF),
        pltpu.VMEM((tp, 3, rpt, sff), BF),
        pltpu.VMEM((3, rpt * tp, sff), BF),
        pltpu.VMEM((2, 3, ep, swid, tok), BF),
        pltpu.VMEM((ne, 3, total, ff), BF),
        pltpu.VMEM((ne, 3, total, ff), F32),
        pltpu.VMEM((tp, ne, 3, rpp, ff), BF),
        pltpu.VMEM((ne, total, 128), BF),
        pltpu.VMEM((ne, ep, cp, dl + 128), BF),
        pltpu.VMEM((ne, ep, cp, dl + 128), BF),
        pltpu.VMEM((tok, dl), F32),
        dma((6,)),
        dma((3,)),
        dma((n_ring,)),
        dma((n_ring,)),
        dma((3 * length,)),
        dma((3 * length,)),
        dma((tp,)),
        dma((tp,)),
        dma((tp,)),
        dma((tp,)),
        dma((3 * ne * tp,)),
        dma((3 * ne * tp,)),
        dma((4 * ne * tp,)),
        dma((4 * ne * tp,)),
        dma((ep,)),
        dma((ep,)),
        dma((ne * ep,)),
        dma((ne * ep,)),
    ]
    sds = jax.ShapeDtypeStruct
    outs = pl.pallas_call(
        functools.partial(rows_kernel, dims),
        out_shape=(
            sds((tok, dl), BF),
            sds((top, tok), F32),
            sds((swid, dl), F32),
            sds((swid, dl), F32),
            sds((swid, dl), F32),
            sds((rows, dl), BF),
            sds((rows, dl), BF),
            sds((ne, total, ff), BF),
            sds((ne, total, ff), BF),
            sds((ne, total, ff), BF),
        ),
        in_specs=[hbm] * 9,
        out_specs=tuple([vm] * 10),
        scratch_shapes=scratch,
        compiler_params=pltpu.CompilerParams(
            collective_id=0, has_side_effects=True, vmem_limit_bytes=60 * 1024 * 1024
        ),
    )(
        meta,
        tokens,
        cotangent,
        expert_gate,
        expert_up,
        expert_down,
        shared_gate,
        shared_up,
        shared_down,
    )
    gtok, gw, osg, osu, osd, stok, scot, hg, hu, hh = outs
    stok = stok.reshape(ne, re, dl)
    scot = scot.reshape(ne, re, dl)
    hg, hu, hh = (h[:, :re] for h in (hg, hu, hh))
    grad_gate = jnp.einsum("esd,esf->edf", stok, hg, preferred_element_type=F32)
    grad_up = jnp.einsum("esd,esf->edf", stok, hu, preferred_element_type=F32)
    grad_down = jnp.einsum("esf,esd->efd", hh, scot, preferred_element_type=F32)
    return gtok, gw.T, grad_gate, grad_up, grad_down, osg.T, osu.T, osd


def line_order(chip, length):
    high = (2 * chip) // length
    far = 1 - 2 * high
    edge = chip * (1 - high) + (length - 1 - chip) * high
    order = [(chip, None, None)]
    for p in range(1, length):
        two_sided = (2 * edge - p + 2 * length) // (2 * length)
        dist = two_sided * ((p + 1) // 2) + (1 - two_sided) * (p - edge)
        toward = far * (1 - 2 * two_sided * (p % 2))
        order.append((chip + toward * dist, chip - toward, two_sided))
    return order


def line_kernel(
    dims,
    routes_in,
    weights_in,
    tok_in,
    cot_in,
    eg_in,
    eu_in,
    ed_in,
    sg_in,
    su_in,
    sd_in,
    gtok,
    gw,
    osg,
    osu,
    osd,
    stok,
    scot,
    hg,
    hu,
    hh,
    routes,
    weights,
    all_tok,
    all_cot,
    all_meta,
    eg,
    eu,
    ed,
    sg,
    su,
    sd,
    gates,
    sh_part,
    sh_exact,
    sh_recv,
    sh_all,
    share_t,
    part,
    exact,
    recv,
    hs,
    dgp,
    dgs,
    dgb,
    back_send,
    back,
    shsum,
    load_sem,
    own_sem,
    own_s,
    line_s,
    line_r,
    mate_s,
    mate_r,
    shr_s,
    shr_r,
    sha_s,
    sha_r,
    pr_s,
    pr_r,
    pa_s,
    pa_r,
    xt_s,
    xt_r,
    xy_s,
    xy_r,
    bk_s,
    bk_r,
):
    ep, tp, tok, dl, ne, ff, sff, cap, rows, width, swidth, swid = dims
    me = lax.axis_index("ep")
    mt = lax.axis_index("tp")
    length = ep // CORES
    chip = me // CORES
    core = me % CORES
    mate = chip * CORES + (1 - core)
    pair = CORES * cap
    group = ne * pair
    home = ne * cap
    part_rows = swid // tp
    order = line_order(chip, length)
    bufs = (all_tok, all_meta, all_cot)

    owns = []
    for n, (src, dst) in enumerate(
        (
            (tok_in, all_tok.at[chip, core]),
            (cot_in, all_cot.at[chip, core]),
            (routes_in, routes),
            (weights_in, weights),
        )
    ):
        c = pltpu.make_async_copy(src, dst, own_sem.at[n])
        c.start()
        owns.append(c)
    loads = []
    for n, (src, dst) in enumerate(
        ((sg_in, sg), (su_in, su), (sd_in, sd), (eg_in, eg), (eu_in, eu), (ed_in, ed))
    ):
        c = pltpu.make_async_copy(src, dst, load_sem.at[n])
        c.start()
        loads.append(c)

    barrier = pltpu.get_barrier_semaphore()
    def greet(there):
        pl.semaphore_signal(barrier, inc=1, device_id={"ep": there * CORES + core})

    pl.semaphore_signal(barrier, inc=1, device_id={"ep": mate})
    for o in range(1, tp):
        pl.semaphore_signal(barrier, inc=1, device_id={"tp": (mt + o) % tp})
    pl.when(chip < length - 1)(lambda: greet(chip + 1))
    pl.when(chip > 0)(lambda: greet(chip - 1))
    above = (2 * length - 2 - chip) // length
    below = (chip + length - 1) // length

    pl.semaphore_wait(barrier, tp + above + below)

    sends = []

    def copy_of(src, dst, ssem, rsem, dev):
        return pltpu.make_async_remote_copy(
            src_ref=src, dst_ref=dst, send_sem=ssem, recv_sem=rsem, device_id=dev
        )

    def remote(src, dst, ssem, rsem, dev):
        copy_of(src, dst, ssem, rsem, dev).start()

    def got(block, sem):
        copy_of(block, block, own_s.at[0], sem, {"ep": mate}).wait_recv()

    def left(block, sem):
        copy_of(block, block, sem, own_s.at[0], {"ep": mate}).wait_send()

    def along_line(b, src, ssem, there):
        block = bufs[b].at[src, core]
        dest = ((there + length) % length) * CORES + core
        return copy_of(block, block, ssem, line_r.at[b * length + src], {"ep": dest})

    def to_mate(b, p):
        block = bufs[b].at[order[p][0], core]
        n = b * length + p
        return copy_of(block, block, mate_s.at[b], mate_r.at[n], {"ep": mate})

    def send_own(b):
        for d, there in enumerate((chip + 1, chip - 1)):
            c = along_line(b, chip, own_s.at[2 * b + d], there)
            inside = chip < length - 1 if d == 0 else chip > 0
            pl.when(inside)(c.start)
            sends.append((inside, c))

    def send_mate(b):
        to_mate(b, 0).start()

    owns[0].wait()
    send_own(0)
    send_mate(0)
    owns[1].wait()
    send_mate(2)

    owns[2].wait()
    owns[3].wait()
    table = jnp.concatenate(
        [
            routes[...].astype(F32),
            weights[...].astype(BF).astype(F32),
            jnp.zeros((4, tok), F32),
        ],
        axis=0,
    )
    picked = table.T
    earlier = lax.broadcasted_iota(jnp.int32, (tok, tok), 0) < lax.broadcasted_iota(
        jnp.int32, (tok, tok), 1
    )

    def count(hits):
        return jnp.sum(hits.astype(F32), axis=0, keepdims=True)

    first, second = picked[:, 0:1], picked[:, 1:2]
    ranks = [
        count((first == table[0:1]) & earlier),
        count((second == table[1:2]) & earlier) + count(first == table[1:2]),
    ]
    ranked = jnp.concatenate(ranks, axis=0)
    named = table[0:2]
    owner = jnp.floor((named + 0.5) * (1.0 / ne))
    which = named - owner * ne
    all_meta[chip, core] = jnp.concatenate(
        [
            named * rows + ranked,
            table[2:4],
            owner * home + which * cap + ranked,
            owner * 128 + which * pair + ranked,
        ],
        axis=0,
    )
    send_own(1)
    send_mate(1)

    relays = {}
    mates = {}
    for p in range(1, length):
        src, there, _ = order[p]
        for b in range(3):
            relays[b, p] = along_line(b, src, line_s.at[b * length + p], there)
            mates[b, p] = to_mate(b, p)
            if p < length - 1 or b < 2:
                sends.append(((there >= 0) & (there < length), relays[b, p]))

    def arrivals(p, which, cond=None):
        def run():
            _, there, _ = order[p]
            for b in which:
                relays[b, p].wait_recv()
                pl.when((there >= 0) & (there < length))(relays[b, p].start)
                mates[b, p].start()

        if cond is None:
            run()
        else:
            pl.when(cond)(run)

    def mate_wait(p, which):
        for b in which:
            to_mate(b, p).wait_recv()

    peers = [(mt + o) % tp for o in range(1, tp)]
    inner = chip * (length - 1 - chip) > 0
    outer = chip * (length - 1 - chip) < 1

    own_tok = all_tok[chip, core]
    own_cot = all_cot[chip, core]
    for n in range(3):
        loads[n].wait()
        val = dot(own_tok, (sg, su)[n][...]) if n < 2 else dot_t(own_cot, sd[...])
        for q in range(tp):
            piece = val[:, q * swidth : (q + 1) * swidth]
            sh_exact[q, n] = piece
            sh_part[q, n] = piece.astype(BF)
    for o in range(1, tp):
        peer = peers[o - 1]
        remote(sh_part.at[peer], sh_recv.at[o], shr_s.at[0], shr_r.at[0], {"tp": peer})
    others = pl.ds(1, tp - 1)
    any_tp = pl.ds(0, tp - 1)

    row_id = lax.broadcasted_iota(jnp.int32, (ne * rows, tok), 0)
    sels = {}

    def selection(p):
        src = order[p][0]
        halves = []
        gate = jnp.zeros((ne * rows, 1), F32)
        for jj in range(CORES):
            m = all_meta[src, jj]
            code = m[0:2, :].astype(jnp.int32) + (jj * cap - me * (ne * rows))
            p0 = (row_id == code[0:1, :]).astype(F32)
            p1 = (row_id == code[1:2, :]).astype(F32)
            halves.append((p0 + p1).astype(BF))
            gate = gate + jnp.sum(p0 * m[2:3, :] + p1 * m[3:4, :], axis=1, keepdims=True)
        sels[p] = jnp.concatenate(halves, axis=1)
        gate = jnp.concatenate([gate[e * rows : e * rows + pair] for e in range(ne)], axis=0)
        gates[p] = jnp.broadcast_to(gate, (group, 128))

    def products(p, which):
        src = order[p][0]
        buf, out = (all_cot, scot) if which == (2,) else (all_tok, stok)
        picked = dot(sels[p], buf[src].reshape(CORES * tok, dl)).astype(BF)
        for e in range(ne):
            out[e, p * rows : (p + 1) * rows, :] = picked[e * rows : (e + 1) * rows]
        for n in which:
            vals = []
            for e in range(ne):
                x = picked[e * rows : (e + 1) * rows]
                val = dot_t(x, ed[e]) if n == 2 else dot(x, (eg, eu)[n][e])
                vals.append(val[:pair])
            val = jnp.concatenate(vals, axis=0)
            for q in range(tp):
                piece = val[:, q * width : (q + 1) * width]
                exact[p, q, n] = piece
                part[p, q, n] = piece.astype(BF)
        half = 1 if which == (2,) else 0
        span = pl.ds(which[0], len(which))
        for o in range(1, tp):
            remote(
                part.at[p, peers[o - 1], span],
                recv.at[p, o, span],
                pr_s.at[0],
                pr_r.at[2 * p + half],
                {"tp": peers[o - 1]},
            )

    def products_all(p):
        selection(p)
        products(p, (0, 1))
        products(p, (2,))

    def send_hidden(p, piece):
        for o in range(1, tp):
            if piece < 2:
                block = hs.at[p, mt, pl.ds(2 * piece, 2 - piece)]
            else:
                block = dgp.at[p, mt]
            remote(
                block, block, pa_s.at[piece // 2], pa_r.at[3 * p + piece], {"tp": peers[o - 1]}
            )

    def hidden_got(p, piece):
        if piece < 2:
            got(hs.at[p, any_tp, pl.ds(2 * piece, 2 - piece)], pa_r.at[3 * p + piece])
        else:
            got(dgp.at[p, any_tp], pa_r.at[3 * p + piece])

    def hidden(p):
        got(recv.at[p, others, pl.ds(0, 2)], pr_r.at[2 * p])
        got(recv.at[p, others, pl.ds(2, 1)], pr_r.at[2 * p + 1])
        tot = [exact[p, mt, n] for n in range(3)]
        for o in range(1, tp):
            for n in range(3):
                tot[n] = tot[n] + recv[p, o, n].astype(F32)
        gate = gates[p][:, 0:1]
        logistic = jax.nn.sigmoid(tot[0])
        silu = tot[0] * logistic
        product = silu * tot[1]
        grad_act = gate * tot[2]
        hs[p, mt, 0] = (
            grad_act * tot[1] * logistic * (1.0 + tot[0] * (1.0 - logistic))
        ).astype(BF)
        hs[p, mt, 1] = (grad_act * silu).astype(BF)
        hs[p, mt, 2] = (gate * product).astype(BF)
        terms = tot[2] * product
        fill = jnp.zeros((128 - group, width), F32)
        cols = jnp.concatenate([terms, fill], axis=0).T
        dgp[p, mt] = jnp.broadcast_to(jnp.sum(cols, axis=0, keepdims=True), (8, 128))
        for piece in (2, 0, 1):
            send_hidden(p, piece)

    def pick_rows():
        at = lax.broadcasted_iota(jnp.int32, (group, group), 0)
        col = lax.broadcasted_iota(jnp.int32, (group, group), 1)
        wanted = at * 0
        for jj in range(CORES):
            for e in range(ne):
                low = jj * home + e * cap
                inside = (at >= low) & (at < low + cap)
                wanted = jnp.where(inside, at - low + e * pair + jj * cap, wanted)
        return (col == wanted).astype(F32).astype(BF)

    pick = pick_rows()
    held = []

    def give(c, hold):
        if hold:
            pl.when(outer)(c.start)
            held.append(c)
        else:
            c.start()

    def give_held():
        for c in held:
            c.start()

    def spread(p, n, out):
        full = jnp.concatenate([hs[p, q, n] for q in range(tp)], axis=1).astype(F32)
        fill = jnp.zeros((rows - pair, ff), F32)
        blocks = []
        for e in range(ne):
            block = full[e * pair : (e + 1) * pair]
            if rows > pair:
                block = jnp.concatenate([block, fill], axis=0)
            block = block.astype(BF)
            out[e, p * rows : (p + 1) * rows, :] = block
            blocks.append(block)
        return blocks

    def slots(p):
        src = order[p][0]
        hidden_got(p, 0)
        if p == length - 1:
            share_columns()
        a = spread(p, 0, hg)
        b = spread(p, 1, hu)
        pieces = 2 if p == length - 1 else 1
        span = dl // pieces
        for i in range(pieces):
            cols = slice(i * span, (i + 1) * span)
            vals = [
                (dot_t(a[e], eg[e, cols, :]) + dot_t(b[e], eu[e, cols, :]))[:pair]
                for e in range(ne)
            ]
            moved = dot(pick, jnp.concatenate(vals, axis=0).astype(BF))
            for jj in range(CORES):
                back_send[p, jj, :, cols] = moved[jj * home : (jj + 1) * home].astype(BF)
            if p == 0:
                back[me, :, cols] = back_send[0, core, :, cols]
                targets = [(1 - core, mate)]
            else:
                targets = [(jj, src * CORES + jj) for jj in range(CORES)]
            for jj, dest in targets:
                c = copy_of(
                    back_send.at[p, jj, :, pl.ds(i * span, span)],
                    back.at[me, :, pl.ds(i * span, span)],
                    bk_s.at[0],
                    bk_r.at[chip],
                    {"ep": dest},
                )
                give(c, p == 1)
        hidden_got(p, 2)
        total = dgp[p, 0]
        for q in range(1, tp):
            total = total + dgp[p, q]
        dgs[p] = total
        if p == 0:
            dgb[me] = total
        for jj, dest in targets:
            c = copy_of(dgs.at[p], dgb.at[me], bk_s.at[1], bk_r.at[length + chip], {"ep": dest})
            give(c, p == 1)

    def shared_hidden():
        got(sh_recv.at[others], shr_r.at[0])
        tot = [sh_exact[mt, n] for n in range(3)]
        for o in range(1, tp):
            for n in range(3):
                tot[n] = tot[n] + sh_recv[o, n].astype(F32)
        a, b, c3, _ = hidden_terms(tot[0], tot[1], tot[2], None)
        sh_all[mt, 0] = a
        sh_all[mt, 1] = b
        sh_all[mt, 2] = c3
        for o in range(1, tp):
            remote(
                sh_all.at[mt], sh_all.at[mt], sha_s.at[0], sha_r.at[0], {"tp": peers[o - 1]}
            )

    def share_columns():
        got(share_t.at[1, :, pl.ds(0, ep - 1), 0], xt_r.at[0])
        for o in range(1, tp):
            block = share_t.at[1, :, :, mt]
            remote(block, block, xy_s.at[0], xy_r.at[0], {"tp": peers[o - 1]})

    def shared_full(n):
        return jnp.concatenate([sh_all[q, n] for q in range(tp)], axis=1)

    def shared_shares():
        for n in range(3):
            back_t = shared_full(n).astype(F32).T.astype(BF)
            for j in range(ep):
                for q in range(tp):
                    low = j * swid + q * part_rows
                    share_t[0, n, j, q] = back_t[low : low + part_rows, :]
        for o in range(1, ep):
            peer = (me + o) % ep
            c = copy_of(
                share_t.at[0, :, peer, mt],
                share_t.at[1, :, me, mt],
                xt_s.at[0],
                xt_r.at[0],
                {"ep": peer},
            )
            give(c, True)
        for n in range(3):
            share_t[1, n, me, mt] = share_t[0, n, me, mt]

    def homeward(p):
        src = order[p][0]
        from_there = pl.ds(src * CORES, CORES) if p else pl.ds(mate, 1)
        got(back.at[from_there], bk_r.at[src])
        got(dgb.at[from_there], bk_r.at[length + src])
        for jj in range(CORES):
            j = src * CORES + jj
            g0 = (hcol == where_home[:, 4:5] - j * home).astype(F32)
            g1 = (hcol == where_home[:, 5:6] - j * home).astype(F32)
            shsum[...] += dot((g0 + g1).astype(BF), back[j])

    def hidden_rows(p):
        hidden_got(p, 1)
        spread(p, 2, hh)

    def first_arrivals(which):
        if length > 1:
            arrivals(1, which)
        if length > 2:
            arrivals(2, which, order[2][2] > 0)

    mate_wait(0, (0, 1))
    for n in range(3):
        loads[3 + n].wait()
    mate_wait(0, (2,))
    products_all(0)
    send_own(2)
    shared_hidden()
    first_arrivals((0, 1))
    hidden(0)
    last = length - 1
    for p in range(1, length):
        split = p == last
        if p == 1:
            first_arrivals((2,))
        elif not split:
            far = order[p][2] < 1 if p % 2 == 0 or p == last else None
            arrivals(p, (0, 1, 2), far)
            if p % 2 == 1 and p + 1 < last:
                arrivals(p + 1, (0, 1, 2), order[p + 1][2] > 0)
        else:
            arrivals(p, (0, 1), outer)
        mate_wait(p, (0, 1))
        selection(p)
        products(p, (0, 1))
        if split:
            got(sh_all.at[any_tp], sha_r.at[0])
            shared_shares()
            arrivals(p, (2,), outer)
        mate_wait(p, (2,))
        products(p, (2,))
        if p + 1 == last and last > 2:
            arrivals(last, (2,), inner)
        slots(p - 1)
        hidden(p)
        if p + 2 == last and last > 2:
            arrivals(last, (0, 1), inner)
    if last > 0:
        there = order[last][1]
        pl.when((there >= 0) & (there < length))(relays[2, last].wait_send)
    pl.when(inner)(give_held)
    shsum[...] = dot_t(shared_full(0), sg[...]) + dot_t(shared_full(1), su[...])
    for p in range(last):
        hidden_rows(p)
    own_meta = all_meta[chip, core]
    where_home = own_meta.T.astype(jnp.int32)
    hcol = lax.broadcasted_iota(jnp.int32, (tok, home), 1)
    lane_at = lax.broadcasted_iota(jnp.int32, (ep * 128, tok), 0)
    lanes = own_meta[6:8, :].astype(jnp.int32) + core * cap
    spots = [(lane_at == lanes[k : k + 1, :]).astype(F32).astype(BF) for k in range(2)]
    spots = jnp.concatenate(spots, axis=1)
    slots(last)
    homeward(0)

    homeward(1)
    homeward(2)
    got(share_t.at[1, :, :, any_tp], xy_r.at[0])
    flat = []
    for n in range(3):
        parts = [
            jnp.concatenate([share_t[1, n, j, q] for j in range(ep)], axis=1) for q in range(tp)
        ]
        flat.append(jnp.concatenate(parts, axis=0))
    tok_flat = all_tok[...].reshape(ep * tok, dl)
    osg[...] = dot(flat[0], tok_flat)
    osu[...] = dot(flat[1], tok_flat)
    osd[...] = dot(flat[2], all_cot[...].reshape(ep * tok, dl))

    hidden_rows(last)
    for p in range(3, length):
        homeward(p)
    gtok[...] = shsum[...].astype(BF)
    dg = jnp.concatenate([dgb[j] for j in range(ep)], axis=1)
    high = dg.astype(BF)
    low = (dg - high.astype(F32)).astype(BF)
    total = dot(high, spots) + dot(low, spots)
    gw[...] = jnp.concatenate(
        [total[0:1, :tok], total[0:1, tok:], jnp.zeros((6, tok), F32)], axis=0
    )
    for cond, c in sends:
        pl.when(cond)(c.wait_send)
    for b in range(3):
        left(bufs[b].at[:, 0], mate_s.at[b])
    left(sh_part.at[any_tp], shr_s.at[0])
    left(sh_all.at[any_tp], sha_s.at[0])
    left(part.at[:, any_tp], pr_s.at[0])
    left(hs.at[:, any_tp], pa_s.at[0])
    left(dgp.at[:, any_tp], pa_s.at[1])
    left(share_t.at[0, :, pl.ds(0, ep - 1), 0], xt_s.at[0])
    left(share_t.at[1, :, :, any_tp], xy_s.at[0])
    left(back.at[pl.ds(0, ep - 1)], bk_s.at[0])
    left(dgb.at[pl.ds(0, ep - 1)], bk_s.at[1])


def grads_kernel(
    dims,
    gtok,
    gw,
    osg,
    osu,
    osd,
    stok,
    scot,
    hg,
    hu,
    hh,
    gtok_out,
    gw_out,
    grad_gate,
    grad_up,
    grad_down,
    osg_out,
    osu_out,
    osd_out,
    gate_rows,
    up_rows,
    down_rows,
    out_sem,
):
    ne, chunks = dims
    outs = []

    def put(src, dst):
        c = pltpu.make_async_copy(src, dst, out_sem.at[len(outs)])
        c.start()
        outs.append(c)

    for src, dst in (
        (gtok, gtok_out),
        (gw.at[pl.ds(0, gw_out.shape[0])], gw_out),
        (osg, osg_out),
        (osu, osu_out),
        (osd, osd_out),
    ):
        put(src, dst)

    def outer(a, b):
        return lax.dot_general(a, b, (((0,), (0,)), ((), ())), preferred_element_type=F32)

    def cut(size):
        step = size // chunks
        return [slice(i * step, (i + 1) * step) for i in range(chunks)]

    for e in range(ne):
        for r in cut(stok.shape[2]):
            left = stok[e, :, r]
            gate_rows[e, r, :] = outer(left, hg[e])
            put(gate_rows.at[e, r], grad_gate.at[e, r])
            up_rows[e, r, :] = outer(left, hu[e])
            put(up_rows.at[e, r], grad_up.at[e, r])
    for e in range(ne):
        for r in cut(hh.shape[2]):
            down_rows[e, r, :] = outer(hh[e, :, r], scot[e])
            put(down_rows.at[e, r], grad_down.at[e, r])
    for c in outs:
        c.wait()


def line_body(
    tokens,
    routes,
    route_weights,
    cotangent,
    expert_gate,
    expert_up,
    expert_down,
    shared_gate,
    shared_up,
    shared_down,
):
    tok, top = routes.shape
    dl = tokens.shape[1]
    ne, _, ff = expert_gate.shape
    sff = shared_gate.shape[1]
    ep, tp = lax.axis_size("ep"), lax.axis_size("tp")
    cap = max(2, 5 * tok * top // (4 * ep * ne))
    length = ep // CORES
    pair = CORES * cap
    rows = up_to(pair, 16)
    group = ne * pair
    home = ne * cap
    width, swidth, swid = ff // tp, sff // tp, sff // ep
    dims = (ep, tp, tok, dl, ne, ff, sff, cap, rows, width, swidth, swid)

    hbm = pl.BlockSpec(memory_space=pltpu.HBM)
    vmem = pl.BlockSpec(memory_space=pltpu.VMEM)
    dma = pltpu.SemaphoreType.DMA
    sds = jax.ShapeDtypeStruct
    shapes = (
        sds((tok, dl), BF),
        sds((8, tok), F32),
        sds((swid, dl), F32),
        sds((swid, dl), F32),
        sds((swid, dl), F32),
        sds((ne, length * rows, dl), BF),
        sds((ne, length * rows, dl), BF),
        sds((ne, length * rows, ff), BF),
        sds((ne, length * rows, ff), BF),
        sds((ne, length * rows, ff), BF),
    )
    scratch = [
        pltpu.VMEM((top, tok), jnp.int32),
        pltpu.VMEM((top, tok), F32),
        pltpu.VMEM((length, CORES, tok, dl), BF),
        pltpu.VMEM((length, CORES, tok, dl), BF),
        pltpu.VMEM((length, CORES, 8, tok), F32),
        pltpu.VMEM(expert_gate.shape, BF),
        pltpu.VMEM(expert_up.shape, BF),
        pltpu.VMEM(expert_down.shape, BF),
        pltpu.VMEM(shared_gate.shape, BF),
        pltpu.VMEM(shared_up.shape, BF),
        pltpu.VMEM(shared_down.shape, BF),
        pltpu.VMEM((length, group, 128), F32),
        pltpu.VMEM((tp, 3, tok, swidth), BF),
        pltpu.VMEM((tp, 3, tok, swidth), F32),
        pltpu.VMEM((tp, 3, tok, swidth), BF),
        pltpu.VMEM((tp, 3, tok, swidth), BF),
        pltpu.VMEM((2, 3, ep, tp, swid // tp, tok), BF),
        pltpu.VMEM((length, tp, 3, group, width), BF),
        pltpu.VMEM((length, tp, 3, group, width), F32),
        pltpu.VMEM((length, tp, 3, group, width), BF),
        pltpu.VMEM((length, tp, 3, group, width), BF),
        pltpu.VMEM((length, tp, 8, 128), F32),
        pltpu.VMEM((length, 8, 128), F32),
        pltpu.VMEM((ep, 8, 128), F32),
        pltpu.VMEM((length, CORES, home, dl), BF),
        pltpu.VMEM((ep, home, dl), BF),
        pltpu.VMEM((tok, dl), F32),
        dma((6,)),
        dma((4,)),
        dma((6,)),
        dma((3 * length,)),
        dma((3 * length,)),
        dma((3,)),
        dma((3 * length,)),
        *[dma((1,))] * 5,
        dma((2 * length,)),
        dma((2,)),
        dma((3 * length,)),
        *[dma((1,))] * 4,
        dma((2,)),
        dma((2 * length,)),
    ]
    outs = pl.pallas_call(
        functools.partial(line_kernel, dims),
        out_shape=tuple([pltpu.VMEM(s.shape, s.dtype) for s in shapes]),
        in_specs=[hbm] * 10,
        out_specs=tuple([vmem] * len(shapes)),
        scratch_shapes=scratch,
        compiler_params=pltpu.CompilerParams(
            collective_id=0, has_side_effects=True, vmem_limit_bytes=48 * 1024 * 1024
        ),
    )(
        *[
            pltpu.with_memory_space_constraint(x, pltpu.HBM)
            for x in (
                routes.T,
                route_weights.T,
                tokens,
                cotangent,
                expert_gate,
                expert_up,
                expert_down,
                shared_gate,
                shared_up,
                shared_down,
            )
        ]
    )
    outs = [pltpu.with_memory_space_constraint(x, pltpu.VMEM) for x in outs]
    chunks = 4
    results = (
        sds((tok, dl), BF),
        sds((top, tok), F32),
        sds((ne, dl, ff), F32),
        sds((ne, dl, ff), F32),
        sds((ne, ff, dl), F32),
        sds((swid, dl), F32),
        sds((swid, dl), F32),
        sds((swid, dl), F32),
    )
    gtok, gw, grad_gate, grad_up, grad_down, osg, osu, osd = pl.pallas_call(
        functools.partial(grads_kernel, (ne, chunks)),
        out_shape=results,
        in_specs=[vmem] * len(shapes),
        out_specs=tuple([hbm] * len(results)),
        scratch_shapes=[
            *[pltpu.VMEM(s.shape, s.dtype) for s in results[2:5]],
            dma((3 * ne * chunks + 5,)),
        ],
        compiler_params=pltpu.CompilerParams(vmem_limit_bytes=24 * 1024 * 1024),
        name="grads",
    )(*outs)
    return gtok, gw.T, grad_gate, grad_up, grad_down, osg.T, osu.T, osd


def body(tokens, routes, *rest):
    tok, top = routes.shape
    ne, _, ff = rest[2].shape
    sff = rest[5].shape[1]
    ep, tp = lax.axis_size("ep"), lax.axis_size("tp")
    cap = max(2, 5 * tok * top // (4 * ep * ne))
    lines = (
        ep == 4 * CORES
        and ff == tp * 128
        and sff == tp * 128
        and (CORES * cap) % 8 == 0
        and (ne * cap) % 8 == 0
        and (ne * CORES * cap) % 16 == 0
        and ne * CORES * cap <= 128
        and tok == 128
        and sff % (ep * tp * 16) == 0
        and top == 2
    )
    return (line_body if lines else rows_body)(tokens, routes, *rest)


def solution(mesh):
    return jax.shard_map(
        body,
        mesh=mesh,
        in_specs=(
            P("ep", "tp"),
            P("ep", None),
            P("ep", None),
            P("ep", "tp"),
            P("ep", "tp", None),
            P("ep", "tp", None),
            P("ep", None, "tp"),
            P("tp", None),
            P("tp", None),
            P(None, "tp"),
        ),
        out_specs=(
            P("ep", "tp"),
            P("ep", None),
            P("ep", "tp", None),
            P("ep", "tp", None),
            P("ep", None, "tp"),
            P("tp", "ep"),
            P("tp", "ep"),
            P("ep", "tp"),
        ),
        check_vma=False,
    )
```

```python
import functools

import jax
import jax.numpy as jnp
from jax import lax
from jax.experimental import pallas as pl
from jax.experimental.pallas import tpu as pltpu
from jax.sharding import PartitionSpec as P

CORES = 2
BF = jnp.bfloat16
F32 = jnp.float32


def up_to(value, unit):
    return -(-value // unit) * unit


def dot(a, b):
    return jnp.dot(a, b, preferred_element_type=F32)


def dot_t(a, b):
    return lax.dot_general(a, b, (((1,), (1,)), ((), ())), preferred_element_type=F32)


def hidden_terms(gate_pre, up_pre, back_grad, scaling):
    logistic = jax.nn.sigmoid(gate_pre)
    silu = gate_pre * logistic
    product = silu * up_pre
    grad_act = back_grad if scaling is None else scaling * back_grad
    gate_grad = grad_act * up_pre * logistic * (1.0 + gate_pre * (1.0 - logistic))
    hidden = product if scaling is None else scaling * product
    return (
        gate_grad.astype(BF),
        (grad_act * silu).astype(BF),
        hidden.astype(BF),
        jnp.sum(back_grad * product, axis=-1, keepdims=True),
    )


def ring_plan(length):
    plan = []
    for step in range(1, length // 2 + 1):
        last_even = length % 2 == 0 and step == length // 2
        plan.append((step, 0, (0,) if last_even else (0, 1)))
        plan.append((step, 1, (1,) if last_even else (1, 0)))
    return plan


def rows_kernel(
    dims,
    meta_in,
    tok_in,
    cot_in,
    eg_in,
    eu_in,
    ed_in,
    sg_in,
    su_in,
    sd_in,
    gtok_out,
    gw_out,
    osg,
    osu,
    osd,
    stok,
    scot,
    hg,
    hu,
    hh,
    all_tok,
    all_cot,
    all_meta,
    eg,
    eu,
    ed,
    sg,
    su,
    sd,
    sel,
    gates,
    sh_part,
    sh_recv,
    sh_all,
    share_t,
    part,
    exact,
    recv,
    dgs,
    back_send,
    back,
    shsum,
    load_sem,
    own_sem,
    ring_s,
    ring_r,
    mate_s,
    mate_r,
    shr_s,
    shr_r,
    sha_s,
    sha_r,
    pr_s,
    pr_r,
    pa_s,
    pa_r,
    xt_s,
    xt_r,
    bk_s,
    bk_r,
):
    ep, tp, tok, dl, ne, ff, sff, cap, re, rows, rpp, rpt, cp, swid = dims
    me = lax.axis_index("ep")
    mt = lax.axis_index("tp")
    length = ep // CORES
    chip = me // CORES
    core = me % CORES
    mate = chip * CORES + (1 - core)
    nxt = ((chip + 1) % length) * CORES + core
    prv = ((chip + length - 1) % length) * CORES + core

    owns = []
    for n, (src, dst) in enumerate(((tok_in, all_tok), (cot_in, all_cot), (meta_in, all_meta))):
        c = pltpu.make_async_copy(src, dst.at[me], own_sem.at[n])
        c.start()
        owns.append(c)
    loads = []
    for n, (src, dst) in enumerate(
        ((sg_in, sg), (su_in, su), (sd_in, sd), (eg_in, eg), (eu_in, eu), (ed_in, ed))
    ):
        c = pltpu.make_async_copy(src, dst, load_sem.at[n])
        c.start()
        loads.append(c)

    barrier = pltpu.get_barrier_semaphore()
    for o in range(1, ep):
        pl.semaphore_signal(barrier, inc=1, device_id={"ep": (me + o) % ep})
    for o in range(1, tp):
        pl.semaphore_signal(barrier, inc=1, device_id={"tp": (mt + o) % tp})
    pl.semaphore_wait(barrier, ep + tp - 2)

    sends = []

    def remote(src, dst, ssem, rsem, dev):
        c = pltpu.make_async_remote_copy(
            src_ref=src, dst_ref=dst, send_sem=ssem, recv_sem=rsem, device_id=dev
        )
        c.start()
        sends.append(c)
        return c

    bufs = (all_tok, all_cot, all_meta)
    ring_copies = {}
    mate_copies = []
    plan = {(step, d): items for step, d, items in ring_plan(length)}

    def ring_send(step, d, item, src):
        dest = nxt if d == 0 else prv
        subs = (0, 2) if item == 0 else (1,)
        for b in subs:
            n = ((step - 1) * 2 + d) * 3 + b
            ring_copies[step, d, b] = remote(
                bufs[b].at[src], bufs[b].at[src], ring_s.at[n], ring_r.at[n], {"ep": dest}
            )

    def mate_send(item, src):
        for b in (0, 2) if item == 0 else (1,):
            n = len(mate_copies)
            mate_copies.append(
                remote(
                    bufs[b].at[src], bufs[b].at[src], mate_s.at[n], mate_r.at[n], {"ep": mate}
                )
            )

    for c in owns:
        c.wait()
    for pos in range(2):
        for d in range(2):
            items = plan.get((1, d), ())
            if pos < len(items):
                ring_send(1, d, items[pos], me)
    mate_send(0, me)
    mate_send(1, me)

    tp_order = [(mt + o) % tp for o in range(1, tp)]
    if rpt * tp > tok:
        sh_part[:, tok:, :] = jnp.zeros((3, rpt * tp - tok, sff), BF)
    for n in range(3):
        loads[n].wait()
        if n < 2:
            val = dot(all_tok[me], (sg, su)[n][...])
        else:
            val = dot_t(all_cot[me], sd[...])
        sh_part[n, :tok, :] = val.astype(BF)
    sh_copies = []
    for o in range(1, tp):
        peer = tp_order[o - 1]
        sh_copies.append(
            remote(
                sh_part.at[:, pl.ds(pl.multiple_of(peer * rpt, 16), rpt), :],
                sh_recv.at[o],
                shr_s.at[o],
                shr_r.at[o],
                {"tp": peer},
            )
        )

    def ring_arrivals(step):
        for pos in range(2):
            for d in range(2):
                items = plan.get((step, d), ())
                if pos >= len(items):
                    continue
                item = items[pos]
                away = length - step if d == 0 else step
                src = ((chip + away) % length) * CORES + core
                for b in (0, 2) if item == 0 else (1,):
                    ring_copies[step, d, b].wait_recv()
                if item in plan.get((step + 1, d), ()):
                    ring_send(step + 1, d, item, src)
                mate_send(item, src)

    if length > 1:
        ring_arrivals(1)

    for c in sh_copies:
        c.wait_recv()
    mine_t = pl.ds(pl.multiple_of(mt * rpt, 16), rpt)
    tot = [sh_part[n, mine_t, :].astype(F32) for n in range(3)]
    for o in range(1, tp):
        for n in range(3):
            tot[n] = tot[n] + sh_recv[o, n].astype(F32)
    a, b, c3, _ = hidden_terms(tot[0], tot[1], tot[2], None)
    sh_all[0, mine_t, :] = a
    sh_all[1, mine_t, :] = b
    sh_all[2, mine_t, :] = c3
    sha = []
    for o in range(1, tp):
        sha.append(
            remote(
                sh_all.at[:, mine_t, :],
                sh_all.at[:, mine_t, :],
                sha_s.at[o],
                sha_r.at[o],
                {"tp": tp_order[o - 1]},
            )
        )

    for step in range(2, length // 2 + 1):
        ring_arrivals(step)
    for c in mate_copies:
        c.wait_recv()

    row_id = lax.broadcasted_iota(jnp.int32, (rows, tok), 0)
    gate = jnp.zeros((rows, 1), F32)
    for j in range(ep):
        m = all_meta[j]
        code = m[0:2, :].astype(jnp.int32) + (j * cap - me * (ne * re))
        p0 = (row_id == code[0:1, :]).astype(F32)
        p1 = (row_id == code[1:2, :]).astype(F32)
        sel[:, j * tok : (j + 1) * tok] = (p0 + p1).astype(BF)
        gate = gate + jnp.sum(p0 * m[2:3, :] + p1 * m[3:4, :], axis=1, keepdims=True)
    te = rpp * tp
    for e in range(ne):
        gates[e, :re, :] = jnp.broadcast_to(gate[e * re : (e + 1) * re, :], (re, 128))
        if te > re:
            gates[e, re:, :] = jnp.zeros((te - re, 128), F32)
            part[e, :, re:, :] = jnp.zeros((3, te - re, ff), BF)
            exact[e, :, re:, :] = jnp.zeros((3, te - re, ff), F32)

    stok[...] = dot(sel[...], all_tok[...].reshape(ep * tok, dl)).astype(BF)
    scot[...] = dot(sel[...], all_cot[...].reshape(ep * tok, dl)).astype(BF)
    for n in range(3):
        loads[3 + n].wait()
    p_copies = [[] for _ in range(ne)]
    for e in range(ne):
        for n in range(3):
            r = slice(e * re, (e + 1) * re)
            val = dot_t(scot[r, :], ed[e]) if n == 2 else dot(stok[r, :], (eg, eu)[n][e])
            exact[e, n, :re, :] = val
            part[e, n, :re, :] = val.astype(BF)
            for o in range(1, tp):
                peer = tp_order[o - 1]
                k = (e * 3 + n) * tp + o
                p_copies[e].append(
                    remote(
                        part.at[e, n, pl.ds(pl.multiple_of(peer * rpp, 8), rpp), :],
                        recv.at[o, e, n],
                        pr_s.at[k],
                        pr_r.at[k],
                        {"tp": peer},
                    )
                )

    for c in sha:
        c.wait_recv()
    for n in range(3):
        back_t = sh_all[n, :tok, :].astype(F32).T.astype(BF)
        for j in range(ep):
            share_t[0, n, j] = back_t[j * swid : (j + 1) * swid, :]
    xts = []
    for o in range(1, ep):
        peer = (me + o) % ep
        xts.append(
            remote(
                share_t.at[0, :, peer],
                share_t.at[1, :, me],
                xt_s.at[o],
                xt_r.at[o],
                {"ep": peer},
            )
        )
    for n in range(3):
        share_t[1, n, me] = share_t[0, n, me]
    mine = pl.ds(pl.multiple_of(mt * rpp, 8), rpp)
    lane = lax.broadcasted_iota(jnp.int32, (rpp, 128), 1)
    pas = []
    for e in range(ne):
        for c in p_copies[e]:
            c.wait_recv()
        tot = [exact[e, n, mine, :] for n in range(3)]
        for o in range(1, tp):
            for n in range(3):
                tot[n] = tot[n] + recv[o, e, n].astype(F32)
        a, b, c3, dg = hidden_terms(tot[0], tot[1], tot[2], gates[e, mine, :][:, 0:1])
        hg[e, mine, :] = a
        hu[e, mine, :] = b
        hh[e, mine, :] = c3
        high = dg.astype(BF).astype(F32)
        dgs[e, mine, :] = jnp.where(
            lane == 0, high, jnp.where(lane == 1, dg - high, 0.0)
        ).astype(BF)
        group = []
        for k, buf in enumerate((hg, hu, dgs, hh)):
            for o in range(1, tp):
                n = (e * 4 + k) * tp + o
                group.append(
                    remote(
                        buf.at[e, mine, :],
                        buf.at[e, mine, :],
                        pa_s.at[n],
                        pa_r.at[n],
                        {"tp": tp_order[o - 1]},
                    )
                )
        pas.append(group)

    col = lax.broadcasted_iota(jnp.int32, (8, re), 1)
    block = jnp.zeros((8, re), jnp.int32)
    for j in range(1, ep):
        block = block + (col >= j * cap).astype(jnp.int32)
    target = block * cp + (col - block * cap)
    target = jnp.where(col < ep * cap, target, -1)
    pick = (
        (lax.broadcasted_iota(jnp.int32, (ep * cp, re), 0) == target[0:1, :])
        .astype(F32)
        .astype(BF)
    )
    bks = []
    for e in range(ne):
        for c in pas[e][: 3 * (tp - 1)]:
            c.wait_recv()
        slot = (dot_t(hg[e, :re, :], eg[e]) + dot_t(hu[e, :re, :], eu[e])).astype(BF)
        back_send[e, :, :, :dl] = dot(pick, slot).astype(BF).reshape(ep, cp, dl)
        back_send[e, :, :, dl:] = dot(pick, dgs[e, :re, :]).astype(BF).reshape(ep, cp, 128)
        for o in range(1, ep):
            peer = (me + o) % ep
            bks.append(
                remote(
                    back_send.at[e, peer],
                    back.at[e, me],
                    bk_s.at[e * ep + o],
                    bk_r.at[e * ep + o],
                    {"ep": peer},
                )
            )
        back[e, me] = back_send[e, me]

    shsum[...] = dot_t(sh_all[0, :tok, :], sg[...]) + dot_t(sh_all[1, :tok, :], su[...])
    for c in xts:
        c.wait_recv()
    flat = [
        jnp.concatenate([share_t[1, n, j] for j in range(ep)], axis=1) for n in range(3)
    ]
    tok_flat = all_tok[...].reshape(ep * tok, dl)
    osg[...] = dot(flat[0], tok_flat)
    osu[...] = dot(flat[1], tok_flat)
    osd[...] = dot(flat[2], all_cot[...].reshape(ep * tok, dl))

    width = ne * ep * cp
    home = all_meta[me].T.astype(jnp.int32)
    hcol = lax.broadcasted_iota(jnp.int32, (tok, width), 1)
    g0 = (hcol == home[:, 4:5]).astype(F32)
    g1 = (hcol == home[:, 5:6]).astype(F32)
    both = (g0 + g1).astype(BF)
    for c in bks:
        c.wait_recv()
    flat_back = back[...].reshape(width, dl + 128)
    gtok_out[...] = (dot(both, flat_back[:, :dl]) + shsum[...]).astype(BF)
    w0 = jnp.sum(dot(g0.astype(BF), flat_back[:, dl:]), axis=1, keepdims=True)
    w1 = jnp.sum(dot(g1.astype(BF), flat_back[:, dl:]), axis=1, keepdims=True)
    wl = lax.broadcasted_iota(jnp.int32, (tok, 128), 1)
    gw_out[...] = jnp.where(wl == 0, w0, w1).T[0:2, :]
    for group in pas:
        for c in group[3 * (tp - 1) :]:
            c.wait_recv()
    for c in sends:
        c.wait_send()


def rows_body(
    tokens,
    routes,
    route_weights,
    cotangent,
    expert_gate,
    expert_up,
    expert_down,
    shared_gate,
    shared_up,
    shared_down,
):
    tok, top = routes.shape
    dl = tokens.shape[1]
    ne, _, ff = expert_gate.shape
    sff = shared_gate.shape[1]
    ep, tp = lax.axis_size("ep"), lax.axis_size("tp")
    cap = max(2, 5 * tok * top // (4 * ep * ne))
    re = up_to(ep * cap, 16)
    rows = ne * re
    rpp = up_to(-(-re // tp), 8)
    rpt = up_to(-(-tok // tp), 16)
    cp = up_to(cap, 8)
    swid = sff // ep
    length = ep // CORES
    total = rpp * tp
    dims = (ep, tp, tok, dl, ne, ff, sff, cap, re, rows, rpp, rpt, cp, swid)

    picked = routes.T.reshape(-1)
    earlier = jnp.arange(top * tok)[None, :] < jnp.arange(top * tok)[:, None]
    same = picked[:, None] == picked[None, :]
    ranked = jnp.sum((same & earlier).astype(jnp.int32), axis=1)
    code = (picked * re + ranked).reshape(top, tok)
    home = (((picked % ne) * ep + picked // ne) * cp + ranked).reshape(top, tok)
    gate = route_weights.astype(BF).astype(F32).T
    meta = jnp.concatenate(
        [code.astype(F32), gate, home.astype(F32), jnp.zeros((8 - 3 * top, tok), F32)], axis=0
    )

    vm = pl.BlockSpec(memory_space=pltpu.VMEM)
    hbm = pl.BlockSpec(memory_space=pl.ANY)
    dma = pltpu.SemaphoreType.DMA
    n_ring = max(1, (length // 2) * 6)
    scratch = [
        pltpu.VMEM((ep, tok, dl), BF),
        pltpu.VMEM((ep, tok, dl), BF),
        pltpu.VMEM((ep, 8, tok), F32),
        pltpu.VMEM(expert_gate.shape, BF),
        pltpu.VMEM(expert_up.shape, BF),
        pltpu.VMEM(expert_down.shape, BF),
        pltpu.VMEM(shared_gate.shape, BF),
        pltpu.VMEM(shared_up.shape, BF),
        pltpu.VMEM(shared_down.shape, BF),
        pltpu.VMEM((rows, ep * tok), BF),
        pltpu.VMEM((ne, total, 128), F32),
        pltpu.VMEM((3, rpt * tp, sff), BF),
        pltpu.VMEM((tp, 3, rpt, sff), BF),
        pltpu.VMEM((3, rpt * tp, sff), BF),
        pltpu.VMEM((2, 3, ep, swid, tok), BF),
        pltpu.VMEM((ne, 3, total, ff), BF),
        pltpu.VMEM((ne, 3, total, ff), F32),
        pltpu.VMEM((tp, ne, 3, rpp, ff), BF),
        pltpu.VMEM((ne, total, 128), BF),
        pltpu.VMEM((ne, ep, cp, dl + 128), BF),
        pltpu.VMEM((ne, ep, cp, dl + 128), BF),
        pltpu.VMEM((tok, dl), F32),
        dma((6,)),
        dma((3,)),
        dma((n_ring,)),
        dma((n_ring,)),
        dma((3 * length,)),
        dma((3 * length,)),
        dma((tp,)),
        dma((tp,)),
        dma((tp,)),
        dma((tp,)),
        dma((3 * ne * tp,)),
        dma((3 * ne * tp,)),
        dma((4 * ne * tp,)),
        dma((4 * ne * tp,)),
        dma((ep,)),
        dma((ep,)),
        dma((ne * ep,)),
        dma((ne * ep,)),
    ]
    sds = jax.ShapeDtypeStruct
    outs = pl.pallas_call(
        functools.partial(rows_kernel, dims),
        out_shape=(
            sds((tok, dl), BF),
            sds((top, tok), F32),
            sds((swid, dl), F32),
            sds((swid, dl), F32),
            sds((swid, dl), F32),
            sds((rows, dl), BF),
            sds((rows, dl), BF),
            sds((ne, total, ff), BF),
            sds((ne, total, ff), BF),
            sds((ne, total, ff), BF),
        ),
        in_specs=[hbm] * 9,
        out_specs=tuple([vm] * 10),
        scratch_shapes=scratch,
        compiler_params=pltpu.CompilerParams(
            collective_id=0, has_side_effects=True, vmem_limit_bytes=60 * 1024 * 1024
        ),
    )(
        meta,
        tokens,
        cotangent,
        expert_gate,
        expert_up,
        expert_down,
        shared_gate,
        shared_up,
        shared_down,
    )
    gtok, gw, osg, osu, osd, stok, scot, hg, hu, hh = outs
    stok = stok.reshape(ne, re, dl)
    scot = scot.reshape(ne, re, dl)
    hg, hu, hh = (h[:, :re] for h in (hg, hu, hh))
    grad_gate = jnp.einsum("esd,esf->edf", stok, hg, preferred_element_type=F32)
    grad_up = jnp.einsum("esd,esf->edf", stok, hu, preferred_element_type=F32)
    grad_down = jnp.einsum("esf,esd->efd", hh, scot, preferred_element_type=F32)
    return gtok, gw.T, grad_gate, grad_up, grad_down, osg.T, osu.T, osd


def line_order(chip, length):
    high = (2 * chip) // length
    far = 1 - 2 * high
    edge = chip * (1 - high) + (length - 1 - chip) * high
    order = [(chip, None, None)]
    for p in range(1, length):
        two_sided = (2 * edge - p + 2 * length) // (2 * length)
        dist = two_sided * ((p + 1) // 2) + (1 - two_sided) * (p - edge)
        toward = far * (1 - 2 * two_sided * (p % 2))
        order.append((chip + toward * dist, chip - toward, two_sided))
    return order


def line_kernel(
    dims,
    routes_in,
    weights_in,
    tok_in,
    cot_in,
    eg_in,
    eu_in,
    ed_in,
    sg_in,
    su_in,
    sd_in,
    gtok,
    gw,
    osg,
    osu,
    osd,
    stok,
    scot,
    hg,
    hu,
    hh,
    routes,
    weights,
    all_tok,
    all_cot,
    all_meta,
    eg,
    eu,
    ed,
    sg,
    su,
    sd,
    gates,
    sh_part,
    sh_exact,
    sh_recv,
    sh_all,
    share_t,
    part,
    exact,
    recv,
    hs,
    dgp,
    dgs,
    dgb,
    back_send,
    back,
    shsum,
    load_sem,
    own_sem,
    own_s,
    line_s,
    line_r,
    mate_s,
    mate_r,
    shr_s,
    shr_r,
    sha_s,
    sha_r,
    pr_s,
    pr_r,
    pa_s,
    pa_r,
    xt_s,
    xt_r,
    xy_s,
    xy_r,
    bk_s,
    bk_r,
):
    ep, tp, tok, dl, ne, ff, sff, cap, rows, width, swidth, swid = dims
    me = lax.axis_index("ep")
    mt = lax.axis_index("tp")
    length = ep // CORES
    chip = me // CORES
    core = me % CORES
    mate = chip * CORES + (1 - core)
    pair = CORES * cap
    group = ne * pair
    home = ne * cap
    part_rows = swid // tp
    order = line_order(chip, length)
    bufs = (all_tok, all_meta, all_cot)

    owns = []
    for n, (src, dst) in enumerate(
        (
            (tok_in, all_tok.at[chip, core]),
            (cot_in, all_cot.at[chip, core]),
            (routes_in, routes),
            (weights_in, weights),
        )
    ):
        c = pltpu.make_async_copy(src, dst, own_sem.at[n])
        c.start()
        owns.append(c)
    loads = []
    for n, (src, dst) in enumerate(
        ((sg_in, sg), (su_in, su), (sd_in, sd), (eg_in, eg), (eu_in, eu), (ed_in, ed))
    ):
        c = pltpu.make_async_copy(src, dst, load_sem.at[n])
        c.start()
        loads.append(c)

    barrier = pltpu.get_barrier_semaphore()
    def greet(there):
        pl.semaphore_signal(barrier, inc=1, device_id={"ep": there * CORES + core})

    pl.semaphore_signal(barrier, inc=1, device_id={"ep": mate})
    for o in range(1, tp):
        pl.semaphore_signal(barrier, inc=1, device_id={"tp": (mt + o) % tp})
    pl.when(chip < length - 1)(lambda: greet(chip + 1))
    pl.when(chip > 0)(lambda: greet(chip - 1))
    above = (2 * length - 2 - chip) // length
    below = (chip + length - 1) // length

    pl.semaphore_wait(barrier, tp + above + below)

    sends = []

    def copy_of(src, dst, ssem, rsem, dev):
        return pltpu.make_async_remote_copy(
            src_ref=src, dst_ref=dst, send_sem=ssem, recv_sem=rsem, device_id=dev
        )

    def remote(src, dst, ssem, rsem, dev):
        copy_of(src, dst, ssem, rsem, dev).start()

    def got(block, sem):
        copy_of(block, block, own_s.at[0], sem, {"ep": mate}).wait_recv()

    def left(block, sem):
        copy_of(block, block, sem, own_s.at[0], {"ep": mate}).wait_send()

    def along_line(b, src, ssem, there):
        block = bufs[b].at[src, core]
        dest = ((there + length) % length) * CORES + core
        return copy_of(block, block, ssem, line_r.at[b * length + src], {"ep": dest})

    def to_mate(b, p):
        block = bufs[b].at[order[p][0], core]
        n = b * length + p
        return copy_of(block, block, mate_s.at[b], mate_r.at[n], {"ep": mate})

    def send_own(b):
        for d, there in enumerate((chip + 1, chip - 1)):
            c = along_line(b, chip, own_s.at[2 * b + d], there)
            inside = chip < length - 1 if d == 0 else chip > 0
            pl.when(inside)(c.start)
            sends.append((inside, c))

    def send_mate(b):
        to_mate(b, 0).start()

    owns[0].wait()
    send_own(0)
    send_mate(0)
    owns[1].wait()
    send_mate(2)

    owns[2].wait()
    owns[3].wait()
    table = jnp.concatenate(
        [
            routes[...].astype(F32),
            weights[...].astype(BF).astype(F32),
            jnp.zeros((4, tok), F32),
        ],
        axis=0,
    )
    picked = table.T
    earlier = lax.broadcasted_iota(jnp.int32, (tok, tok), 0) < lax.broadcasted_iota(
        jnp.int32, (tok, tok), 1
    )

    def count(hits):
        return jnp.sum(hits.astype(F32), axis=0, keepdims=True)

    first, second = picked[:, 0:1], picked[:, 1:2]
    ranks = [
        count((first == table[0:1]) & earlier),
        count((second == table[1:2]) & earlier) + count(first == table[1:2]),
    ]
    ranked = jnp.concatenate(ranks, axis=0)
    named = table[0:2]
    owner = jnp.floor((named + 0.5) * (1.0 / ne))
    which = named - owner * ne
    all_meta[chip, core] = jnp.concatenate(
        [
            named * rows + ranked,
            table[2:4],
            owner * home + which * cap + ranked,
            owner * 128 + which * pair + ranked,
        ],
        axis=0,
    )
    send_own(1)
    send_mate(1)

    relays = {}
    mates = {}
    for p in range(1, length):
        src, there, _ = order[p]
        for b in range(3):
            relays[b, p] = along_line(b, src, line_s.at[b * length + p], there)
            mates[b, p] = to_mate(b, p)
            if p < length - 1 or b < 2:
                sends.append(((there >= 0) & (there < length), relays[b, p]))

    def arrivals(p, which, cond=None):
        def run():
            _, there, _ = order[p]
            for b in which:
                relays[b, p].wait_recv()
                pl.when((there >= 0) & (there < length))(relays[b, p].start)
                mates[b, p].start()

        if cond is None:
            run()
        else:
            pl.when(cond)(run)

    def mate_wait(p, which):
        for b in which:
            to_mate(b, p).wait_recv()

    peers = [(mt + o) % tp for o in range(1, tp)]
    inner = chip * (length - 1 - chip) > 0
    outer = chip * (length - 1 - chip) < 1

    own_tok = all_tok[chip, core]
    own_cot = all_cot[chip, core]
    for n in range(3):
        loads[n].wait()
        val = dot(own_tok, (sg, su)[n][...]) if n < 2 else dot_t(own_cot, sd[...])
        for q in range(tp):
            piece = val[:, q * swidth : (q + 1) * swidth]
            sh_exact[q, n] = piece
            sh_part[q, n] = piece.astype(BF)
    for o in range(1, tp):
        peer = peers[o - 1]
        remote(sh_part.at[peer], sh_recv.at[o], shr_s.at[0], shr_r.at[0], {"tp": peer})
    others = pl.ds(1, tp - 1)
    any_tp = pl.ds(0, tp - 1)

    row_id = lax.broadcasted_iota(jnp.int32, (ne * rows, tok), 0)
    sels = {}

    def selection(p):
        src = order[p][0]
        halves = []
        gate = jnp.zeros((ne * rows, 1), F32)
        for jj in range(CORES):
            m = all_meta[src, jj]
            code = m[0:2, :].astype(jnp.int32) + (jj * cap - me * (ne * rows))
            p0 = (row_id == code[0:1, :]).astype(F32)
            p1 = (row_id == code[1:2, :]).astype(F32)
            halves.append((p0 + p1).astype(BF))
            gate = gate + jnp.sum(p0 * m[2:3, :] + p1 * m[3:4, :], axis=1, keepdims=True)
        sels[p] = jnp.concatenate(halves, axis=1)
        gate = jnp.concatenate([gate[e * rows : e * rows + pair] for e in range(ne)], axis=0)
        gates[p] = jnp.broadcast_to(gate, (group, 128))

    def products(p, which):
        src = order[p][0]
        buf, out = (all_cot, scot) if which == (2,) else (all_tok, stok)
        picked = dot(sels[p], buf[src].reshape(CORES * tok, dl)).astype(BF)
        for e in range(ne):
            out[e, p * rows : (p + 1) * rows, :] = picked[e * rows : (e + 1) * rows]
        for n in which:
            vals = []
            for e in range(ne):
                x = picked[e * rows : (e + 1) * rows]
                val = dot_t(x, ed[e]) if n == 2 else dot(x, (eg, eu)[n][e])
                vals.append(val[:pair])
            val = jnp.concatenate(vals, axis=0)
            for q in range(tp):
                piece = val[:, q * width : (q + 1) * width]
                exact[p, q, n] = piece
                part[p, q, n] = piece.astype(BF)
        half = 1 if which == (2,) else 0
        span = pl.ds(which[0], len(which))
        for o in range(1, tp):
            remote(
                part.at[p, peers[o - 1], span],
                recv.at[p, o, span],
                pr_s.at[0],
                pr_r.at[2 * p + half],
                {"tp": peers[o - 1]},
            )

    def products_all(p):
        selection(p)
        products(p, (0, 1))
        products(p, (2,))

    def send_hidden(p, piece):
        for o in range(1, tp):
            if piece < 2:
                block = hs.at[p, mt, pl.ds(2 * piece, 2 - piece)]
            else:
                block = dgp.at[p, mt]
            remote(
                block, block, pa_s.at[piece // 2], pa_r.at[3 * p + piece], {"tp": peers[o - 1]}
            )

    def hidden_got(p, piece):
        if piece < 2:
            got(hs.at[p, any_tp, pl.ds(2 * piece, 2 - piece)], pa_r.at[3 * p + piece])
        else:
            got(dgp.at[p, any_tp], pa_r.at[3 * p + piece])

    def hidden(p):
        got(recv.at[p, others, pl.ds(0, 2)], pr_r.at[2 * p])
        got(recv.at[p, others, pl.ds(2, 1)], pr_r.at[2 * p + 1])
        tot = [exact[p, mt, n] for n in range(3)]
        for o in range(1, tp):
            for n in range(3):
                tot[n] = tot[n] + recv[p, o, n].astype(F32)
        gate = gates[p][:, 0:1]
        logistic = jax.nn.sigmoid(tot[0])
        silu = tot[0] * logistic
        product = silu * tot[1]
        grad_act = gate * tot[2]
        hs[p, mt, 0] = (
            grad_act * tot[1] * logistic * (1.0 + tot[0] * (1.0 - logistic))
        ).astype(BF)
        hs[p, mt, 1] = (grad_act * silu).astype(BF)
        hs[p, mt, 2] = (gate * product).astype(BF)
        terms = tot[2] * product
        fill = jnp.zeros((128 - group, width), F32)
        cols = jnp.concatenate([terms, fill], axis=0).T
        dgp[p, mt] = jnp.broadcast_to(jnp.sum(cols, axis=0, keepdims=True), (8, 128))
        for piece in (2, 0, 1):
            send_hidden(p, piece)

    def pick_rows():
        at = lax.broadcasted_iota(jnp.int32, (group, group), 0)
        col = lax.broadcasted_iota(jnp.int32, (group, group), 1)
        wanted = at * 0
        for jj in range(CORES):
            for e in range(ne):
                low = jj * home + e * cap
                inside = (at >= low) & (at < low + cap)
                wanted = jnp.where(inside, at - low + e * pair + jj * cap, wanted)
        return (col == wanted).astype(F32).astype(BF)

    pick = pick_rows()
    held = []

    def give(c, hold):
        if hold:
            pl.when(outer)(c.start)
            held.append(c)
        else:
            c.start()

    def give_held():
        for c in held:
            c.start()

    def spread(p, n, out):
        full = jnp.concatenate([hs[p, q, n] for q in range(tp)], axis=1).astype(F32)
        fill = jnp.zeros((rows - pair, ff), F32)
        blocks = []
        for e in range(ne):
            block = full[e * pair : (e + 1) * pair]
            if rows > pair:
                block = jnp.concatenate([block, fill], axis=0)
            block = block.astype(BF)
            out[e, p * rows : (p + 1) * rows, :] = block
            blocks.append(block)
        return blocks

    def slots(p):
        src = order[p][0]
        hidden_got(p, 0)
        if p == length - 1:
            share_columns()
        a = spread(p, 0, hg)
        b = spread(p, 1, hu)
        pieces = 2 if p == length - 1 else 1
        span = dl // pieces
        for i in range(pieces):
            cols = slice(i * span, (i + 1) * span)
            vals = [
                (dot_t(a[e], eg[e, cols, :]) + dot_t(b[e], eu[e, cols, :]))[:pair]
                for e in range(ne)
            ]
            moved = dot(pick, jnp.concatenate(vals, axis=0).astype(BF))
            for jj in range(CORES):
                back_send[p, jj, :, cols] = moved[jj * home : (jj + 1) * home].astype(BF)
            if p == 0:
                back[me, :, cols] = back_send[0, core, :, cols]
                targets = [(1 - core, mate)]
            else:
                targets = [(jj, src * CORES + jj) for jj in range(CORES)]
            for jj, dest in targets:
                c = copy_of(
                    back_send.at[p, jj, :, pl.ds(i * span, span)],
                    back.at[me, :, pl.ds(i * span, span)],
                    bk_s.at[0],
                    bk_r.at[chip],
                    {"ep": dest},
                )
                give(c, p == 1)
        hidden_got(p, 2)
        total = dgp[p, 0]
        for q in range(1, tp):
            total = total + dgp[p, q]
        dgs[p] = total
        if p == 0:
            dgb[me] = total
        for jj, dest in targets:
            c = copy_of(dgs.at[p], dgb.at[me], bk_s.at[1], bk_r.at[length + chip], {"ep": dest})
            give(c, p == 1)

    def shared_hidden():
        got(sh_recv.at[others], shr_r.at[0])
        tot = [sh_exact[mt, n] for n in range(3)]
        for o in range(1, tp):
            for n in range(3):
                tot[n] = tot[n] + sh_recv[o, n].astype(F32)
        a, b, c3, _ = hidden_terms(tot[0], tot[1], tot[2], None)
        sh_all[mt, 0] = a
        sh_all[mt, 1] = b
        sh_all[mt, 2] = c3
        for o in range(1, tp):
            remote(
                sh_all.at[mt], sh_all.at[mt], sha_s.at[0], sha_r.at[0], {"tp": peers[o - 1]}
            )

    def share_columns():
        got(share_t.at[1, :, pl.ds(0, ep - 1), 0], xt_r.at[0])
        for o in range(1, tp):
            block = share_t.at[1, :, :, mt]
            remote(block, block, xy_s.at[0], xy_r.at[0], {"tp": peers[o - 1]})

    def shared_full(n):
        return jnp.concatenate([sh_all[q, n] for q in range(tp)], axis=1)

    def shared_shares():
        for n in range(3):
            back_t = shared_full(n).astype(F32).T.astype(BF)
            for j in range(ep):
                for q in range(tp):
                    low = j * swid + q * part_rows
                    share_t[0, n, j, q] = back_t[low : low + part_rows, :]
        for o in range(1, ep):
            peer = (me + o) % ep
            c = copy_of(
                share_t.at[0, :, peer, mt],
                share_t.at[1, :, me, mt],
                xt_s.at[0],
                xt_r.at[0],
                {"ep": peer},
            )
            give(c, True)
        for n in range(3):
            share_t[1, n, me, mt] = share_t[0, n, me, mt]

    def homeward(p):
        src = order[p][0]
        from_there = pl.ds(src * CORES, CORES) if p else pl.ds(mate, 1)
        got(back.at[from_there], bk_r.at[src])
        got(dgb.at[from_there], bk_r.at[length + src])
        for jj in range(CORES):
            j = src * CORES + jj
            g0 = (hcol == where_home[:, 4:5] - j * home).astype(F32)
            g1 = (hcol == where_home[:, 5:6] - j * home).astype(F32)
            shsum[...] += dot((g0 + g1).astype(BF), back[j])

    def hidden_rows(p):
        hidden_got(p, 1)
        spread(p, 2, hh)

    def first_arrivals(which):
        if length > 1:
            arrivals(1, which)
        if length > 2:
            arrivals(2, which, order[2][2] > 0)

    mate_wait(0, (0, 1))
    for n in range(3):
        loads[3 + n].wait()
    mate_wait(0, (2,))
    products_all(0)
    send_own(2)
    shared_hidden()
    first_arrivals((0, 1))
    hidden(0)
    last = length - 1
    for p in range(1, length):
        split = p == last
        if p == 1:
            first_arrivals((2,))
        elif not split:
            far = order[p][2] < 1 if p % 2 == 0 or p == last else None
            arrivals(p, (0, 1, 2), far)
            if p % 2 == 1 and p + 1 < last:
                arrivals(p + 1, (0, 1, 2), order[p + 1][2] > 0)
        else:
            arrivals(p, (0, 1), outer)
        mate_wait(p, (0, 1))
        selection(p)
        products(p, (0, 1))
        if split:
            got(sh_all.at[any_tp], sha_r.at[0])
            shared_shares()
            arrivals(p, (2,), outer)
        mate_wait(p, (2,))
        products(p, (2,))
        if p + 1 == last and last > 2:
            arrivals(last, (2,), inner)
        slots(p - 1)
        hidden(p)
        if p + 2 == last and last > 2:
            arrivals(last, (0, 1), inner)
    if last > 0:
        there = order[last][1]
        pl.when((there >= 0) & (there < length))(relays[2, last].wait_send)
    pl.when(inner)(give_held)
    shsum[...] = dot_t(shared_full(0), sg[...]) + dot_t(shared_full(1), su[...])
    for p in range(last):
        hidden_rows(p)
    own_meta = all_meta[chip, core]
    where_home = own_meta.T.astype(jnp.int32)
    hcol = lax.broadcasted_iota(jnp.int32, (tok, home), 1)
    lane_at = lax.broadcasted_iota(jnp.int32, (ep * 128, tok), 0)
    lanes = own_meta[6:8, :].astype(jnp.int32) + core * cap
    spots = [(lane_at == lanes[k : k + 1, :]).astype(F32).astype(BF) for k in range(2)]
    spots = jnp.concatenate(spots, axis=1)
    slots(last)
    homeward(0)

    homeward(1)
    homeward(2)
    got(share_t.at[1, :, :, any_tp], xy_r.at[0])
    flat = []
    for n in range(3):
        parts = [
            jnp.concatenate([share_t[1, n, j, q] for j in range(ep)], axis=1) for q in range(tp)
        ]
        flat.append(jnp.concatenate(parts, axis=0))
    tok_flat = all_tok[...].reshape(ep * tok, dl)
    osg[...] = dot(flat[0], tok_flat)
    osu[...] = dot(flat[1], tok_flat)
    osd[...] = dot(flat[2], all_cot[...].reshape(ep * tok, dl))

    hidden_rows(last)
    for p in range(3, length):
        homeward(p)
    gtok[...] = shsum[...].astype(BF)
    dg = jnp.concatenate([dgb[j] for j in range(ep)], axis=1)
    high = dg.astype(BF)
    low = (dg - high.astype(F32)).astype(BF)
    total = dot(high, spots) + dot(low, spots)
    gw[...] = jnp.concatenate(
        [total[0:1, :tok], total[0:1, tok:], jnp.zeros((6, tok), F32)], axis=0
    )
    for cond, c in sends:
        pl.when(cond)(c.wait_send)
    for b in range(3):
        left(bufs[b].at[:, 0], mate_s.at[b])
    left(sh_part.at[any_tp], shr_s.at[0])
    left(sh_all.at[any_tp], sha_s.at[0])
    left(part.at[:, any_tp], pr_s.at[0])
    left(hs.at[:, any_tp], pa_s.at[0])
    left(dgp.at[:, any_tp], pa_s.at[1])
    left(share_t.at[0, :, pl.ds(0, ep - 1), 0], xt_s.at[0])
    left(share_t.at[1, :, :, any_tp], xy_s.at[0])
    left(back.at[pl.ds(0, ep - 1)], bk_s.at[0])
    left(dgb.at[pl.ds(0, ep - 1)], bk_s.at[1])


def grads_kernel(
    dims,
    gtok,
    gw,
    osg,
    osu,
    osd,
    stok,
    scot,
    hg,
    hu,
    hh,
    gtok_out,
    gw_out,
    grad_gate,
    grad_up,
    grad_down,
    osg_out,
    osu_out,
    osd_out,
    gate_rows,
    up_rows,
    down_rows,
    out_sem,
):
    ne, chunks = dims
    outs = []

    def put(src, dst):
        c = pltpu.make_async_copy(src, dst, out_sem.at[len(outs)])
        c.start()
        outs.append(c)

    for src, dst in (
        (gtok, gtok_out),
        (gw.at[pl.ds(0, gw_out.shape[0])], gw_out),
        (osg, osg_out),
        (osu, osu_out),
        (osd, osd_out),
    ):
        put(src, dst)

    def send(src, dst, n):
        pltpu.make_async_copy(src, dst, out_sem.at[5 + n]).start()

    def outer(a, b):
        return lax.dot_general(a, b, (((0,), (0,)), ((), ())), preferred_element_type=F32)

    def cut(size):
        step = size // chunks
        return [slice(i * step, (i + 1) * step) for i in range(chunks)]

    for e in range(ne):
        for r in cut(stok.shape[2]):
            left = stok[e, :, r]
            gate_rows[e, r, :] = outer(left, hg[e])
            send(gate_rows.at[e, r], grad_gate.at[e, r], 0)
            up_rows[e, r, :] = outer(left, hu[e])
            send(up_rows.at[e, r], grad_up.at[e, r], 1)
    for e in range(ne):
        for r in cut(hh.shape[2]):
            down_rows[e, r, :] = outer(hh[e, :, r], scot[e])
            send(down_rows.at[e, r], grad_down.at[e, r], 2)
    for c in outs:
        c.wait()
    for n, (src, dst) in enumerate(
        ((gate_rows, grad_gate), (up_rows, grad_up), (down_rows, grad_down))
    ):
        pltpu.make_async_copy(src, dst, out_sem.at[5 + n]).wait()


def line_body(
    tokens,
    routes,
    route_weights,
    cotangent,
    expert_gate,
    expert_up,
    expert_down,
    shared_gate,
    shared_up,
    shared_down,
):
    tok, top = routes.shape
    dl = tokens.shape[1]
    ne, _, ff = expert_gate.shape
    sff = shared_gate.shape[1]
    ep, tp = lax.axis_size("ep"), lax.axis_size("tp")
    cap = max(2, 5 * tok * top // (4 * ep * ne))
    length = ep // CORES
    pair = CORES * cap
    rows = up_to(pair, 16)
    group = ne * pair
    home = ne * cap
    width, swidth, swid = ff // tp, sff // tp, sff // ep
    dims = (ep, tp, tok, dl, ne, ff, sff, cap, rows, width, swidth, swid)

    hbm = pl.BlockSpec(memory_space=pltpu.HBM)
    vmem = pl.BlockSpec(memory_space=pltpu.VMEM)
    dma = pltpu.SemaphoreType.DMA
    sds = jax.ShapeDtypeStruct
    shapes = (
        sds((tok, dl), BF),
        sds((8, tok), F32),
        sds((swid, dl), F32),
        sds((swid, dl), F32),
        sds((swid, dl), F32),
        sds((ne, length * rows, dl), BF),
        sds((ne, length * rows, dl), BF),
        sds((ne, length * rows, ff), BF),
        sds((ne, length * rows, ff), BF),
        sds((ne, length * rows, ff), BF),
    )
    scratch = [
        pltpu.VMEM((top, tok), jnp.int32),
        pltpu.VMEM((top, tok), F32),
        pltpu.VMEM((length, CORES, tok, dl), BF),
        pltpu.VMEM((length, CORES, tok, dl), BF),
        pltpu.VMEM((length, CORES, 8, tok), F32),
        pltpu.VMEM(expert_gate.shape, BF),
        pltpu.VMEM(expert_up.shape, BF),
        pltpu.VMEM(expert_down.shape, BF),
        pltpu.VMEM(shared_gate.shape, BF),
        pltpu.VMEM(shared_up.shape, BF),
        pltpu.VMEM(shared_down.shape, BF),
        pltpu.VMEM((length, group, 128), F32),
        pltpu.VMEM((tp, 3, tok, swidth), BF),
        pltpu.VMEM((tp, 3, tok, swidth), F32),
        pltpu.VMEM((tp, 3, tok, swidth), BF),
        pltpu.VMEM((tp, 3, tok, swidth), BF),
        pltpu.VMEM((2, 3, ep, tp, swid // tp, tok), BF),
        pltpu.VMEM((length, tp, 3, group, width), BF),
        pltpu.VMEM((length, tp, 3, group, width), F32),
        pltpu.VMEM((length, tp, 3, group, width), BF),
        pltpu.VMEM((length, tp, 3, group, width), BF),
        pltpu.VMEM((length, tp, 8, 128), F32),
        pltpu.VMEM((length, 8, 128), F32),
        pltpu.VMEM((ep, 8, 128), F32),
        pltpu.VMEM((length, CORES, home, dl), BF),
        pltpu.VMEM((ep, home, dl), BF),
        pltpu.VMEM((tok, dl), F32),
        dma((6,)),
        dma((4,)),
        dma((6,)),
        dma((3 * length,)),
        dma((3 * length,)),
        dma((3,)),
        dma((3 * length,)),
        *[dma((1,))] * 5,
        dma((2 * length,)),
        dma((2,)),
        dma((3 * length,)),
        *[dma((1,))] * 4,
        dma((2,)),
        dma((2 * length,)),
    ]
    outs = pl.pallas_call(
        functools.partial(line_kernel, dims),
        out_shape=tuple([pltpu.VMEM(s.shape, s.dtype) for s in shapes]),
        in_specs=[hbm] * 10,
        out_specs=tuple([vmem] * len(shapes)),
        scratch_shapes=scratch,
        compiler_params=pltpu.CompilerParams(
            collective_id=0, has_side_effects=True, vmem_limit_bytes=48 * 1024 * 1024
        ),
    )(
        *[
            pltpu.with_memory_space_constraint(x, pltpu.HBM)
            for x in (
                routes.T,
                route_weights.T,
                tokens,
                cotangent,
                expert_gate,
                expert_up,
                expert_down,
                shared_gate,
                shared_up,
                shared_down,
            )
        ]
    )
    outs = [pltpu.with_memory_space_constraint(x, pltpu.VMEM) for x in outs]
    chunks = 4
    results = (
        sds((tok, dl), BF),
        sds((top, tok), F32),
        sds((ne, dl, ff), F32),
        sds((ne, dl, ff), F32),
        sds((ne, ff, dl), F32),
        sds((swid, dl), F32),
        sds((swid, dl), F32),
        sds((swid, dl), F32),
    )
    gtok, gw, grad_gate, grad_up, grad_down, osg, osu, osd = pl.pallas_call(
        functools.partial(grads_kernel, (ne, chunks)),
        out_shape=results,
        in_specs=[vmem] * len(shapes),
        out_specs=tuple([hbm] * len(results)),
        scratch_shapes=[
            *[pltpu.VMEM(s.shape, s.dtype) for s in results[2:5]],
            dma((8,)),
        ],
        compiler_params=pltpu.CompilerParams(vmem_limit_bytes=24 * 1024 * 1024),
        name="grads",
    )(*outs)
    return gtok, gw.T, grad_gate, grad_up, grad_down, osg.T, osu.T, osd


def body(tokens, routes, *rest):
    tok, top = routes.shape
    ne, _, ff = rest[2].shape
    sff = rest[5].shape[1]
    ep, tp = lax.axis_size("ep"), lax.axis_size("tp")
    cap = max(2, 5 * tok * top // (4 * ep * ne))
    lines = (
        ep == 4 * CORES
        and ff == tp * 128
        and sff == tp * 128
        and (CORES * cap) % 8 == 0
        and (ne * cap) % 8 == 0
        and (ne * CORES * cap) % 16 == 0
        and ne * CORES * cap <= 128
        and tok == 128
        and sff % (ep * tp * 16) == 0
        and top == 2
    )
    return (line_body if lines else rows_body)(tokens, routes, *rest)


def solution(mesh):
    return jax.shard_map(
        body,
        mesh=mesh,
        in_specs=(
            P("ep", "tp"),
            P("ep", None),
            P("ep", None),
            P("ep", "tp"),
            P("ep", "tp", None),
            P("ep", "tp", None),
            P("ep", None, "tp"),
            P("tp", None),
            P("tp", None),
            P(None, "tp"),
        ),
        out_specs=(
            P("ep", "tp"),
            P("ep", None),
            P("ep", "tp", None),
            P("ep", "tp", None),
            P("ep", None, "tp"),
            P("tp", "ep"),
            P("tp", "ep"),
            P("ep", "tp"),
        ),
        check_vma=False,
    )
```
